32 devices in a mesh: sp: 16 (over z, y, x), tp: 2 (over core).
Axes of the slice: x: 2, y: 2, z: 4, core: 2. Of those that a mesh axis runs over, the one named last changes fastest.
Arguments:
- activations: bfloat16 [2048, 2048], P('sp', 'tp'), may hold values from -200 to 200
- norm_gain: float32 [2048], replicated, may hold values from 0.1 to 1.9
- state_proj: bfloat16 [2048, 1024], P(None, 'tp'), may hold values from -0.125 to 0.125
- value_proj: bfloat16 [2048, 1024], P(None, 'tp'), may hold values from -0.125 to 0.125
- post_gate_proj: bfloat16 [2048, 1024], P(None, 'tp'), may hold values from -0.125 to 0.125
- pre_gate_proj: bfloat16 [2048, 1024], P(None, 'tp'), may hold values from -0.125 to 0.125
- input_map: bfloat16 [64, 16, 128], P('tp'), may hold values from -1.5 to 1.5
- output_map: float32 [64, 128, 16], P('tp'), may hold values from -0.5 to 0.5
- skip_gain: float32 [1024], P('tp'), may hold values from -4 to 4
- rotation: float32 [64, 64], P('tp'), may hold values from -3.140625 to 3.140625
- log_decay: float32 [2048, 64], P('sp', 'tp'), may hold values from -1.5 to 0, as said below
- initial_state: float32 [2, 64, 64], P(None, 'tp'), may hold values from -12 to 12
- conv_taps: bfloat16 [3, 1024], P(None, 'tp'), may hold values from -3.5 to 3.5
- state_out: bfloat16 [1024, 2048], P(None, 'tp'), may hold values from -0.125 to 0.125
- conv_out: bfloat16 [1024, 2048], P(None, 'tp'), may hold values from -0.125 to 0.125
Outputs:
- layer_out: bfloat16 [2048, 2048], P('sp', 'tp')
The draws below stay inside these ranges and needn't reach their ends.
Inputs may be any that keep to these rules, and one draw needn't show every extreme that they name: `log_decay`: every entry is negative.
All inputs are finite; a program needn't handle non-finite values.
Results may differ from the reference program's by a relative error of at most 0.014.
Values may be sent and summed in bfloat16 or wider, within the bound.
A program may use at most 64 MiB of HBM per device.

```python
import math
import jax
import jax.numpy as jnp
from jax import lax

D = 2048
GROUP_CH = 16
STATE = 64
CONV_W = 3
TOK_DEV = 128
D_SSM = 1024
D_CONV = 1024
GROUPS = 64
TOKENS = 2048


def draw_activations(key, part):
    key_base, key_rows = jax.random.split(key, 2)
    column = jnp.arange(D, dtype=jnp.float32) / (D - 1)
    base = jnp.clip(jax.random.normal(key_base, (TOKENS, D), jnp.float32), -5.0, 5.0)
    row_scale = jnp.exp(jax.random.uniform(key_rows, (TOKENS, 1), jnp.float32, 0.0, math.log(4.0)))
    col_scale = jnp.exp(column * math.log(4.0))
    return (base * row_scale * col_scale[None, :]).astype(jnp.bfloat16)


def draw_log_decay(key, part):
    keys = jax.random.split(key, 5)
    share = 0.5
    slow = jax.random.bernoulli(keys[0], share, (1, GROUPS))
    blocks = TOKENS // TOK_DEV
    factor = jnp.exp(jax.random.uniform(keys[1], (blocks, 1, GROUPS), jnp.float32, 0.0, math.log(3.0)))
    factor = jnp.broadcast_to(factor, (blocks, TOK_DEV, GROUPS)).reshape(TOKENS, GROUPS)
    rough = jax.random.uniform(keys[2], (TOKENS, GROUPS), jnp.float32, 0.5, 1.5)
    rate = jnp.where(slow, 0.35 / TOKENS, 0.02)
    value = -rate * factor * rough
    spots = jax.random.randint(keys[3], (2, GROUPS), 0, TOKENS)
    depth = jnp.log(jax.random.uniform(keys[4], (2, GROUPS), jnp.float32, 0.5, 0.8))
    hit = jnp.arange(TOKENS, dtype=jnp.int32)[:, None, None] == spots[None, :, :]
    value = value + jnp.sum(jnp.where(hit, depth[None, :, :], 0.0), axis=1)
    return value.astype(jnp.float32)


def block_scale(key, dims, cuts, low, largest):
    def one(dim, blocks):
        steps = jax.random.uniform(jax.random.fold_in(jax.random.fold_in(key, 6), dim), (blocks,), jnp.float32, low / len(cuts), largest / len(cuts))
        return jnp.repeat(jnp.exp(steps), dims[dim] // blocks).reshape((-1,) + (1,) * (len(dims) - dim - 1))

    gain = one(*cuts[0])
    for cut in cuts[1:]:
        gain = gain * one(*cut)
    return gain


def gaussian(own_key, dims, width, reach, pieces=(), kind=jnp.bfloat16):
    values = jax.random.normal(own_key, dims, jnp.float32) * width
    if len(pieces) > 0:
        values = block_scale(own_key, dims, pieces, -0.22, 0.18) * values
    return jnp.clip(values, min=-reach, max=reach).astype(kind)


def setup_inputs(seed: int = 0) -> dict:
    arg_keys = jax.random.split(jax.random.key(seed), 16)
    activations = draw_activations(jax.random.fold_in(arg_keys[15], 71), 0)
    norm_gain = jnp.clip(1.0 + 0.18 * jax.random.normal(arg_keys[1], (D,), jnp.float32), 0.1, 1.9)
    state_proj = gaussian(arg_keys[2], (D, D_SSM), D ** -0.5, 0.125, ((1, 2),))
    value_proj = gaussian(arg_keys[3], (D, D_CONV), D ** -0.5, 0.125, ((1, 2),))
    post_gate_proj = gaussian(arg_keys[4], (D, D_CONV), D ** -0.5, 0.125, ((1, 2),))
    pre_gate_proj = gaussian(arg_keys[5], (D, D_CONV), D ** -0.5, 0.125, ((1, 2),))
    input_map = gaussian(arg_keys[6], (GROUPS, GROUP_CH, 2 * STATE), GROUP_CH ** -0.5, 1.5, ((0, 2),))
    output_map = gaussian(arg_keys[7], (GROUPS, 2 * STATE, GROUP_CH), (2 * STATE) ** -0.5, 0.5, ((0, 2),), jnp.float32)
    skip_gain = gaussian(arg_keys[8], (D_SSM,), 1.0, 4.0, ((0, 2),), jnp.float32)
    rotation = jnp.clip(jax.random.uniform(arg_keys[9], (GROUPS, STATE), jnp.float32, -3.140625, 3.140625), -3.140625, 3.140625)
    log_decay = draw_log_decay(jax.random.fold_in(arg_keys[15], 71), 0)
    initial_state = gaussian(arg_keys[11], (2, GROUPS, STATE), 2.0, 12.0, ((1, 2),), jnp.float32)
    conv_taps = gaussian(arg_keys[12], (CONV_W, D_CONV), CONV_W ** -0.5, 3.5, ((1, 2),))
    state_out = gaussian(arg_keys[13], (D_SSM, D), (D_SSM + D_CONV) ** -0.5, 0.125, ((1, 2),))
    conv_out = gaussian(arg_keys[14], (D_CONV, D), (D_SSM + D_CONV) ** -0.5, 0.125, ((1, 2),))
    return dict(activations=activations, norm_gain=norm_gain, state_proj=state_proj, value_proj=value_proj, post_gate_proj=post_gate_proj, pre_gate_proj=pre_gate_proj, input_map=input_map, output_map=output_map, skip_gain=skip_gain, rotation=rotation, log_decay=log_decay, initial_state=initial_state, conv_taps=conv_taps, state_out=state_out, conv_out=conv_out)


EPS = 1e-06

def combine(earlier, later):
    early_are, early_aim, early_hre, early_him = earlier
    late_are, late_aim, late_hre, late_him = later
    return (early_are * late_are - early_aim * late_aim, early_are * late_aim + early_aim * late_are, late_are * early_hre - late_aim * early_him + late_hre, late_are * early_him + late_aim * early_hre + late_him)

def reference(activations, norm_gain, state_proj, value_proj, post_gate_proj, pre_gate_proj, input_map, output_map, skip_gain, rotation, log_decay, initial_state, conv_taps, state_out, conv_out):
    span = math.gcd(TOKENS, 512)
    count = TOKENS // span
    states = GROUPS * STATE
    cos_rot = jnp.cos(rotation).reshape(1, states)
    sin_rot = jnp.sin(rotation).reshape(1, states)
    weights_in = (state_proj, value_proj, post_gate_proj, pre_gate_proj)
    taps = conv_taps.astype(jnp.float32)

    def block_step(carry, index):
        h_re, h_im, tail = carry
        start = (index * span).astype(jnp.int32)
        rows = lax.dynamic_slice_in_dim(activations, start, span, 0)
        decay = lax.dynamic_slice_in_dim(log_decay, start, span, 0)
        wide = rows.astype(jnp.float32)
        scale = lax.rsqrt(lax.optimization_barrier(jnp.mean(wide * wide, axis=1, keepdims=True)) + EPS)
        scaled = (wide * norm_gain[None, :]).astype(jnp.bfloat16)
        drive_in, value, post_gate, pre_gate = [(jnp.dot(scaled, weight, preferred_element_type=jnp.float32) * scale).astype(jnp.bfloat16) for weight in weights_in]
        grouped = drive_in.reshape(span, GROUPS, GROUP_CH).astype(jnp.float32)
        drive = jnp.einsum('tgc,gck->tgk', grouped, input_map.astype(jnp.float32))
        drive = drive * jnp.sqrt(-jnp.expm1(2.0 * decay))[:, :, None]
        drive_re = drive[:, :, :STATE].reshape(span, states)
        drive_im = drive[:, :, STATE:].reshape(span, states)
        magnitude = jnp.repeat(jnp.exp(decay), STATE, axis=1)
        factor_re = magnitude * cos_rot
        factor_im = magnitude * sin_rot
        cum_re, cum_im, loc_re, loc_im = lax.associative_scan(combine, (factor_re, factor_im, drive_re, drive_im), axis=0)
        state_re = loc_re + cum_re * h_re - cum_im * h_im
        state_im = loc_im + cum_re * h_im + cum_im * h_re
        stacked = jnp.concatenate([state_re.reshape(span, GROUPS, STATE), state_im.reshape(span, GROUPS, STATE)], axis=2)
        read = jnp.einsum('tgk,gkc->tgc', stacked, output_map, precision=lax.Precision.HIGHEST).reshape(span, D_SSM)
        hidden_state = jax.nn.gelu(read + skip_gain[None, :] * drive_in.astype(jnp.float32)).astype(jnp.bfloat16)
        mixed_in = (pre_gate.astype(jnp.float32) * value.astype(jnp.float32)).astype(jnp.bfloat16)
        padded = jnp.concatenate([tail, mixed_in], axis=0)
        conv = jnp.zeros((span, D_CONV), jnp.float32)
        for k in range(CONV_W):
            conv = conv + padded[k:k + span].astype(jnp.float32) * taps[k][None, :]
        hidden_conv = (post_gate.astype(jnp.float32) * conv).astype(jnp.bfloat16)
        result = (jnp.dot(hidden_state, state_out, preferred_element_type=jnp.float32) + jnp.dot(hidden_conv, conv_out, preferred_element_type=jnp.float32)).astype(jnp.bfloat16)
        return ((state_re[span - 1:], state_im[span - 1:], padded[span:]), result)
    start_carry = (initial_state[0].reshape(1, states).astype(jnp.float32), initial_state[1].reshape(1, states).astype(jnp.float32), jnp.zeros((CONV_W - 1, D_CONV), jnp.bfloat16))
    ignored, blocks = lax.scan(block_step, start_carry, jnp.arange(count, dtype=jnp.int32))
    return blocks.reshape(TOKENS, D)
```

```python
import functools

import jax
import jax.numpy as jnp
from jax import lax
from jax.experimental import pallas as pl
from jax.experimental.pallas import tpu as pltpu
from jax.sharding import PartitionSpec as P

EPS = 1e-06
LANES = 128
MESH = pl.DeviceIdType.MESH
F32 = jnp.float32
BF16 = jnp.bfloat16


def minus_expm1(y):
    poly = jnp.ones_like(y)
    for k in range(11, 1, -1):
        poly = 1.0 + poly * y * (1.0 / k)
    return jnp.where(y > -0.5, -y * poly, 1.0 - jnp.exp(y))


def split3(v):
    hi = v.astype(BF16)
    rest = v - hi.astype(F32)
    mid = rest.astype(BF16)
    low = (rest - mid.astype(F32)).astype(BF16)
    return hi, mid, low


def cmul(a, b):
    return a[0] * b[0] - a[1] * b[1], a[0] * b[1] + a[1] * b[0]


def cpow(base, count):
    result = None
    while count:
        if count & 1:
            result = base if result is None else cmul(result, base)
        count >>= 1
        if count:
            base = cmul(base, base)
    return result


def gelu(x):
    return 0.5 * x * (1.0 + jnp.tanh(0.7978845608028654 * (x + 0.044715 * x * x * x)))


def kernel(
    n,
    x_hbm,
    gain_hbm,
    w0_hbm,
    w1_hbm,
    w2_hbm,
    w3_hbm,
    imap_hbm,
    omap_hbm,
    skip_hbm,
    rot_hbm,
    ld_hbm,
    init_hbm,
    taps_hbm,
    so_hbm,
    co_hbm,
    out_ref,
    x_ref,
    gain_ref,
    imap_ref,
    omap_ref,
    skip_ref,
    rot_ref,
    ld_ref,
    init_ref,
    taps_ref,
    wv,
    ov,
    xr,
    acc,
    din,
    bd_in,
    bd_out,
    wide_w,
    mag,
    drv,
    pairs,
    pad,
    pay,
    ends,
    tot,
    tots,
    hs,
    hc,
    oacc,
    in_sem,
    wsem,
    osem,
    x_sem,
    tail_sem,
    hc_sem,
    hs_sem,
    send_sem,
    recv_sem,
    tsend_sem,
    trecv_sem,
    near,
    far_sem,
):
    sp, tp = lax.axis_index("sp"), lax.axis_index("tp")
    other = 1 - tp
    rows, half = x_ref.shape
    groups, state = rot_ref.shape
    gch = imap_ref.shape[1]
    chans = groups * gch
    states = groups * state
    prow = states // LANES
    per_block = LANES // gch
    blocks = groups // per_block
    quads = prow // blocks
    pitch = drv.shape[0] // rows
    bstates = quads * LANES
    cwide = taps_ref.shape[1]
    width = taps_ref.shape[0]

    barrier = pltpu.get_barrier_semaphore()
    partner = {"sp": sp, "tp": other}

    def greet(j, c):
        pl.semaphore_signal(barrier, inc=1, device_id={"sp": j, "tp": 1}, device_id_type=MESH)
        return c

    @pl.when(tp == 1)
    def _():
        pl.semaphore_signal(barrier, inc=1, device_id=partner, device_id_type=MESH)

    lax.fori_loop(0, sp, greet, 0)

    in_copies = {}
    def fetch(i, src, dst):
        in_copies[i] = pltpu.make_async_copy(src, dst, in_sem.at[i])
        in_copies[i].start()

    wcopies = {}

    def fetch_weight(i, h):
        w = (w0_hbm, w1_hbm, w2_hbm, w3_hbm)[i]
        part = (tp, other)[h]
        wcopies[i, h] = pltpu.make_async_copy(
            w.at[pl.ds(part * half, half), :], wv.at[i, h], wsem.at[i, h]
        )
        wcopies[i, h].start()

    fetch(0, x_hbm, x_ref)
    fetch(1, gain_hbm, gain_ref)
    fetch(2, rot_hbm, rot_ref)
    fetch(3, init_hbm, init_ref)
    fetch(4, ld_hbm, ld_ref)
    fetch(5, imap_hbm, imap_ref)
    fetch_weight(0, 0)
    fetch_weight(0, 1)
    fetch(6, omap_hbm, omap_ref)
    fetch(7, skip_hbm, skip_ref)
    fetch(8, taps_hbm, taps_ref)
    for i in (1, 3, 2):
        fetch_weight(i, 0)
        fetch_weight(i, 1)
    ocopies = {}
    for i, w, deep in ((1, co_hbm, cwide), (0, so_hbm, chans)):
        for h, part in ((0, tp), (1, other)):
            copy = pltpu.make_async_copy(w.at[pl.ds(part * deep, deep), :], ov.at[i, h], osem.at[i, h])
            copy.start()
            ocopies[i, h] = copy

    @pl.when(tp == 0)
    def _():
        pl.semaphore_wait(barrier, 1)
        pl.semaphore_signal(near, inc=1, device_id=partner, device_id_type=MESH)

    @pl.when(tp == 1)
    def _():
        pl.semaphore_wait(near, 1)

    def remote(src, dst, s, r, dev):
        return pltpu.make_async_remote_copy(
            src_ref=src, dst_ref=dst, send_sem=s, recv_sem=r, device_id=dev, device_id_type=MESH
        )

    in_copies[0].wait()
    x_copy = remote(x_ref, xr, x_sem.at[0], x_sem.at[1], partner)
    x_copy.start()

    for i in range(2, 6):
        in_copies[i].wait()

    lane = lax.broadcasted_iota(jnp.int32, (1, LANES), 1)
    for i, v in enumerate((rot_ref[...], init_ref[0], init_ref[1])):
        pairs[pl.ds(i * groups, groups), :] = jnp.concatenate([v, v], axis=1)

    def paired(i):
        even = pairs[pl.ds(i * groups, prow, stride=2), :]
        odd = pairs[pl.ds(i * groups + 1, prow, stride=2), :]
        return jnp.where(lane < state, even, odd)

    theta = paired(0)
    cosv, sinv = jnp.cos(theta), jnp.sin(theta)
    whole = cpow((cosv, sinv), rows)

    def spread_map(src, dst):
        dst[...] = jnp.zeros_like(dst)
        for b in range(blocks):
            for q in range(quads):
                g = b * per_block + 2 * q
                one = src[g].astype(F32)
                two = src[g + 1].astype(F32)
                one_r = jnp.concatenate([one[:, state:], one[:, :state]], axis=1)
                two_r = jnp.concatenate([two[:, state:], two[:, :state]], axis=1)
                low = lane < state
                re = jnp.concatenate([jnp.where(low, one, 0.0), jnp.where(low, 0.0, two_r)], axis=0)
                im = jnp.concatenate([jnp.where(low, one_r, 0.0), jnp.where(low, 0.0, two)], axis=0)
                at = pl.ds(b * LANES + q * 2 * gch, 2 * gch)
                dst[at, q * LANES : (q + 1) * LANES] = re.astype(BF16)
                dst[at, bstates + q * LANES : bstates + (q + 1) * LANES] = im.astype(BF16)

    spread_map(imap_ref, bd_in)

    ld = ld_ref[...].T
    mags = split3(jnp.exp(ld))
    whole_mags = split3(jnp.exp(jnp.sum(ld, axis=0, keepdims=True)))
    gains = split3(jnp.sqrt(minus_expm1(2.0 * ld)))[:2]
    for b in range(blocks):
        col = lax.broadcasted_iota(jnp.int32, (groups, bstates), 1) + b * bstates
        row = lax.broadcasted_iota(jnp.int32, (groups, bstates), 0)
        spread = jnp.where(
            (col >= row * state) & (col < (row + 1) * state), 1.0, 0.0
        ).astype(BF16)

        def over(pieces):
            total = None
            for piece in pieces:
                d = jnp.dot(piece, spread, preferred_element_type=F32)
                total = d if total is None else total + d
            return total

        m = over(mags)
        for q in range(quads):
            mag[pl.ds(b * quads + q, rows, stride=prow), :] = m[:, q * LANES : (q + 1) * LANES]
        m = over(whole_mags)
        for q in range(quads):
            tot[b * quads + q : b * quads + q + 1, :] = m[:, q * LANES : (q + 1) * LANES]
        wide_w[:, b * bstates : (b + 1) * bstates] = over(gains)

    def tot_copy(j):
        return remote(
            tot, tots.at[sp], tsend_sem.at[j], trecv_sem.at[sp], {"sp": j, "tp": tp}
        )

    def send_tot(j, c):
        tot_copy(j).start()
        return c

    in_copies[1].wait()
    own = x_ref[...].astype(F32)
    scaled = (own * gain_ref[:, pl.ds(pl.multiple_of(tp * half, LANES), half)]).astype(BF16)
    squares = jnp.sum(own * own, axis=1, keepdims=True)
    wcopies[0, 0].wait()
    partial = jnp.dot(scaled, wv[0, 0], preferred_element_type=F32)
    acc[0] = scaled

    x_copy.wait_recv()
    far_x = xr[...].astype(F32)
    scaled_far = (far_x * gain_ref[:, pl.ds(pl.multiple_of(other * half, LANES), half)]).astype(BF16)
    squares = squares + jnp.sum(far_x * far_x, axis=1, keepdims=True)
    scale = lax.rsqrt(squares / (2 * half) + EPS)

    acc[1] = scaled_far
    wcopies[0, 1].wait()
    total = partial + jnp.dot(scaled_far, wv[0, 1], preferred_element_type=F32)
    drive_in = (total * scale).astype(BF16)
    din[...] = drive_in
    for b in range(blocks):
        blk = jnp.dot(
            drive_in[:, b * LANES : (b + 1) * LANES],
            bd_in[b * LANES : (b + 1) * LANES, :],
            preferred_element_type=F32,
        )
        for q in range(quads):
            r = b * quads + q
            w = wide_w[:, r * LANES : (r + 1) * LANES]
            drv[pl.ds(r, rows, stride=pitch), :] = blk[:, q * LANES : (q + 1) * LANES] * w
            drv[pl.ds(prow + r, rows, stride=pitch), :] = (
                blk[:, bstates + q * LANES : bstates + (q + 1) * LANES] * w
            )

    def advance(t, h):
        m = mag[pl.ds(pl.multiple_of(t * prow, prow), prow), :]
        base = pl.multiple_of(t * pitch, 8)
        d_re = drv[pl.ds(base, prow), :]
        d_im = drv[pl.ds(base + prow, prow), :]
        f_re, f_im = m * cosv, m * sinv
        new_re = (f_re * h[0] + d_re) - f_im * h[1]
        new_im = (f_re * h[1] + d_im) + f_im * h[0]
        return base, (new_re, new_im)

    def first(t, c):
        base, h = advance(t, c)
        return h

    zero = jnp.zeros((prow, LANES), F32)
    e_re, e_im = lax.fori_loop(0, rows, first, (zero, zero), unroll=8)
    pay[pl.ds(0, prow), :] = e_re.astype(BF16)
    pay[pl.ds(prow, prow), :] = e_im.astype(BF16)

    def end_copy(j):
        return remote(
            pay, ends.at[sp], send_sem.at[j], recv_sem.at[sp], {"sp": j, "tp": tp}
        )

    def send_end(j, c):
        end_copy(j).start()
        return c

    @pl.when((tp == 1) & (sp < n - 1))
    def _():
        pl.semaphore_wait(barrier, 2 * (n - 1 - sp))
        pl.semaphore_signal(far_sem, inc=1, device_id=partner, device_id_type=MESH)

    @pl.when((tp == 0) & (sp < n - 1))
    def _():
        pl.semaphore_wait(far_sem, 1)

    lax.fori_loop(sp + 1, n, send_end, 0)
    lax.fori_loop(sp + 1, n, send_tot, 0)

    def project(i):
        wcopies[i, 0].wait()
        wcopies[i, 1].wait()
        total = jnp.dot(acc[0], wv[i, 0], preferred_element_type=F32)
        total = total + jnp.dot(acc[1], wv[i, 1], preferred_element_type=F32)
        return (total * scale).astype(BF16)

    value = project(1)
    pre_gate = project(3)
    mixed = (pre_gate.astype(F32) * value.astype(F32)).astype(BF16).astype(F32)
    pad[pl.ds(8, rows), :] = mixed
    tail_copy = remote(
        pad.at[pl.ds(rows, 8), :],
        pad.at[pl.ds(0, 8), :],
        tail_sem.at[0],
        tail_sem.at[1],
        {"sp": lax.rem(sp + 1, n), "tp": tp},
    )

    @pl.when(sp < n - 1)
    def _():
        tail_copy.start()

    hc[0] = project(2)

    for i in (6, 7):
        in_copies[i].wait()
    spread_map(omap_ref, bd_out)

    def gather(k, h):
        remote(pay, ends.at[k], send_sem.at[k], recv_sem.at[k], {"sp": k, "tp": tp}).wait_recv()
        remote(tot, tots.at[k], tsend_sem.at[k], trecv_sem.at[k], {"sp": k, "tp": tp}).wait_recv()
        k_mag = tots[k]
        moved = cmul((whole[0] * k_mag, whole[1] * k_mag), h)
        k_re = ends[k, pl.ds(0, prow), :].astype(F32)
        k_im = ends[k, pl.ds(prow, prow), :].astype(F32)
        return moved[0] + k_re, moved[1] + k_im

    enter = lax.fori_loop(0, sp, gather, (paired(1), paired(2)))

    def second(t, c):
        base, h = advance(t, c)
        drv[pl.ds(base, prow), :] = h[0]
        drv[pl.ds(base + prow, prow), :] = h[1]
        return h

    lax.fori_loop(0, rows, second, enter, unroll=8)

    @pl.when(sp == 0)
    def _():
        pad[pl.ds(0, 8), :] = jnp.zeros((8, cwide), F32)

    in_copies[8].wait()

    @pl.when(sp > 0)
    def _():
        tail_copy.wait_recv()

    conv = jnp.zeros((rows, cwide), F32)
    for k in range(width):
        conv = conv + pad[pl.ds(8 + k - (width - 1), rows), :] * taps_ref[k : k + 1, :].astype(F32)
    hc[0] = (hc[0].astype(F32) * conv).astype(BF16)
    hc_copy = remote(hc.at[0], hc.at[1], hc_sem.at[0], hc_sem.at[1], partner)
    hc_copy.start()
    hs_copies = []
    for b in range(blocks):
        at = [b * quads + q for q in range(quads)]
        at = at + [prow + r for r in at]
        cols = slice(b * LANES, (b + 1) * LANES)
        st = jnp.concatenate(
            [drv[pl.ds(r, rows, stride=pitch), :].astype(BF16) for r in at], axis=1
        )
        read = lax.dot_general(
            st, bd_out[cols, :], (((1,), (1,)), ((), ())), preferred_element_type=F32
        )
        hs[0, :, cols] = gelu(read + skip_ref[:, cols] * din[:, cols].astype(F32)).astype(BF16)
        if b % 2 == 1:
            two = pl.ds((b - 1) * LANES, 2 * LANES)
            copy = remote(
                hs.at[0, :, two], hs.at[1, :, two], hs_sem.at[0, b // 2], hs_sem.at[1, b // 2], partner
            )
            copy.start()
            hs_copies.append(copy)
    for i in (0, 1):
        for h in (0, 1):
            ocopies[i, h].wait()
    oacc[...] = jnp.dot(hc[0], ov[1, 0], preferred_element_type=F32)
    oacc[...] += jnp.dot(hs[0], ov[0, 0], preferred_element_type=F32)
    hc_copy.wait_recv()
    oacc[...] += jnp.dot(hc[1], ov[1, 1], preferred_element_type=F32)
    for copy in hs_copies:
        copy.wait_recv()
    out_ref[...] = (oacc[...] + jnp.dot(hs[1], ov[0, 1], preferred_element_type=F32)).astype(BF16)

    x_copy.wait_send()
    hc_copy.wait_send()
    for copy in hs_copies:
        copy.wait_send()

    @pl.when(sp < n - 1)
    def _():
        tail_copy.wait_send()

    def sent(j, c):
        end_copy(j).wait_send()
        tot_copy(j).wait_send()
        return c

    lax.fori_loop(sp + 1, n, sent, 0)


def on_device(
    activations,
    norm_gain,
    state_proj,
    value_proj,
    post_gate_proj,
    pre_gate_proj,
    input_map,
    output_map,
    skip_gain,
    rotation,
    log_decay,
    initial_state,
    conv_taps,
    state_out,
    conv_out,
):
    n = lax.axis_size("sp")
    rows, half = activations.shape
    groups, state = rotation.shape
    chans = state_proj.shape[1]
    cwide = value_proj.shape[1]
    outs = state_out.shape[1]
    states = groups * state
    prow = states // LANES
    bdw = 2 * states // (chans // LANES)
    vmem = pl.BlockSpec(memory_space=pltpu.VMEM)
    hbm = pl.BlockSpec(memory_space=pl.ANY)
    dma = pltpu.SemaphoreType.DMA
    return pl.pallas_call(
        functools.partial(kernel, n),
        out_shape=pltpu.VMEM((rows, outs), BF16),
        in_specs=[hbm] * 15,
        out_specs=vmem,
        scratch_shapes=[
            pltpu.VMEM((rows, half), BF16),
            pltpu.VMEM((1, 2 * half), F32),
            pltpu.VMEM(input_map.shape, BF16),
            pltpu.VMEM((groups, output_map.shape[2], output_map.shape[1]), F32),
            pltpu.VMEM((1, chans), F32),
            pltpu.VMEM((groups, state), F32),
            pltpu.VMEM((groups, rows), F32),
            pltpu.VMEM(initial_state.shape, F32),
            pltpu.VMEM(conv_taps.shape, BF16),
            pltpu.VMEM((4, 2, half, chans), BF16),
            pltpu.VMEM((2, 2, chans, outs), BF16),
            pltpu.VMEM((rows, half), BF16),
            pltpu.VMEM((2, rows, half), BF16),
            pltpu.VMEM((rows, chans), BF16),
            pltpu.VMEM((chans, bdw), BF16),
            pltpu.VMEM((chans, bdw), BF16),
            pltpu.VMEM((rows, states), F32),
            pltpu.VMEM((rows * prow, LANES), F32),
            pltpu.VMEM((rows * (2 * prow + 8), LANES), F32),
            pltpu.VMEM((3 * groups, LANES), F32),
            pltpu.VMEM((rows + 8, cwide), F32),
            pltpu.VMEM((2 * prow, LANES), BF16),
            pltpu.VMEM((n, 2 * prow, LANES), BF16),
            pltpu.VMEM((prow, LANES), F32),
            pltpu.VMEM((n, prow, LANES), F32),
            pltpu.VMEM((2, rows, chans), BF16),
            pltpu.VMEM((2, rows, cwide), BF16),
            pltpu.VMEM((rows, outs), F32),
            dma((9,)),
            dma((4, 2)),
            dma((2, 2)),
            dma((2,)),
            dma((2,)),
            dma((2,)),
            dma((2, chans // (2 * LANES))),
            dma((n,)),
            dma((n,)),
            dma((n,)),
            dma((n,)),
            pltpu.SemaphoreType.REGULAR,
            pltpu.SemaphoreType.REGULAR,
        ],
        compiler_params=pltpu.CompilerParams(collective_id=0, has_side_effects=True),
    )(
        activations,
        norm_gain.reshape(1, -1),
        state_proj,
        value_proj,
        post_gate_proj,
        pre_gate_proj,
        input_map,
        jnp.swapaxes(output_map, 1, 2),
        skip_gain.reshape(1, -1),
        rotation,
        jnp.swapaxes(log_decay, 0, 1),
        initial_state,
        conv_taps,
        state_out,
        conv_out,
    )


def solution(mesh):
    return jax.shard_map(
        on_device,
        mesh=mesh,
        in_specs=(
            P("sp", "tp"),
            P(),
            P(None, "tp"),
            P(None, "tp"),
            P(None, "tp"),
            P(None, "tp"),
            P("tp", None, None),
            P("tp", None, None),
            P("tp"),
            P("tp", None),
            P("sp", "tp"),
            P(None, "tp", None),
            P(None, "tp"),
            P(None, "tp"),
            P(None, "tp"),
        ),
        out_specs=P("sp", "tp"),
        check_vma=False,
    )
```

```python
import functools

import jax
import jax.numpy as jnp
from jax import lax
from jax.experimental import pallas as pl
from jax.experimental.pallas import tpu as pltpu
from jax.sharding import PartitionSpec as P

EPS = 1e-06
LANES = 128
MESH = pl.DeviceIdType.MESH
F32 = jnp.float32
BF16 = jnp.bfloat16


def minus_expm1(y):
    poly = jnp.ones_like(y)
    for k in range(11, 1, -1):
        poly = 1.0 + poly * y * (1.0 / k)
    return jnp.where(y > -0.5, -y * poly, 1.0 - jnp.exp(y))


def split3(v):
    hi = v.astype(BF16)
    rest = v - hi.astype(F32)
    mid = rest.astype(BF16)
    low = (rest - mid.astype(F32)).astype(BF16)
    return hi, mid, low


def cmul(a, b):
    return a[0] * b[0] - a[1] * b[1], a[0] * b[1] + a[1] * b[0]


def cpow(base, count):
    result = None
    while count:
        if count & 1:
            result = base if result is None else cmul(result, base)
        count >>= 1
        if count:
            base = cmul(base, base)
    return result


def inner_of(n):
    return max(d for d in range(1, n + 1) if n % d == 0 and d * d <= n)


def gelu(x):
    return 0.5 * x * (1.0 + jnp.tanh(0.7978845608028654 * (x + 0.044715 * x * x * x)))


def kernel(
    n,
    x_hbm,
    gain_hbm,
    w0_hbm,
    w1_hbm,
    w2_hbm,
    w3_hbm,
    imap_hbm,
    omap_hbm,
    skip_hbm,
    rot_hbm,
    ld_hbm,
    init_hbm,
    taps_hbm,
    so_hbm,
    co_hbm,
    out_ref,
    x_ref,
    gain_ref,
    imap_ref,
    omap_ref,
    skip_ref,
    rot_ref,
    ld_ref,
    init_ref,
    taps_ref,
    wv,
    ov,
    xr,
    acc,
    din,
    bd_in,
    bd_out,
    wide_w,
    mag,
    drv,
    pairs,
    pad,
    tot,
    near_in,
    far_in,
    far_out,
    hs,
    hc,
    oacc,
    in_sem,
    wsem,
    osem,
    x_sem,
    tail_sem,
    hc_sem,
    hs_sem,
    near_send,
    near_recv,
    far_send,
    far_recv,
    near,
    far_sem,
):
    sp, tp = lax.axis_index("sp"), lax.axis_index("tp")
    other = 1 - tp
    rows, half = x_ref.shape
    groups, state = rot_ref.shape
    gch = imap_ref.shape[1]
    chans = groups * gch
    states = groups * state
    prow = states // LANES
    per_block = LANES // gch
    blocks = groups // per_block
    quads = prow // blocks
    pitch = drv.shape[0] // rows
    bstates = quads * LANES
    cwide = taps_ref.shape[1]
    width = taps_ref.shape[0]

    barrier = pltpu.get_barrier_semaphore()
    partner = {"sp": sp, "tp": other}

    inner = inner_of(n)
    outer = n // inner
    a, b = lax.div(sp, inner), lax.rem(sp, inner)
    last = outer - 1

    def greet(j):
        pl.semaphore_signal(barrier, inc=1, device_id={"sp": j, "tp": 1}, device_id_type=MESH)

    def greet_far(k, c):
        greet(k * inner + b)
        return c

    @pl.when(tp == 1)
    def _():
        pl.semaphore_signal(barrier, inc=1, device_id=partner, device_id_type=MESH)

    for k in range(1, inner):
        greet(a * inner + lax.rem(b + k, inner))
    lax.fori_loop(0, a, greet_far, 0)

    @pl.when((b == 0) & (a > 0) & (inner > 1))
    def _():
        greet(sp - 1)

    in_copies = {}
    def fetch(i, src, dst):
        in_copies[i] = pltpu.make_async_copy(src, dst, in_sem.at[i])
        in_copies[i].start()

    w_hbm = (w0_hbm, w1_hbm, w2_hbm, w3_hbm)

    def fetch_weight(i, h, sem):
        part = (tp, other)[h]
        pltpu.make_async_copy(
            w_hbm[i].at[pl.ds(part * half, half), :], wv.at[i, pl.ds(h * half, half), :], sem
        ).start()

    def wait_weight(i):
        pltpu.make_async_copy(w_hbm[i], wv.at[i], wsem.at[i]).wait()

    fetch(0, x_hbm, x_ref)
    fetch(1, gain_hbm, gain_ref)
    fetch(2, rot_hbm, rot_ref)
    fetch(3, init_hbm, init_ref)
    fetch(4, ld_hbm, ld_ref)
    fetch(5, imap_hbm, imap_ref)
    fetch_weight(0, 0, wsem.at[0])
    fetch_weight(0, 1, wsem.at[4])
    fetch(6, omap_hbm, omap_ref)
    fetch(7, skip_hbm, skip_ref)
    fetch(8, taps_hbm, taps_ref)
    for i in (1, 3, 2):
        for h in (0, 1):
            fetch_weight(i, h, wsem.at[i])
    for i, w, deep in ((1, co_hbm, cwide), (0, so_hbm, chans)):
        for h, part in ((0, tp), (1, other)):
            pltpu.make_async_copy(
                w.at[pl.ds(part * deep, deep), :], ov.at[i, pl.ds(h * deep, deep), :], osem.at[i]
            ).start()

    @pl.when(tp == 0)
    def _():
        pl.semaphore_wait(barrier, 1)
        pl.semaphore_signal(near, inc=1, device_id=partner, device_id_type=MESH)

    @pl.when(tp == 1)
    def _():
        pl.semaphore_wait(near, 1)

    def remote(src, dst, s, r, dev):
        return pltpu.make_async_remote_copy(
            src_ref=src, dst_ref=dst, send_sem=s, recv_sem=r, device_id=dev, device_id_type=MESH
        )

    in_copies[0].wait()
    x_copy = remote(x_ref, xr, x_sem.at[0], x_sem.at[1], partner)
    x_copy.start()

    for i in range(2, 6):
        in_copies[i].wait()

    lane = lax.broadcasted_iota(jnp.int32, (1, LANES), 1)
    for i, v in enumerate((rot_ref[...], init_ref[0], init_ref[1])):
        pairs[pl.ds(i * groups, groups), :] = jnp.concatenate([v, v], axis=1)

    def paired(i):
        even = pairs[pl.ds(i * groups, prow, stride=2), :]
        odd = pairs[pl.ds(i * groups + 1, prow, stride=2), :]
        return jnp.where(lane < state, even, odd)

    theta = paired(0)
    cosv, sinv = jnp.cos(theta), jnp.sin(theta)
    whole = cpow((cosv, sinv), rows)

    def spread_map(src, dst):
        dst[...] = jnp.zeros_like(dst)
        for b in range(blocks):
            for q in range(quads):
                g = b * per_block + 2 * q
                one = src[g].astype(F32)
                two = src[g + 1].astype(F32)
                one_r = jnp.concatenate([one[:, state:], one[:, :state]], axis=1)
                two_r = jnp.concatenate([two[:, state:], two[:, :state]], axis=1)
                low = lane < state
                re = jnp.concatenate([jnp.where(low, one, 0.0), jnp.where(low, 0.0, two_r)], axis=0)
                im = jnp.concatenate([jnp.where(low, one_r, 0.0), jnp.where(low, 0.0, two)], axis=0)
                at = pl.ds(b * LANES + q * 2 * gch, 2 * gch)
                dst[at, q * LANES : (q + 1) * LANES] = re.astype(BF16)
                dst[at, bstates + q * LANES : bstates + (q + 1) * LANES] = im.astype(BF16)

    spread_map(imap_ref, bd_in)

    ld = ld_ref[...].T
    mags = split3(jnp.exp(ld))
    whole_mags = split3(jnp.exp(jnp.sum(ld, axis=0, keepdims=True)))
    gains = split3(jnp.sqrt(minus_expm1(2.0 * ld)))[:2]
    for blk in range(blocks):
        col = lax.broadcasted_iota(jnp.int32, (groups, bstates), 1) + blk * bstates
        row = lax.broadcasted_iota(jnp.int32, (groups, bstates), 0)
        spread = jnp.where(
            (col >= row * state) & (col < (row + 1) * state), 1.0, 0.0
        ).astype(BF16)

        def over(pieces):
            total = None
            for piece in pieces:
                d = jnp.dot(piece, spread, preferred_element_type=F32)
                total = d if total is None else total + d
            return total

        m = over(mags)
        for q in range(quads):
            mag[pl.ds(blk * quads + q, rows, stride=prow), :] = m[:, q * LANES : (q + 1) * LANES]
        m = over(whole_mags[:2])
        for q in range(quads):
            tot[blk * quads + q : blk * quads + q + 1, :] = m[:, q * LANES : (q + 1) * LANES]
        wide_w[:, blk * bstates : (blk + 1) * bstates] = over(gains)

    in_copies[1].wait()
    own = x_ref[...].astype(F32)
    scaled = (own * gain_ref[:, pl.ds(pl.multiple_of(tp * half, LANES), half)]).astype(BF16)
    squares = jnp.sum(own * own, axis=1, keepdims=True)
    half_copy = pltpu.make_async_copy(w_hbm[0].at[pl.ds(0, half), :], wv.at[0, pl.ds(0, half), :], wsem.at[0])
    half_copy.wait()
    partial = jnp.dot(scaled, wv[0, :half], preferred_element_type=F32)
    acc[:, :half] = scaled

    x_copy.wait_recv()
    far_x = xr[...].astype(F32)
    scaled_far = (far_x * gain_ref[:, pl.ds(pl.multiple_of(other * half, LANES), half)]).astype(BF16)
    squares = squares + jnp.sum(far_x * far_x, axis=1, keepdims=True)
    scale = lax.rsqrt(squares / (2 * half) + EPS)

    acc[:, half:] = scaled_far
    rest_copy = pltpu.make_async_copy(
        w_hbm[0].at[pl.ds(0, half), :], wv.at[0, pl.ds(half, half), :], wsem.at[4]
    )
    rest_copy.wait()
    total = partial + jnp.dot(scaled_far, wv[0, half:], preferred_element_type=F32)
    drive_in = (total * scale).astype(BF16)
    din[...] = drive_in
    for k in range(blocks):
        blk = jnp.dot(
            drive_in[:, k * LANES : (k + 1) * LANES],
            bd_in[k * LANES : (k + 1) * LANES, :],
            preferred_element_type=F32,
        )
        for q in range(quads):
            r = k * quads + q
            w = wide_w[:, r * LANES : (r + 1) * LANES]
            drv[pl.ds(r, rows, stride=pitch), :] = blk[:, q * LANES : (q + 1) * LANES] * w
            drv[pl.ds(prow + r, rows, stride=pitch), :] = (
                blk[:, bstates + q * LANES : bstates + (q + 1) * LANES] * w
            )

    def advance(t, h):
        m = mag[pl.ds(pl.multiple_of(t * prow, prow), prow), :]
        base = pl.multiple_of(t * pitch, 8)
        d_re = drv[pl.ds(base, prow), :]
        d_im = drv[pl.ds(base + prow, prow), :]
        f_re, f_im = m * cosv, m * sinv
        new_re = (f_re * h[0] + d_re) - f_im * h[1]
        new_im = (f_re * h[1] + d_im) + f_im * h[0]
        return base, (new_re, new_im)

    def first(t, c):
        base, h = advance(t, c)
        return h

    zero = jnp.zeros((prow, LANES), F32)
    e_re, e_im = lax.fori_loop(0, rows, first, (zero, zero), unroll=8)
    near_in[b, pl.ds(0, prow), :] = e_re.astype(BF16)
    near_in[b, pl.ds(prow, prow), :] = e_im.astype(BF16)
    own_hi, own_lo, _ = split3(tot[...])
    near_in[b, pl.ds(2 * prow, prow), :] = own_hi
    near_in[b, pl.ds(3 * prow, prow), :] = own_lo

    def near_copy(k):
        return remote(
            near_in.at[b], near_in.at[b], near_send.at[k], near_recv.at[b], {"sp": a * inner + k, "tp": tp}
        )

    def far_copy(k):
        return remote(
            far_out, far_in.at[a], far_send.at[k], far_recv.at[a], {"sp": k * inner + b, "tp": tp}
        )

    near_from = jnp.where(a < last, 0, b + 1)
    near_upto = jnp.where(a < last, inner, b)
    later = 2 * (inner - 1) + 2 * (last - a) + jnp.where((b == inner - 1) & (a < last) & (inner > 1), 2, 0)

    @pl.when((tp == 1) & (later > 0))
    def _():
        pl.semaphore_wait(barrier, later)
        pl.semaphore_signal(far_sem, inc=1, device_id=partner, device_id_type=MESH)

    @pl.when((tp == 0) & (later > 0))
    def _():
        pl.semaphore_wait(far_sem, 1)

    def send_near(k, c):
        @pl.when(k != b)
        def _():
            near_copy(k).start()

        return c

    lax.fori_loop(near_from, inner, send_near, 0)

    def project(i):
        wait_weight(i)
        total = jnp.dot(acc[...], wv[i], preferred_element_type=F32)
        return (total * scale).astype(BF16)

    value = project(1)
    pre_gate = project(3)
    mixed = (pre_gate.astype(F32) * value.astype(F32)).astype(BF16).astype(F32)
    pad[pl.ds(8, rows), :] = mixed
    tail_copy = remote(
        pad.at[pl.ds(rows, 8), :],
        pad.at[pl.ds(0, 8), :],
        tail_sem.at[0],
        tail_sem.at[1],
        {"sp": lax.rem(sp + 1, n), "tp": tp},
    )

    @pl.when(sp < n - 1)
    def _():
        tail_copy.start()

    hc[0] = project(2)

    for i in (6, 7):
        in_copies[i].wait()
    spread_map(omap_ref, bd_out)

    def near_step(k, c):
        @pl.when(k != b)
        def _():
            remote(
                near_in.at[k], near_in.at[k], near_send.at[k], near_recv.at[k], {"sp": a * inner + k, "tp": tp}
            ).wait_recv()

        ends, mag_all, turn, mine = c[0:2], c[2], c[3:5], c[5:]
        k_mag = near_in[k, pl.ds(2 * prow, prow), :].astype(F32) + near_in[
            k, pl.ds(3 * prow, prow), :
        ].astype(F32)
        moved = cmul((whole[0] * k_mag, whole[1] * k_mag), ends)
        now = (
            moved[0] + near_in[k, pl.ds(0, prow), :].astype(F32),
            moved[1] + near_in[k, pl.ds(prow, prow), :].astype(F32),
            mag_all * k_mag,
        ) + cmul(whole, turn)
        return now + tuple(jnp.where(k < b, v, w) for v, w in zip(now, mine))

    one = jnp.ones((prow, LANES), F32)
    begin = tuple(jnp.where(a == 0, v, zero) for v in (paired(1), paired(2))) + (one, one, zero)
    plane = lax.fori_loop(0, near_upto, near_step, begin + begin)

    def send_far(k, c):
        far_copy(k).start()
        return c

    @pl.when(a < last)
    def _():
        far_out[pl.ds(0, prow), :] = plane[0].astype(BF16)
        far_out[pl.ds(prow, prow), :] = plane[1].astype(BF16)
        all_hi, all_lo, _ = split3(plane[2])
        far_out[pl.ds(2 * prow, prow), :] = all_hi
        far_out[pl.ds(3 * prow, prow), :] = all_lo
        lax.fori_loop(a + 1, outer, send_far, 0)

    @pl.when(sp == 0)
    def _():
        pad[pl.ds(0, 8), :] = jnp.zeros((8, cwide), F32)

    in_copies[8].wait()

    @pl.when(sp > 0)
    def _():
        tail_copy.wait_recv()

    conv = jnp.zeros((rows, cwide), F32)
    for k in range(width):
        conv = conv + pad[pl.ds(8 + k - (width - 1), rows), :] * taps_ref[k : k + 1, :].astype(F32)
    hc[0] = (hc[0].astype(F32) * conv).astype(BF16)
    hc_copy = remote(hc.at[0], hc.at[1], hc_sem.at[0], hc_sem.at[1], partner)
    hc_copy.start()
    for i in (0, 1):
        pltpu.make_async_copy((so_hbm, co_hbm)[i], ov.at[i], osem.at[i]).wait()
    oacc[...] = jnp.dot(hc[0], ov[1, :cwide], preferred_element_type=F32)
    hc_copy.wait_recv()
    oacc[...] += jnp.dot(hc[1], ov[1, cwide:], preferred_element_type=F32)

    whole_plane = cpow(whole, inner)

    def far_step(k, h):
        remote(
            far_out, far_in.at[k], far_send.at[k], far_recv.at[k], {"sp": k * inner + b, "tp": tp}
        ).wait_recv()
        k_mag = far_in[k, pl.ds(2 * prow, prow), :].astype(F32) + far_in[
            k, pl.ds(3 * prow, prow), :
        ].astype(F32)
        moved = cmul((whole_plane[0] * k_mag, whole_plane[1] * k_mag), h)
        k_re = far_in[k, pl.ds(0, prow), :].astype(F32)
        k_im = far_in[k, pl.ds(prow, prow), :].astype(F32)
        return moved[0] + k_re, moved[1] + k_im

    before = lax.fori_loop(0, a, far_step, (zero, zero))
    mine = plane[5:]
    moved = cmul((mine[3] * mine[2], mine[4] * mine[2]), before)
    enter = (mine[0] + moved[0], mine[1] + moved[1])

    def second(t, c):
        base, h = advance(t, c)
        drv[pl.ds(base, prow), :] = h[0]
        drv[pl.ds(base + prow, prow), :] = h[1]
        return h

    lax.fori_loop(0, rows, second, enter, unroll=8)

    hs_copies = []
    for k in range(blocks):
        at = [k * quads + q for q in range(quads)]
        at = at + [prow + r for r in at]
        cols = slice(k * LANES, (k + 1) * LANES)
        st = jnp.concatenate(
            [drv[pl.ds(r, rows, stride=pitch), :].astype(BF16) for r in at], axis=1
        )
        read = lax.dot_general(
            st, bd_out[cols, :], (((1,), (1,)), ((), ())), preferred_element_type=F32
        )
        hs[0, :, cols] = gelu(read + skip_ref[:, cols] * din[:, cols].astype(F32)).astype(BF16)
        if k % 2 == 1:
            two = pl.ds((k - 1) * LANES, 2 * LANES)
            copy = remote(
                hs.at[0, :, two], hs.at[1, :, two], hs_sem.at[0, k // 2], hs_sem.at[1, k // 2], partner
            )
            copy.start()
            hs_copies.append(copy)
    oacc[...] += jnp.dot(hs[0], ov[0, :chans], preferred_element_type=F32)
    for copy in hs_copies:
        copy.wait_recv()
    out_ref[...] = (oacc[...] + jnp.dot(hs[1], ov[0, chans:], preferred_element_type=F32)).astype(BF16)

    x_copy.wait_send()
    hc_copy.wait_send()
    for copy in hs_copies:
        copy.wait_send()

    @pl.when(sp < n - 1)
    def _():
        tail_copy.wait_send()

    def near_sent(k, c):
        @pl.when(k != b)
        def _():
            near_copy(k).wait_send()

        return c

    def far_sent(k, c):
        far_copy(k).wait_send()
        return c

    lax.fori_loop(near_from, inner, near_sent, 0)
    lax.fori_loop(a + 1, outer, far_sent, 0)


def on_device(
    activations,
    norm_gain,
    state_proj,
    value_proj,
    post_gate_proj,
    pre_gate_proj,
    input_map,
    output_map,
    skip_gain,
    rotation,
    log_decay,
    initial_state,
    conv_taps,
    state_out,
    conv_out,
):
    n = lax.axis_size("sp")
    rows, half = activations.shape
    groups, state = rotation.shape
    chans = state_proj.shape[1]
    cwide = value_proj.shape[1]
    outs = state_out.shape[1]
    states = groups * state
    prow = states // LANES
    inner = inner_of(n)
    bdw = 2 * states // (chans // LANES)
    vmem = pl.BlockSpec(memory_space=pltpu.VMEM)
    hbm = pl.BlockSpec(memory_space=pl.ANY)
    dma = pltpu.SemaphoreType.DMA
    return pl.pallas_call(
        functools.partial(kernel, n),
        out_shape=pltpu.VMEM((rows, outs), BF16),
        in_specs=[hbm] * 15,
        out_specs=vmem,
        scratch_shapes=[
            pltpu.VMEM((rows, half), BF16),
            pltpu.VMEM((1, 2 * half), F32),
            pltpu.VMEM(input_map.shape, BF16),
            pltpu.VMEM((groups, output_map.shape[2], output_map.shape[1]), F32),
            pltpu.VMEM((1, chans), F32),
            pltpu.VMEM((groups, state), F32),
            pltpu.VMEM((groups, rows), F32),
            pltpu.VMEM(initial_state.shape, F32),
            pltpu.VMEM(conv_taps.shape, BF16),
            pltpu.VMEM((4, 2 * half, chans), BF16),
            pltpu.VMEM((2, 2 * chans, outs), BF16),
            pltpu.VMEM((rows, half), BF16),
            pltpu.VMEM((rows, 2 * half), BF16),
            pltpu.VMEM((rows, chans), BF16),
            pltpu.VMEM((chans, bdw), BF16),
            pltpu.VMEM((chans, bdw), BF16),
            pltpu.VMEM((rows, states), F32),
            pltpu.VMEM((rows * prow, LANES), F32),
            pltpu.VMEM((rows * (2 * prow + 8), LANES), F32),
            pltpu.VMEM((3 * groups, LANES), F32),
            pltpu.VMEM((rows + 8, cwide), F32),
            pltpu.VMEM((prow, LANES), F32),
            pltpu.VMEM((inner, 4 * prow, LANES), BF16),
            pltpu.VMEM((n // inner, 4 * prow, LANES), BF16),
            pltpu.VMEM((4 * prow, LANES), BF16),
            pltpu.VMEM((2, rows, chans), BF16),
            pltpu.VMEM((2, rows, cwide), BF16),
            pltpu.VMEM((rows, outs), F32),
            dma((9,)),
            dma((5,)),
            dma((2,)),
            dma((2,)),
            dma((2,)),
            dma((2,)),
            dma((2, chans // (2 * LANES))),
            dma((inner,)),
            dma((inner,)),
            dma((n // inner,)),
            dma((n // inner,)),
            pltpu.SemaphoreType.REGULAR,
            pltpu.SemaphoreType.REGULAR,
        ],
        compiler_params=pltpu.CompilerParams(collective_id=0, has_side_effects=True),
    )(
        activations,
        norm_gain.reshape(1, -1),
        state_proj,
        value_proj,
        post_gate_proj,
        pre_gate_proj,
        input_map,
        jnp.swapaxes(output_map, 1, 2),
        skip_gain.reshape(1, -1),
        rotation,
        jnp.swapaxes(log_decay, 0, 1),
        initial_state,
        conv_taps,
        state_out,
        conv_out,
    )


def solution(mesh):
    return jax.shard_map(
        on_device,
        mesh=mesh,
        in_specs=(
            P("sp", "tp"),
            P(),
            P(None, "tp"),
            P(None, "tp"),
            P(None, "tp"),
            P(None, "tp"),
            P("tp", None, None),
            P("tp", None, None),
            P("tp"),
            P("tp", None),
            P("sp", "tp"),
            P(None, "tp", None),
            P(None, "tp"),
            P(None, "tp"),
            P(None, "tp"),
        ),
        out_specs=P("sp", "tp"),
        check_vma=False,
    )
```

```python
import functools

import jax
import jax.numpy as jnp
from jax import lax
from jax.experimental import pallas as pl
from jax.experimental.pallas import tpu as pltpu
from jax.sharding import PartitionSpec as P

EPS = 1e-06
LANES = 128
MESH = pl.DeviceIdType.MESH
F32 = jnp.float32
BF16 = jnp.bfloat16


def minus_expm1(y):
    poly = jnp.ones_like(y)
    for k in range(11, 1, -1):
        poly = 1.0 + poly * y * (1.0 / k)
    return jnp.where(y > -0.5, -y * poly, 1.0 - jnp.exp(y))


def split3(v):
    hi = v.astype(BF16)
    rest = v - hi.astype(F32)
    mid = rest.astype(BF16)
    low = (rest - mid.astype(F32)).astype(BF16)
    return hi, mid, low


def cmul(a, b):
    return a[0] * b[0] - a[1] * b[1], a[0] * b[1] + a[1] * b[0]


def cpow(base, count):
    result = None
    while count:
        if count & 1:
            result = base if result is None else cmul(result, base)
        count >>= 1
        if count:
            base = cmul(base, base)
    return result


def inner_of(n):
    return max(d for d in range(1, n + 1) if n % d == 0 and d * d <= n)


def gelu(x):
    return 0.5 * x * (1.0 + jnp.tanh(0.7978845608028654 * (x + 0.044715 * x * x * x)))


def kernel(
    n,
    x_hbm,
    gain_hbm,
    w0_hbm,
    w1_hbm,
    w2_hbm,
    w3_hbm,
    imap_hbm,
    omap_hbm,
    skip_hbm,
    rot_hbm,
    ld_hbm,
    init_hbm,
    taps_hbm,
    so_hbm,
    co_hbm,
    out_ref,
    x_ref,
    gain_ref,
    imap_ref,
    omap_ref,
    skip_ref,
    rot_ref,
    ld_ref,
    init_ref,
    taps_ref,
    wv,
    ov,
    xr,
    acc,
    din,
    bd_in,
    bd_out,
    coef,
    tbl,
    powers,
    chan_d,
    chan_end,
    chan_gain,
    rowed,
    pre,
    mag,
    drv,
    pairs,
    pad,
    near_in,
    far_in,
    far_out,
    hs,
    hc,
    oacc,
    in_sem,
    wsem,
    osem,
    x_sem,
    tail_sem,
    hc_sem,
    hs_sem,
    near_send,
    near_recv,
    far_send,
    far_recv,
    near,
    far_sem,
):
    sp, tp = lax.axis_index("sp"), lax.axis_index("tp")
    other = 1 - tp
    rows, half = x_ref.shape
    groups, state = rot_ref.shape
    gch = imap_ref.shape[1]
    chans = groups * gch
    states = groups * state
    prow = states // LANES
    per_block = LANES // gch
    blocks = groups // per_block
    quads = prow // blocks
    pitch = drv.shape[0] // rows
    bstates = quads * LANES
    cwide = taps_ref.shape[1]
    width = taps_ref.shape[0]

    barrier = pltpu.get_barrier_semaphore()
    partner = {"sp": sp, "tp": other}

    inner = inner_of(n)
    outer = n // inner
    a, b = lax.div(sp, inner), lax.rem(sp, inner)
    last = outer - 1

    def greet(j):
        pl.semaphore_signal(barrier, inc=1, device_id={"sp": j, "tp": 1}, device_id_type=MESH)

    def greet_far(k, c):
        greet(k * inner + b)
        return c

    @pl.when(tp == 1)
    def _():
        pl.semaphore_signal(barrier, inc=1, device_id=partner, device_id_type=MESH)

    for k in range(1, inner):
        greet(a * inner + lax.rem(b + k, inner))
    lax.fori_loop(0, a, greet_far, 0)

    @pl.when((b == 0) & (a > 0) & (inner > 1))
    def _():
        greet(sp - 1)

    in_copies = {}
    def fetch(i, src, dst):
        in_copies[i] = pltpu.make_async_copy(src, dst, in_sem.at[i])
        in_copies[i].start()

    w_hbm = (w0_hbm, w1_hbm, w2_hbm, w3_hbm)

    def fetch_weight(i, h, sem):
        part = (tp, other)[h]
        pltpu.make_async_copy(
            w_hbm[i].at[pl.ds(part * half, half), :], wv.at[i, pl.ds(h * half, half), :], sem
        ).start()

    def wait_weight(i):
        pltpu.make_async_copy(w_hbm[i], wv.at[i], wsem.at[i]).wait()

    fetch(0, x_hbm, x_ref)
    fetch(4, ld_hbm, ld_ref)
    fetch(2, rot_hbm, rot_ref)
    fetch(1, gain_hbm, gain_ref)
    fetch(5, imap_hbm, imap_ref)
    fetch_weight(0, 0, wsem.at[0])
    fetch_weight(0, 1, wsem.at[4])

    @pl.when(tp == 0)
    def _():
        pl.semaphore_wait(barrier, 1)
        pl.semaphore_signal(near, inc=1, device_id=partner, device_id_type=MESH)

    @pl.when(tp == 1)
    def _():
        pl.semaphore_wait(near, 1)

    def remote(src, dst, s, r, dev):
        return pltpu.make_async_remote_copy(
            src_ref=src, dst_ref=dst, send_sem=s, recv_sem=r, device_id=dev, device_id_type=MESH
        )

    in_copies[0].wait()
    x_copy = remote(x_ref, xr, x_sem.at[0], x_sem.at[1], partner)
    x_copy.start()

    fetch(3, init_hbm, init_ref)
    fetch(6, omap_hbm, omap_ref)
    fetch(7, skip_hbm, skip_ref)
    fetch(8, taps_hbm, taps_ref)
    for i in (1, 3, 2):
        for h in (0, 1):
            fetch_weight(i, h, wsem.at[i])
    for i, w, deep in ((1, co_hbm, cwide), (0, so_hbm, chans)):
        for h, part in ((0, tp), (1, other)):
            pltpu.make_async_copy(
                w.at[pl.ds(part * deep, deep), :], ov.at[i, pl.ds(h * deep, deep), :], osem.at[i]
            ).start()

    lane = lax.broadcasted_iota(jnp.int32, (1, LANES), 1)

    def pair_up(i, v):
        pairs[pl.ds(i * groups, groups), :] = v
        even = pairs[pl.ds(i * groups, prow, stride=2), :]
        odd = pairs[pl.ds(i * groups + 1, prow, stride=2), :]
        return jnp.where(lane < state, even, odd)

    def twice(v):
        return jnp.concatenate([v, v], axis=1)

    in_copies[2].wait()
    theta = pair_up(0, twice(rot_ref[...]))
    turn = jnp.cos(theta), jnp.sin(theta)
    step = turn
    for k in range(8):
        for i in (0, 1):
            powers[i, pl.ds(k * prow, prow), :] = step[i]
        step = cmul(step, turn) if k < 7 else step
    far_step16 = cmul(step, step)
    for i in (0, 1):
        powers[i, pl.ds(8 * prow, prow), :] = far_step16[i]
    whole = cpow(step, rows // 8)
    for r in range(prow):
        even = [powers[i, pl.ds(r, 8, stride=prow), :] for i in (0, 1)]
        eight = [powers[i, pl.ds(7 * prow + r, 1), :] for i in (0, 1)]
        sixteen = [powers[i, pl.ds(8 * prow + r, 1), :] for i in (0, 1)]
        odd = cmul(even, eight)
        for t in range(0, rows, 16):
            for i in (0, 1):
                tbl[t : t + 16, (2 * r + i) * LANES : (2 * r + i + 1) * LANES] = jnp.concatenate(
                    [even[i], odd[i]], axis=0
                ).astype(BF16)
            even = cmul(even, sixteen)
            odd = cmul(odd, sixteen)

    in_copies[4].wait()
    ld = ld_ref[...]
    when = lax.broadcasted_iota(jnp.int32, (rows, 2 * rows), 0)
    upto = lax.broadcasted_iota(jnp.int32, (rows, 2 * rows), 1)
    sums = jnp.where(
        ((upto < rows) & (when <= upto)) | ((upto >= rows) & (when > upto - rows)), 1.0, 0.0
    ).astype(BF16)
    added = jnp.dot(jnp.concatenate(split3(ld), axis=0), sums, preferred_element_type=F32)
    added = added[:groups] + added[groups : 2 * groups] + added[2 * groups :]
    gain = jnp.sqrt(minus_expm1(2.0 * ld))
    decays = jnp.exp(added)
    per_group = jnp.concatenate([decays[:, :rows], gain * decays[:, rows:], gain], axis=1).T
    col = lax.broadcasted_iota(jnp.int32, (groups, chans), 1)
    row = lax.broadcasted_iota(jnp.int32, (groups, chans), 0)
    to_chan = jnp.where((col >= row * gch) & (col < (row + 1) * gch), 1.0, 0.0).astype(BF16)
    hi, mid, _ = split3(per_group)
    wide = jnp.dot(hi, to_chan, preferred_element_type=F32) + jnp.dot(
        mid, to_chan, preferred_element_type=F32
    )
    chan_d[...] = wide[:rows]
    chan_end[...] = wide[rows : 2 * rows]
    chan_gain[...] = wide[2 * rows :]
    tot = pair_up(
        3, jnp.broadcast_to(jnp.exp(jnp.sum(ld, axis=1, keepdims=True)), (groups, LANES))
    )

    def spread_map(src, dst):
        dst[...] = jnp.zeros_like(dst)
        for b in range(blocks):
            for q in range(quads):
                g = b * per_block + 2 * q
                one = src[g].astype(F32)
                two = src[g + 1].astype(F32)
                one_r = jnp.concatenate([one[:, state:], one[:, :state]], axis=1)
                two_r = jnp.concatenate([two[:, state:], two[:, :state]], axis=1)
                low = lane < state
                re = jnp.concatenate([jnp.where(low, one, 0.0), jnp.where(low, 0.0, two_r)], axis=0)
                im = jnp.concatenate([jnp.where(low, one_r, 0.0), jnp.where(low, 0.0, two)], axis=0)
                at = pl.ds(b * LANES + q * 2 * gch, 2 * gch)
                dst[at, 2 * q * LANES : (2 * q + 1) * LANES] = re.astype(BF16)
                dst[at, (2 * q + 1) * LANES : (2 * q + 2) * LANES] = im.astype(BF16)

    in_copies[1].wait()
    own = x_ref[...].astype(F32)
    scaled = (own * gain_ref[:, pl.ds(pl.multiple_of(tp * half, LANES), half)]).astype(BF16)
    squares = jnp.sum(own * own, axis=1, keepdims=True)
    half_copy = pltpu.make_async_copy(w_hbm[0].at[pl.ds(0, half), :], wv.at[0, pl.ds(0, half), :], wsem.at[0])
    half_copy.wait()
    partial = jnp.dot(scaled, wv[0, :half], preferred_element_type=F32)
    acc[:, :half] = scaled
    in_copies[5].wait()
    spread_map(imap_ref, bd_in)

    x_copy.wait_recv()
    far_x = xr[...].astype(F32)
    scaled_far = (far_x * gain_ref[:, pl.ds(pl.multiple_of(other * half, LANES), half)]).astype(BF16)
    squares = squares + jnp.sum(far_x * far_x, axis=1, keepdims=True)
    scale = lax.rsqrt(squares / (2 * half) + EPS)

    acc[:, half:] = scaled_far
    rest_copy = pltpu.make_async_copy(
        w_hbm[0].at[pl.ds(0, half), :], wv.at[0, pl.ds(half, half), :], wsem.at[4]
    )
    rest_copy.wait()
    total = partial + jnp.dot(scaled_far, wv[0, half:], preferred_element_type=F32)
    drive_in = (total * scale).astype(BF16)
    din[...] = drive_in
    ends_in = (drive_in.astype(F32) * chan_end[...]).astype(BF16).T
    for r in range(prow):
        q = r % quads
        at = slice(r * 2 * gch, (r + 1) * 2 * gch)
        seen = jnp.dot(
            ends_in[at], tbl[:, 2 * r * LANES : (2 * r + 2) * LANES], preferred_element_type=F32
        )
        m_re = bd_in[at, 2 * q * LANES : (2 * q + 1) * LANES].astype(F32)
        m_im = bd_in[at, (2 * q + 1) * LANES : (2 * q + 2) * LANES].astype(F32)
        c, d = seen[:, :LANES], seen[:, LANES:]
        rowed[0, r : r + 1, :] = jnp.sum(c * m_re + d * m_im, axis=0, keepdims=True)
        rowed[1, r : r + 1, :] = jnp.sum(c * m_im - d * m_re, axis=0, keepdims=True)
    e_re, e_im = cmul(whole, (rowed[0], rowed[1]))

    near_in[b, pl.ds(0, prow), :] = e_re.astype(BF16)
    near_in[b, pl.ds(prow, prow), :] = e_im.astype(BF16)
    own_hi, own_lo, _ = split3(tot)
    near_in[b, pl.ds(2 * prow, prow), :] = own_hi
    near_in[b, pl.ds(3 * prow, prow), :] = own_lo

    def near_copy(k):
        return remote(
            near_in.at[b], near_in.at[b], near_send.at[k], near_recv.at[b], {"sp": a * inner + k, "tp": tp}
        )

    def far_copy(k):
        return remote(
            far_out, far_in.at[a], far_send.at[k], far_recv.at[a], {"sp": k * inner + b, "tp": tp}
        )

    near_from = jnp.where(a < last, 0, b + 1)
    near_upto = jnp.where(a < last, inner, b)
    later = 2 * (inner - 1) + 2 * (last - a) + jnp.where((b == inner - 1) & (a < last) & (inner > 1), 2, 0)

    @pl.when((tp == 1) & (later > 0))
    def _():
        pl.semaphore_wait(barrier, later)
        pl.semaphore_signal(far_sem, inc=1, device_id=partner, device_id_type=MESH)

    @pl.when((tp == 0) & (later > 0))
    def _():
        pl.semaphore_wait(far_sem, 1)

    def send_near(k, c):
        @pl.when(k != b)
        def _():
            near_copy(k).start()

        return c

    lax.fori_loop(near_from, inner, send_near, 0)

    def project(i):
        wait_weight(i)
        total = jnp.dot(acc[...], wv[i], preferred_element_type=F32)
        return (total * scale).astype(BF16)

    value = project(1)
    pre_gate = project(3)
    mixed = (pre_gate.astype(F32) * value.astype(F32)).astype(BF16).astype(F32)
    pad[pl.ds(8, rows), :] = mixed
    tail_copy = remote(
        pad.at[pl.ds(rows, 8), :],
        pad.at[pl.ds(0, 8), :],
        tail_sem.at[0],
        tail_sem.at[1],
        {"sp": lax.rem(sp + 1, n), "tp": tp},
    )

    @pl.when(sp < n - 1)
    def _():
        tail_copy.start()

    hc[0] = project(2)

    for i in (6, 7):
        in_copies[i].wait()
    spread_map(omap_ref, bd_out)

    mags = split3(jnp.exp(ld_ref[...]).T)[:2]
    for k in range(blocks):
        col = lax.broadcasted_iota(jnp.int32, (groups, bstates), 1) + k * bstates
        row = lax.broadcasted_iota(jnp.int32, (groups, bstates), 0)
        spread = jnp.where(
            (col >= row * state) & (col < (row + 1) * state), 1.0, 0.0
        ).astype(BF16)
        m = jnp.dot(mags[0], spread, preferred_element_type=F32) + jnp.dot(
            mags[1], spread, preferred_element_type=F32
        )
        for q in range(quads):
            mag[pl.ds(k * quads + q, rows, stride=prow), :] = m[:, q * LANES : (q + 1) * LANES]

    gained = (din[...].astype(F32) * chan_gain[...]).astype(BF16)
    for k in range(blocks):
        blk = jnp.dot(
            gained[:, k * LANES : (k + 1) * LANES],
            bd_in[k * LANES : (k + 1) * LANES, :],
            preferred_element_type=F32,
        )
        for q in range(quads):
            r = k * quads + q
            drv[pl.ds(r, rows, stride=pitch), :] = blk[:, 2 * q * LANES : (2 * q + 1) * LANES]
            drv[pl.ds(prow + r, rows, stride=pitch), :] = blk[
                :, (2 * q + 1) * LANES : (2 * q + 2) * LANES
            ]

    def scan(t, h):
        m = mag[pl.ds(pl.multiple_of(t * prow, prow), prow), :]
        base = pl.multiple_of(t * pitch, 8)
        d_re = drv[pl.ds(base, prow), :]
        d_im = drv[pl.ds(base + prow, prow), :]
        f_re, f_im = m * turn[0], m * turn[1]
        new_re = (f_re * h[0] + d_re) - f_im * h[1]
        new_im = (f_re * h[1] + d_im) + f_im * h[0]
        drv[pl.ds(base, prow), :] = new_re
        drv[pl.ds(base + prow, prow), :] = new_im
        return new_re, new_im

    zero = jnp.zeros((prow, LANES), F32)
    lax.fori_loop(0, rows, scan, (zero, zero), unroll=8)
    for k in range(blocks):
        cols = slice(k * LANES, (k + 1) * LANES)
        at = [half_row + k * quads + q for q in range(quads) for half_row in (0, prow)]
        st = jnp.concatenate(
            [drv[pl.ds(r, rows, stride=pitch), :].astype(BF16) for r in at], axis=1
        )
        read = lax.dot_general(
            st, bd_out[cols, :], (((1,), (1,)), ((), ())), preferred_element_type=F32
        )
        pre[:, cols] = read + skip_ref[:, cols] * din[:, cols].astype(F32)
    coef[...] = jnp.zeros_like(coef)

    in_copies[3].wait()
    first = pair_up(1, twice(init_ref[0])), pair_up(2, twice(init_ref[1]))

    def near_step(k, c):
        @pl.when(k != b)
        def _():
            remote(
                near_in.at[k], near_in.at[k], near_send.at[k], near_recv.at[k], {"sp": a * inner + k, "tp": tp}
            ).wait_recv()

        ends, mag_all, phase, mine = c[0:2], c[2], c[3:5], c[5:]
        k_mag = near_in[k, pl.ds(2 * prow, prow), :].astype(F32) + near_in[
            k, pl.ds(3 * prow, prow), :
        ].astype(F32)
        moved = cmul((whole[0] * k_mag, whole[1] * k_mag), ends)
        now = (
            moved[0] + near_in[k, pl.ds(0, prow), :].astype(F32),
            moved[1] + near_in[k, pl.ds(prow, prow), :].astype(F32),
            mag_all * k_mag,
        ) + cmul(whole, phase)
        return now + tuple(jnp.where(k < b, v, w) for v, w in zip(now, mine))

    one = jnp.ones((prow, LANES), F32)
    begin = tuple(jnp.where(a == 0, v, zero) for v in first) + (one, one, zero)
    plane = lax.fori_loop(0, near_upto, near_step, begin + begin)

    def send_far(k, c):
        far_copy(k).start()
        return c

    @pl.when(a < last)
    def _():
        far_out[pl.ds(0, prow), :] = plane[0].astype(BF16)
        far_out[pl.ds(prow, prow), :] = plane[1].astype(BF16)
        all_hi, all_lo, _ = split3(plane[2])
        far_out[pl.ds(2 * prow, prow), :] = all_hi
        far_out[pl.ds(3 * prow, prow), :] = all_lo
        lax.fori_loop(a + 1, outer, send_far, 0)

    @pl.when(sp == 0)
    def _():
        pad[pl.ds(0, 8), :] = jnp.zeros((8, cwide), F32)

    in_copies[8].wait()

    @pl.when(sp > 0)
    def _():
        tail_copy.wait_recv()

    conv = jnp.zeros((rows, cwide), F32)
    for k in range(width):
        conv = conv + pad[pl.ds(8 + k - (width - 1), rows), :] * taps_ref[k : k + 1, :].astype(F32)
    hc[0] = (hc[0].astype(F32) * conv).astype(BF16)
    hc_copy = remote(hc.at[0], hc.at[1], hc_sem.at[0], hc_sem.at[1], partner)
    hc_copy.start()
    for i in (0, 1):
        pltpu.make_async_copy((so_hbm, co_hbm)[i], ov.at[i], osem.at[i]).wait()
    oacc[...] = jnp.dot(hc[0], ov[1, :cwide], preferred_element_type=F32)
    whole_plane = cpow(whole, inner)

    def far_step(k, h):
        remote(
            far_out, far_in.at[k], far_send.at[k], far_recv.at[k], {"sp": k * inner + b, "tp": tp}
        ).wait_recv()
        k_mag = far_in[k, pl.ds(2 * prow, prow), :].astype(F32) + far_in[
            k, pl.ds(3 * prow, prow), :
        ].astype(F32)
        moved = cmul((whole_plane[0] * k_mag, whole_plane[1] * k_mag), h)
        k_re = far_in[k, pl.ds(0, prow), :].astype(F32)
        k_im = far_in[k, pl.ds(prow, prow), :].astype(F32)
        return moved[0] + k_re, moved[1] + k_im

    before = lax.fori_loop(0, a, far_step, (zero, zero))
    mine = plane[5:]
    moved = cmul((mine[3] * mine[2], mine[4] * mine[2]), before)
    enter = (mine[0] + moved[0], mine[1] + moved[1])

    rowed[0] = enter[0]
    rowed[1] = enter[1]
    hs_copies = []
    for k in range(blocks):
        cols = slice(k * LANES, (k + 1) * LANES)
        for q in range(quads):
            r = k * quads + q
            at = slice(r * 2 * gch, (r + 1) * 2 * gch)
            left = slice(2 * q * LANES, (2 * q + 1) * LANES)
            right = slice((2 * q + 1) * LANES, (2 * q + 2) * LANES)
            h_re, h_im = rowed[0, r : r + 1, :], rowed[1, r : r + 1, :]
            o_re, o_im = bd_out[at, left].astype(F32), bd_out[at, right].astype(F32)
            coef[at, left] = (h_re * o_re + h_im * o_im).astype(BF16)
            coef[at, right] = (h_re * o_im - h_im * o_re).astype(BF16)
        moved = lax.dot_general(
            tbl[:, 2 * k * bstates : 2 * (k + 1) * bstates],
            coef[cols, :],
            (((1,), (1,)), ((), ())),
            preferred_element_type=F32,
        )
        hs[0, :, cols] = gelu(pre[:, cols] + chan_d[:, cols] * moved).astype(BF16)
        if k % 2 == 1:
            two = pl.ds((k - 1) * LANES, 2 * LANES)
            copy = remote(
                hs.at[0, :, two], hs.at[1, :, two], hs_sem.at[0, k // 2], hs_sem.at[1, k // 2], partner
            )
            copy.start()
            hs_copies.append(copy)
    oacc[...] += jnp.dot(hs[0], ov[0, :chans], preferred_element_type=F32)
    hc_copy.wait_recv()
    oacc[...] += jnp.dot(hc[1], ov[1, cwide:], preferred_element_type=F32)
    for copy in hs_copies:
        copy.wait_recv()
    out_ref[...] = (oacc[...] + jnp.dot(hs[1], ov[0, chans:], preferred_element_type=F32)).astype(BF16)

    x_copy.wait_send()
    hc_copy.wait_send()
    for copy in hs_copies:
        copy.wait_send()

    @pl.when(sp < n - 1)
    def _():
        tail_copy.wait_send()

    def near_sent(k, c):
        @pl.when(k != b)
        def _():
            near_copy(k).wait_send()

        return c

    def far_sent(k, c):
        far_copy(k).wait_send()
        return c

    lax.fori_loop(near_from, inner, near_sent, 0)
    lax.fori_loop(a + 1, outer, far_sent, 0)


def on_device(
    activations,
    norm_gain,
    state_proj,
    value_proj,
    post_gate_proj,
    pre_gate_proj,
    input_map,
    output_map,
    skip_gain,
    rotation,
    log_decay,
    initial_state,
    conv_taps,
    state_out,
    conv_out,
):
    n = lax.axis_size("sp")
    rows, half = activations.shape
    groups, state = rotation.shape
    chans = state_proj.shape[1]
    cwide = value_proj.shape[1]
    outs = state_out.shape[1]
    states = groups * state
    prow = states // LANES
    inner = inner_of(n)
    bdw = 2 * states // (chans // LANES)
    vmem = pl.BlockSpec(memory_space=pltpu.VMEM)
    hbm = pl.BlockSpec(memory_space=pl.ANY)
    dma = pltpu.SemaphoreType.DMA
    return pl.pallas_call(
        functools.partial(kernel, n),
        out_shape=pltpu.VMEM((rows, outs), BF16),
        in_specs=[hbm] * 15,
        out_specs=vmem,
        scratch_shapes=[
            pltpu.VMEM((rows, half), BF16),
            pltpu.VMEM((1, 2 * half), F32),
            pltpu.VMEM(input_map.shape, BF16),
            pltpu.VMEM((groups, output_map.shape[2], output_map.shape[1]), F32),
            pltpu.VMEM((1, chans), F32),
            pltpu.VMEM((groups, state), F32),
            pltpu.VMEM((groups, rows), F32),
            pltpu.VMEM(initial_state.shape, F32),
            pltpu.VMEM(conv_taps.shape, BF16),
            pltpu.VMEM((4, 2 * half, chans), BF16),
            pltpu.VMEM((2, 2 * chans, outs), BF16),
            pltpu.VMEM((rows, half), BF16),
            pltpu.VMEM((rows, 2 * half), BF16),
            pltpu.VMEM((rows, chans), BF16),
            pltpu.VMEM((chans, bdw), BF16),
            pltpu.VMEM((chans, bdw), BF16),
            pltpu.VMEM((chans, bdw), BF16),
            pltpu.VMEM((rows, 2 * states), BF16),
            pltpu.VMEM((2, 9 * prow, LANES), F32),
            pltpu.VMEM((rows, chans), F32),
            pltpu.VMEM((rows, chans), F32),
            pltpu.VMEM((rows, chans), F32),
            pltpu.VMEM((2, prow, LANES), F32),
            pltpu.VMEM((rows, chans), F32),
            pltpu.VMEM((rows * prow, LANES), F32),
            pltpu.VMEM((rows * (2 * prow + 8), LANES), F32),
            pltpu.VMEM((4 * groups, LANES), F32),
            pltpu.VMEM((rows + 8, cwide), F32),
            pltpu.VMEM((inner, 4 * prow, LANES), BF16),
            pltpu.VMEM((n // inner, 4 * prow, LANES), BF16),
            pltpu.VMEM((4 * prow, LANES), BF16),
            pltpu.VMEM((2, rows, chans), BF16),
            pltpu.VMEM((2, rows, cwide), BF16),
            pltpu.VMEM((rows, outs), F32),
            dma((9,)),
            dma((5,)),
            dma((2,)),
            dma((2,)),
            dma((2,)),
            dma((2,)),
            dma((2, chans // (2 * LANES))),
            dma((inner,)),
            dma((inner,)),
            dma((n // inner,)),
            dma((n // inner,)),
            pltpu.SemaphoreType.REGULAR,
            pltpu.SemaphoreType.REGULAR,
        ],
        compiler_params=pltpu.CompilerParams(collective_id=0, has_side_effects=True),
    )(
        activations,
        norm_gain.reshape(1, -1),
        state_proj,
        value_proj,
        post_gate_proj,
        pre_gate_proj,
        input_map,
        jnp.swapaxes(output_map, 1, 2),
        skip_gain.reshape(1, -1),
        rotation,
        jnp.swapaxes(log_decay, 0, 1),
        initial_state,
        conv_taps,
        state_out,
        conv_out,
    )


def solution(mesh):
    return jax.shard_map(
        on_device,
        mesh=mesh,
        in_specs=(
            P("sp", "tp"),
            P(),
            P(None, "tp"),
            P(None, "tp"),
            P(None, "tp"),
            P(None, "tp"),
            P("tp", None, None),
            P("tp", None, None),
            P("tp"),
            P("tp", None),
            P("sp", "tp"),
            P(None, "tp", None),
            P(None, "tp"),
            P(None, "tp"),
            P(None, "tp"),
        ),
        out_specs=P("sp", "tp"),
        check_vma=False,
    )
```

```python
import functools

import jax
import jax.numpy as jnp
from jax import lax
from jax.experimental import pallas as pl
from jax.experimental.pallas import tpu as pltpu
from jax.sharding import PartitionSpec as P

EPS = 1e-06
LANES = 128
MESH = pl.DeviceIdType.MESH
F32 = jnp.float32
BF16 = jnp.bfloat16


def minus_expm1(y):
    poly = jnp.ones_like(y)
    for k in range(11, 1, -1):
        poly = 1.0 + poly * y * (1.0 / k)
    return jnp.where(y > -0.5, -y * poly, 1.0 - jnp.exp(y))


def split3(v):
    hi = v.astype(BF16)
    rest = v - hi.astype(F32)
    mid = rest.astype(BF16)
    low = (rest - mid.astype(F32)).astype(BF16)
    return hi, mid, low


def cmul(a, b):
    return a[0] * b[0] - a[1] * b[1], a[0] * b[1] + a[1] * b[0]


def cpow(base, count):
    result = None
    while count:
        if count & 1:
            result = base if result is None else cmul(result, base)
        count >>= 1
        if count:
            base = cmul(base, base)
    return result


def inner_of(n):
    return max(d for d in range(1, n + 1) if n % d == 0 and d * d <= n)


def gelu(x):
    return 0.5 * x * (1.0 + jnp.tanh(0.7978845608028654 * (x + 0.044715 * x * x * x)))


def kernel(
    n,
    x_hbm,
    gain_hbm,
    w0_hbm,
    w1_hbm,
    w2_hbm,
    w3_hbm,
    imap_hbm,
    omap_hbm,
    skip_hbm,
    rot_hbm,
    ld_hbm,
    init_hbm,
    taps_hbm,
    so_hbm,
    co_hbm,
    out_ref,
    x_ref,
    gain_ref,
    imap_ref,
    omap_ref,
    skip_ref,
    rot_ref,
    ld_ref,
    init_ref,
    taps_ref,
    wv,
    ov,
    xr,
    acc,
    din,
    bd_in,
    bd_out,
    coef,
    tbl,
    powers,
    chan_d,
    chan_end,
    chan_gain,
    rowed,
    pre,
    held,
    sums,
    to_chan,
    mag,
    drv,
    pairs,
    pad,
    near_in,
    far_in,
    far_out,
    hs,
    hc,
    oacc,
    in_sem,
    wsem,
    osem,
    x_sem,
    tail_sem,
    hc_sem,
    hs_sem,
    near_send,
    near_recv,
    far_send,
    far_recv,
    near_ready,
    far_ready,
):
    sp, tp = lax.axis_index("sp"), lax.axis_index("tp")
    other = 1 - tp
    rows, half = x_ref.shape
    groups, state = rot_ref.shape
    gch = imap_ref.shape[1]
    chans = groups * gch
    states = groups * state
    prow = states // LANES
    per_block = LANES // gch
    blocks = groups // per_block
    quads = prow // blocks
    pitch = drv.shape[0] // rows
    bstates = quads * LANES
    cwide = taps_ref.shape[1]
    width = taps_ref.shape[0]

    barrier = pltpu.get_barrier_semaphore()
    partner = {"sp": sp, "tp": other}

    inner = inner_of(n)
    outer = n // inner
    a, b = lax.div(sp, inner), lax.rem(sp, inner)
    last = outer - 1

    hop_back = (b == 0) & (a > 0) & (inner > 1)
    hop_on = (b == inner - 1) & (a < last) & (inner > 1)

    def tell(sem, j):
        pl.semaphore_signal(sem, inc=1, device_id={"sp": j, "tp": tp}, device_id_type=MESH)

    def greet_near(k, c):
        tell(barrier, a * inner + k)
        return c

    def greet_far(k, c):
        tell(barrier, k * inner + b)
        return c

    pl.semaphore_signal(barrier, inc=1, device_id=partner, device_id_type=MESH)
    lax.fori_loop(b + 1, inner, greet_near, 0)

    @pl.when(hop_on)
    def _():
        tell(barrier, sp + 1)

    lax.fori_loop(a + 1, outer, greet_far, 0)

    in_copies = {}
    def fetch(i, src, dst):
        in_copies[i] = pltpu.make_async_copy(src, dst, in_sem.at[i])
        in_copies[i].start()

    w_hbm = (w0_hbm, w1_hbm, w2_hbm, w3_hbm)

    def fetch_weight(i, h, sem):
        part = (tp, other)[h]
        pltpu.make_async_copy(
            w_hbm[i].at[pl.ds(part * half, half), :], wv.at[i, pl.ds(h * half, half), :], sem
        ).start()

    def wait_weight(i):
        pltpu.make_async_copy(w_hbm[i], wv.at[i], wsem.at[i]).wait()

    fetch(0, x_hbm, x_ref)
    fetch(4, ld_hbm, ld_ref)
    fetch(2, rot_hbm, rot_ref)
    fetch(5, imap_hbm, imap_ref)
    fetch(1, gain_hbm, gain_ref)
    fetch_weight(0, 0, wsem.at[0])
    fetch_weight(0, 1, wsem.at[4])

    pl.semaphore_wait(barrier, 1 + b + a + jnp.where(hop_back, 1, 0))

    def ready_near(k, c):
        tell(near_ready, a * inner + k)
        return c

    def ready_far(k, c):
        tell(far_ready, k * inner + b)
        return c

    lax.fori_loop(0, b, ready_near, 0)

    @pl.when(hop_back)
    def _():
        tell(near_ready, sp - 1)

    lax.fori_loop(0, a, ready_far, 0)

    when = lax.broadcasted_iota(jnp.int32, (rows, 2 * rows), 0)
    upto = lax.broadcasted_iota(jnp.int32, (rows, 2 * rows), 1)
    sums[...] = jnp.where(
        ((upto < rows) & (when <= upto)) | ((upto >= rows) & (when > upto - rows)), 1.0, 0.0
    ).astype(BF16)
    col = lax.broadcasted_iota(jnp.int32, (groups, chans), 1)
    row = lax.broadcasted_iota(jnp.int32, (groups, chans), 0)
    to_chan[...] = jnp.where((col >= row * gch) & (col < (row + 1) * gch), 1.0, 0.0).astype(BF16)

    def remote(src, dst, s, r, dev):
        return pltpu.make_async_remote_copy(
            src_ref=src, dst_ref=dst, send_sem=s, recv_sem=r, device_id=dev, device_id_type=MESH
        )

    in_copies[0].wait()
    x_copy = remote(x_ref, xr, x_sem.at[0], x_sem.at[1], partner)
    x_copy.start()

    fetch(3, init_hbm, init_ref)
    fetch(6, omap_hbm, omap_ref)
    fetch(7, skip_hbm, skip_ref)
    fetch(8, taps_hbm, taps_ref)
    for i in (1, 3, 2):
        for h in (0, 1):
            fetch_weight(i, h, wsem.at[i])
    for i, w, deep in ((1, co_hbm, cwide), (0, so_hbm, chans)):
        for h, part in ((0, tp), (1, other)):
            pltpu.make_async_copy(
                w.at[pl.ds(part * deep, deep), :], ov.at[i, pl.ds(h * deep, deep), :], osem.at[i]
            ).start()

    lane = lax.broadcasted_iota(jnp.int32, (1, LANES), 1)

    def pair_up(i, v):
        pairs[pl.ds(i * groups, groups), :] = v
        even = pairs[pl.ds(i * groups, prow, stride=2), :]
        odd = pairs[pl.ds(i * groups + 1, prow, stride=2), :]
        return jnp.where(lane < state, even, odd)

    def twice(v):
        return jnp.concatenate([v, v], axis=1)

    for i in (4, 2, 5, 1):
        in_copies[i].wait()
    ld = ld_ref[...]

    def time_sums(cols):
        added = jnp.dot(jnp.concatenate(split3(ld), axis=0), sums[:, cols], preferred_element_type=F32)
        return added[:groups] + added[groups : 2 * groups] + added[2 * groups :]

    def per_channel(v):
        hi, mid, _ = split3(v.T)
        return jnp.dot(hi, to_chan[...], preferred_element_type=F32) + jnp.dot(
            mid, to_chan[...], preferred_element_type=F32
        )

    gain = jnp.sqrt(minus_expm1(2.0 * ld))
    chan_end[...] = per_channel(gain * jnp.exp(time_sums(slice(rows, 2 * rows))))
    tot = pair_up(
        3, jnp.broadcast_to(jnp.exp(jnp.sum(ld, axis=1, keepdims=True)), (groups, LANES))
    )
    theta = pair_up(0, twice(rot_ref[...]))
    turn = jnp.cos(theta), jnp.sin(theta)
    step = turn
    for k in range(8):
        for i in (0, 1):
            powers[i, pl.ds(k * prow, prow), :] = step[i]
        step = cmul(step, turn) if k < 7 else step
    far_step16 = cmul(step, step)
    for i in (0, 1):
        powers[i, pl.ds(8 * prow, prow), :] = far_step16[i]
    whole = cpow(step, rows // 8)
    for r in range(prow):
        even = [powers[i, pl.ds(r, 8, stride=prow), :] for i in (0, 1)]
        eight = [powers[i, pl.ds(7 * prow + r, 1), :] for i in (0, 1)]
        sixteen = [powers[i, pl.ds(8 * prow + r, 1), :] for i in (0, 1)]
        odd = cmul(even, eight)
        for t in range(0, rows, 16):
            for i in (0, 1):
                tbl[t : t + 16, (2 * r + i) * LANES : (2 * r + i + 1) * LANES] = jnp.concatenate(
                    [even[i], odd[i]], axis=0
                ).astype(BF16)
            even = cmul(even, sixteen)
            odd = cmul(odd, sixteen)

    def spread_map(src, dst):
        dst[...] = jnp.zeros_like(dst)
        for b in range(blocks):
            for q in range(quads):
                g = b * per_block + 2 * q
                one = src[g].astype(F32)
                two = src[g + 1].astype(F32)
                one_r = jnp.concatenate([one[:, state:], one[:, :state]], axis=1)
                two_r = jnp.concatenate([two[:, state:], two[:, :state]], axis=1)
                low = lane < state
                re = jnp.concatenate([jnp.where(low, one, 0.0), jnp.where(low, 0.0, two_r)], axis=0)
                im = jnp.concatenate([jnp.where(low, one_r, 0.0), jnp.where(low, 0.0, two)], axis=0)
                at = pl.ds(b * LANES + q * 2 * gch, 2 * gch)
                dst[at, 2 * q * LANES : (2 * q + 1) * LANES] = re.astype(BF16)
                dst[at, (2 * q + 1) * LANES : (2 * q + 2) * LANES] = im.astype(BF16)

    spread_map(imap_ref, bd_in)
    own = x_ref[...].astype(F32)
    scaled = (own * gain_ref[:, pl.ds(pl.multiple_of(tp * half, LANES), half)]).astype(BF16)
    squares = jnp.sum(own * own, axis=1, keepdims=True)
    half_copy = pltpu.make_async_copy(w_hbm[0].at[pl.ds(0, half), :], wv.at[0, pl.ds(0, half), :], wsem.at[0])
    half_copy.wait()
    partial = jnp.dot(scaled, wv[0, :half], preferred_element_type=F32)
    acc[:, :half] = scaled

    x_copy.wait_recv()
    far_x = xr[...].astype(F32)
    scaled_far = (far_x * gain_ref[:, pl.ds(pl.multiple_of(other * half, LANES), half)]).astype(BF16)
    squares = squares + jnp.sum(far_x * far_x, axis=1, keepdims=True)
    scale = lax.rsqrt(squares / (2 * half) + EPS)

    acc[:, half:] = scaled_far
    rest_copy = pltpu.make_async_copy(
        w_hbm[0].at[pl.ds(0, half), :], wv.at[0, pl.ds(half, half), :], wsem.at[4]
    )
    rest_copy.wait()
    total = partial + jnp.dot(scaled_far, wv[0, half:], preferred_element_type=F32)
    drive_in = (total * scale).astype(BF16)
    din[...] = drive_in
    ends_in = (drive_in.astype(F32) * chan_end[...]).astype(BF16).T
    for r in range(prow):
        q = r % quads
        at = slice(r * 2 * gch, (r + 1) * 2 * gch)
        seen = jnp.dot(
            ends_in[at], tbl[:, 2 * r * LANES : (2 * r + 2) * LANES], preferred_element_type=F32
        )
        m_re = bd_in[at, 2 * q * LANES : (2 * q + 1) * LANES].astype(F32)
        m_im = bd_in[at, (2 * q + 1) * LANES : (2 * q + 2) * LANES].astype(F32)
        c, d = seen[:, :LANES], seen[:, LANES:]
        rowed[0, r : r + 1, :] = jnp.sum(c * m_re + d * m_im, axis=0, keepdims=True)
        rowed[1, r : r + 1, :] = jnp.sum(c * m_im - d * m_re, axis=0, keepdims=True)
    e_re, e_im = cmul(whole, (rowed[0], rowed[1]))

    near_in[b, pl.ds(0, prow), :] = e_re.astype(BF16)
    near_in[b, pl.ds(prow, prow), :] = e_im.astype(BF16)
    own_hi, own_lo, _ = split3(tot)
    near_in[b, pl.ds(2 * prow, prow), :] = own_hi
    near_in[b, pl.ds(3 * prow, prow), :] = own_lo

    def near_copy(k):
        return remote(
            near_in.at[b], near_in.at[b], near_send.at[k], near_recv.at[b], {"sp": a * inner + k, "tp": tp}
        )

    def far_copy(k):
        return remote(
            far_out, far_in.at[a], far_send.at[k], far_recv.at[a], {"sp": k * inner + b, "tp": tp}
        )

    near_from = jnp.where(a < last, 0, b + 1)
    near_upto = jnp.where(a < last, inner, b)
    after = inner - 1 - b + jnp.where(hop_on, 1, 0)

    @pl.when(after > 0)
    def _():
        pl.semaphore_wait(near_ready, after)

    def send_near(k, c):
        @pl.when(k != b)
        def _():
            near_copy(k).start()

        return c

    lax.fori_loop(near_from, inner, send_near, 0)

    def project(i):
        wait_weight(i)
        total = jnp.dot(acc[...], wv[i], preferred_element_type=F32)
        return (total * scale).astype(BF16)

    value = project(1)
    pre_gate = project(3)
    mixed = (pre_gate.astype(F32) * value.astype(F32)).astype(BF16).astype(F32)
    pad[pl.ds(8, rows), :] = mixed
    tail_copy = remote(
        pad.at[pl.ds(rows, 8), :],
        pad.at[pl.ds(0, 8), :],
        tail_sem.at[0],
        tail_sem.at[1],
        {"sp": lax.rem(sp + 1, n), "tp": tp},
    )

    @pl.when(sp < n - 1)
    def _():
        tail_copy.start()

    for i in (6, 7):
        in_copies[i].wait()
    spread_map(omap_ref, bd_out)

    ld = ld_ref[...]
    gain = jnp.sqrt(minus_expm1(2.0 * ld))
    late = per_channel(jnp.concatenate([jnp.exp(time_sums(slice(0, rows))), gain], axis=1))
    chan_d[...] = late[:rows]
    chan_gain[...] = late[rows:]
    mags = split3(jnp.exp(ld).T)[:2]
    for k in range(blocks):
        col = lax.broadcasted_iota(jnp.int32, (groups, bstates), 1) + k * bstates
        row = lax.broadcasted_iota(jnp.int32, (groups, bstates), 0)
        spread = jnp.where(
            (col >= row * state) & (col < (row + 1) * state), 1.0, 0.0
        ).astype(BF16)
        m = jnp.dot(mags[0], spread, preferred_element_type=F32) + jnp.dot(
            mags[1], spread, preferred_element_type=F32
        )
        for q in range(quads):
            mag[pl.ds(k * quads + q, rows, stride=prow), :] = m[:, q * LANES : (q + 1) * LANES]

    hc[0] = project(2)
    gained = (din[...].astype(F32) * chan_gain[...]).astype(BF16)
    for k in range(blocks):
        blk = jnp.dot(
            gained[:, k * LANES : (k + 1) * LANES],
            bd_in[k * LANES : (k + 1) * LANES, :],
            preferred_element_type=F32,
        )
        for q in range(quads):
            r = k * quads + q
            drv[pl.ds(r, rows, stride=pitch), :] = blk[:, 2 * q * LANES : (2 * q + 1) * LANES]
            drv[pl.ds(prow + r, rows, stride=pitch), :] = blk[
                :, (2 * q + 1) * LANES : (2 * q + 2) * LANES
            ]

    def near_step(k, c):
        @pl.when(k != b)
        def _():
            remote(
                near_in.at[k], near_in.at[k], near_send.at[k], near_recv.at[k], {"sp": a * inner + k, "tp": tp}
            ).wait_recv()

        ends, mag_all, phase, mine = c[0:2], c[2], c[3:5], c[5:]
        k_mag = near_in[k, pl.ds(2 * prow, prow), :].astype(F32) + near_in[
            k, pl.ds(3 * prow, prow), :
        ].astype(F32)
        moved = cmul((whole[0] * k_mag, whole[1] * k_mag), ends)
        now = (
            moved[0] + near_in[k, pl.ds(0, prow), :].astype(F32),
            moved[1] + near_in[k, pl.ds(prow, prow), :].astype(F32),
            mag_all * k_mag,
        ) + cmul(whole, phase)
        return now + tuple(jnp.where(k < b, v, w) for v, w in zip(now, mine))

    def send_far(k, c):
        far_copy(k).start()
        return c

    def join_near():
        one = jnp.ones((prow, LANES), F32)
        first = pair_up(1, twice(init_ref[0])), pair_up(2, twice(init_ref[1]))
        begin = tuple(jnp.where(a == 0, v, zero) for v in first) + (one, one, zero)
        plane = lax.fori_loop(0, near_upto, near_step, begin + begin)
        for i in range(5):
            held[i] = plane[5 + i]

        @pl.when(a < last)
        def _():
            far_out[pl.ds(0, prow), :] = plane[0].astype(BF16)
            far_out[pl.ds(prow, prow), :] = plane[1].astype(BF16)
            all_hi, all_lo, _ = split3(plane[2])
            far_out[pl.ds(2 * prow, prow), :] = all_hi
            far_out[pl.ds(3 * prow, prow), :] = all_lo
            pl.semaphore_wait(far_ready, last - a)
            lax.fori_loop(a + 1, outer, send_far, 0)

    zero = jnp.zeros((prow, LANES), F32)
    in_copies[3].wait()

    @pl.when(b > 0)
    def _():
        join_near()

    def scan(t, h):
        m = mag[pl.ds(pl.multiple_of(t * prow, prow), prow), :]
        base = pl.multiple_of(t * pitch, 8)
        d_re = drv[pl.ds(base, prow), :]
        d_im = drv[pl.ds(base + prow, prow), :]
        f_re, f_im = m * turn[0], m * turn[1]
        new_re = (f_re * h[0] + d_re) - f_im * h[1]
        new_im = (f_re * h[1] + d_im) + f_im * h[0]
        drv[pl.ds(base, prow), :] = new_re
        drv[pl.ds(base + prow, prow), :] = new_im
        return new_re, new_im

    lax.fori_loop(0, rows, scan, (zero, zero), unroll=8)
    for k in range(blocks):
        cols = slice(k * LANES, (k + 1) * LANES)
        at = [half_row + k * quads + q for q in range(quads) for half_row in (0, prow)]
        st = jnp.concatenate(
            [drv[pl.ds(r, rows, stride=pitch), :].astype(BF16) for r in at], axis=1
        )
        read = lax.dot_general(
            st, bd_out[cols, :], (((1,), (1,)), ((), ())), preferred_element_type=F32
        )
        pre[:, cols] = read + skip_ref[:, cols] * din[:, cols].astype(F32)
    coef[...] = jnp.zeros_like(coef)

    @pl.when(b == 0)
    def _():
        join_near()

    @pl.when(sp == 0)
    def _():
        pad[pl.ds(0, 8), :] = jnp.zeros((8, cwide), F32)

    in_copies[8].wait()

    @pl.when(sp > 0)
    def _():
        tail_copy.wait_recv()

    conv = jnp.zeros((rows, cwide), F32)
    for k in range(width):
        conv = conv + pad[pl.ds(8 + k - (width - 1), rows), :] * taps_ref[k : k + 1, :].astype(F32)
    hc[0] = (hc[0].astype(F32) * conv).astype(BF16)
    hc_copy = remote(hc.at[0], hc.at[1], hc_sem.at[0], hc_sem.at[1], partner)
    hc_copy.start()
    for i in (0, 1):
        pltpu.make_async_copy((so_hbm, co_hbm)[i], ov.at[i], osem.at[i]).wait()
    oacc[...] = jnp.dot(hc[0], ov[1, :cwide], preferred_element_type=F32)
    whole_plane = cpow(whole, inner)

    def far_step(k, h):
        remote(
            far_out, far_in.at[k], far_send.at[k], far_recv.at[k], {"sp": k * inner + b, "tp": tp}
        ).wait_recv()
        k_mag = far_in[k, pl.ds(2 * prow, prow), :].astype(F32) + far_in[
            k, pl.ds(3 * prow, prow), :
        ].astype(F32)
        moved = cmul((whole_plane[0] * k_mag, whole_plane[1] * k_mag), h)
        k_re = far_in[k, pl.ds(0, prow), :].astype(F32)
        k_im = far_in[k, pl.ds(prow, prow), :].astype(F32)
        return moved[0] + k_re, moved[1] + k_im

    before = lax.fori_loop(0, a, far_step, (zero, zero))
    mine = [held[i] for i in range(5)]
    moved = cmul((mine[3] * mine[2], mine[4] * mine[2]), before)
    enter = (mine[0] + moved[0], mine[1] + moved[1])

    rowed[0] = enter[0]
    rowed[1] = enter[1]
    hs_copies = []
    for k in range(blocks):
        cols = slice(k * LANES, (k + 1) * LANES)
        for q in range(quads):
            r = k * quads + q
            at = slice(r * 2 * gch, (r + 1) * 2 * gch)
            left = slice(2 * q * LANES, (2 * q + 1) * LANES)
            right = slice((2 * q + 1) * LANES, (2 * q + 2) * LANES)
            h_re, h_im = rowed[0, r : r + 1, :], rowed[1, r : r + 1, :]
            o_re, o_im = bd_out[at, left].astype(F32), bd_out[at, right].astype(F32)
            coef[at, left] = (h_re * o_re + h_im * o_im).astype(BF16)
            coef[at, right] = (h_re * o_im - h_im * o_re).astype(BF16)
        moved = lax.dot_general(
            tbl[:, 2 * k * bstates : 2 * (k + 1) * bstates],
            coef[cols, :],
            (((1,), (1,)), ((), ())),
            preferred_element_type=F32,
        )
        hs[0, :, cols] = gelu(pre[:, cols] + chan_d[:, cols] * moved).astype(BF16)
        if k % 2 == 1:
            two = pl.ds((k - 1) * LANES, 2 * LANES)
            copy = remote(
                hs.at[0, :, two], hs.at[1, :, two], hs_sem.at[0, k // 2], hs_sem.at[1, k // 2], partner
            )
            copy.start()
            hs_copies.append(copy)
    oacc[...] += jnp.dot(hs[0], ov[0, :chans], preferred_element_type=F32)
    hc_copy.wait_recv()
    oacc[...] += jnp.dot(hc[1], ov[1, cwide:], preferred_element_type=F32)
    for copy in hs_copies:
        copy.wait_recv()
    out_ref[...] = (oacc[...] + jnp.dot(hs[1], ov[0, chans:], preferred_element_type=F32)).astype(BF16)

    x_copy.wait_send()
    hc_copy.wait_send()
    for copy in hs_copies:
        copy.wait_send()

    @pl.when(sp < n - 1)
    def _():
        tail_copy.wait_send()

    def near_sent(k, c):
        @pl.when(k != b)
        def _():
            near_copy(k).wait_send()

        return c

    def far_sent(k, c):
        far_copy(k).wait_send()
        return c

    lax.fori_loop(near_from, inner, near_sent, 0)
    lax.fori_loop(a + 1, outer, far_sent, 0)


def on_device(
    activations,
    norm_gain,
    state_proj,
    value_proj,
    post_gate_proj,
    pre_gate_proj,
    input_map,
    output_map,
    skip_gain,
    rotation,
    log_decay,
    initial_state,
    conv_taps,
    state_out,
    conv_out,
):
    n = lax.axis_size("sp")
    rows, half = activations.shape
    groups, state = rotation.shape
    chans = state_proj.shape[1]
    cwide = value_proj.shape[1]
    outs = state_out.shape[1]
    states = groups * state
    prow = states // LANES
    inner = inner_of(n)
    bdw = 2 * states // (chans // LANES)
    vmem = pl.BlockSpec(memory_space=pltpu.VMEM)
    hbm = pl.BlockSpec(memory_space=pl.ANY)
    dma = pltpu.SemaphoreType.DMA
    return pl.pallas_call(
        functools.partial(kernel, n),
        out_shape=pltpu.VMEM((rows, outs), BF16),
        in_specs=[hbm] * 15,
        out_specs=vmem,
        scratch_shapes=[
            pltpu.VMEM((rows, half), BF16),
            pltpu.VMEM((1, 2 * half), F32),
            pltpu.VMEM(input_map.shape, BF16),
            pltpu.VMEM((groups, output_map.shape[2], output_map.shape[1]), F32),
            pltpu.VMEM((1, chans), F32),
            pltpu.VMEM((groups, state), F32),
            pltpu.VMEM((groups, rows), F32),
            pltpu.VMEM(initial_state.shape, F32),
            pltpu.VMEM(conv_taps.shape, BF16),
            pltpu.VMEM((4, 2 * half, chans), BF16),
            pltpu.VMEM((2, 2 * chans, outs), BF16),
            pltpu.VMEM((rows, half), BF16),
            pltpu.VMEM((rows, 2 * half), BF16),
            pltpu.VMEM((rows, chans), BF16),
            pltpu.VMEM((chans, bdw), BF16),
            pltpu.VMEM((chans, bdw), BF16),
            pltpu.VMEM((chans, bdw), BF16),
            pltpu.VMEM((rows, 2 * states), BF16),
            pltpu.VMEM((2, 9 * prow, LANES), F32),
            pltpu.VMEM((rows, chans), F32),
            pltpu.VMEM((rows, chans), F32),
            pltpu.VMEM((rows, chans), F32),
            pltpu.VMEM((2, prow, LANES), F32),
            pltpu.VMEM((rows, chans), F32),
            pltpu.VMEM((5, prow, LANES), F32),
            pltpu.VMEM((rows, 2 * rows), BF16),
            pltpu.VMEM((groups, chans), BF16),
            pltpu.VMEM((rows * prow, LANES), F32),
            pltpu.VMEM((rows * (2 * prow + 8), LANES), F32),
            pltpu.VMEM((4 * groups, LANES), F32),
            pltpu.VMEM((rows + 8, cwide), F32),
            pltpu.VMEM((inner, 4 * prow, LANES), BF16),
            pltpu.VMEM((n // inner, 4 * prow, LANES), BF16),
            pltpu.VMEM((4 * prow, LANES), BF16),
            pltpu.VMEM((2, rows, chans), BF16),
            pltpu.VMEM((2, rows, cwide), BF16),
            pltpu.VMEM((rows, outs), F32),
            dma((9,)),
            dma((5,)),
            dma((2,)),
            dma((2,)),
            dma((2,)),
            dma((2,)),
            dma((2, chans // (2 * LANES))),
            dma((inner,)),
            dma((inner,)),
            dma((n // inner,)),
            dma((n // inner,)),
            pltpu.SemaphoreType.REGULAR,
            pltpu.SemaphoreType.REGULAR,
        ],
        compiler_params=pltpu.CompilerParams(collective_id=0, has_side_effects=True),
    )(
        activations,
        norm_gain.reshape(1, -1),
        state_proj,
        value_proj,
        post_gate_proj,
        pre_gate_proj,
        input_map,
        jnp.swapaxes(output_map, 1, 2),
        skip_gain.reshape(1, -1),
        rotation,
        jnp.swapaxes(log_decay, 0, 1),
        initial_state,
        conv_taps,
        state_out,
        conv_out,
    )


def solution(mesh):
    return jax.shard_map(
        on_device,
        mesh=mesh,
        in_specs=(
            P("sp", "tp"),
            P(),
            P(None, "tp"),
            P(None, "tp"),
            P(None, "tp"),
            P(None, "tp"),
            P("tp", None, None),
            P("tp", None, None),
            P("tp"),
            P("tp", None),
            P("sp", "tp"),
            P(None, "tp", None),
            P(None, "tp"),
            P(None, "tp"),
            P(None, "tp"),
        ),
        out_specs=P("sp", "tp"),
        check_vma=False,
    )
```

```python
import functools

import jax
import jax.numpy as jnp
from jax import lax
from jax.experimental import pallas as pl
from jax.experimental.pallas import tpu as pltpu
from jax.sharding import PartitionSpec as P

EPS = 1e-06
LANES = 128
MESH = pl.DeviceIdType.MESH
F32 = jnp.float32
BF16 = jnp.bfloat16


def minus_expm1(y):
    poly = jnp.ones_like(y)
    for k in range(11, 1, -1):
        poly = 1.0 + poly * y * (1.0 / k)
    return jnp.where(y > -0.5, -y * poly, 1.0 - jnp.exp(y))


def split3(v):
    hi = v.astype(BF16)
    rest = v - hi.astype(F32)
    mid = rest.astype(BF16)
    low = (rest - mid.astype(F32)).astype(BF16)
    return hi, mid, low


def cmul(a, b):
    return a[0] * b[0] - a[1] * b[1], a[0] * b[1] + a[1] * b[0]


def cpow(base, count):
    result = None
    while count:
        if count & 1:
            result = base if result is None else cmul(result, base)
        count >>= 1
        if count:
            base = cmul(base, base)
    return result


def inner_of(n):
    return max(d for d in range(1, n + 1) if n % d == 0 and d * d <= n)


def gelu(x):
    return 0.5 * x * (1.0 + jnp.tanh(0.7978845608028654 * (x + 0.044715 * x * x * x)))


def kernel(
    n,
    x_hbm,
    gain_hbm,
    w0_hbm,
    w1_hbm,
    w2_hbm,
    w3_hbm,
    imap_hbm,
    omap_hbm,
    skip_hbm,
    rot_hbm,
    ld_hbm,
    init_hbm,
    taps_hbm,
    so_hbm,
    co_hbm,
    out_ref,
    x_ref,
    gain_ref,
    imap_ref,
    omap_ref,
    skip_ref,
    rot_ref,
    ld_ref,
    init_ref,
    taps_ref,
    wv,
    ov,
    xr,
    acc,
    din,
    bd_in,
    bd_out,
    map_t,
    tbl,
    powers,
    chan_d,
    chan_end,
    chan_gain,
    rowed,
    pre,
    held,
    sums,
    to_chan,
    mag,
    drv,
    pairs,
    pad,
    near_in,
    far_in,
    far_out,
    hs,
    hc,
    oacc,
    in_sem,
    wsem,
    osem,
    x_sem,
    tail_sem,
    hc_sem,
    hs_sem,
    near_send,
    near_recv,
    far_send,
    far_recv,
    near_ready,
    far_ready,
):
    sp, tp = lax.axis_index("sp"), lax.axis_index("tp")
    other = 1 - tp
    rows, half = x_ref.shape
    groups, state = rot_ref.shape
    gch = imap_ref.shape[1]
    chans = groups * gch
    states = groups * state
    prow = states // LANES
    per_block = LANES // gch
    blocks = groups // per_block
    quads = prow // blocks
    pitch = drv.shape[0] // rows
    bstates = quads * LANES
    cwide = taps_ref.shape[1]
    width = taps_ref.shape[0]

    barrier = pltpu.get_barrier_semaphore()
    partner = {"sp": sp, "tp": other}

    inner = inner_of(n)
    outer = n // inner
    a, b = lax.div(sp, inner), lax.rem(sp, inner)
    last = outer - 1

    hop_on = (b == inner - 1) & (a < last)

    def tell(sem, j):
        pl.semaphore_signal(sem, inc=1, device_id={"sp": j, "tp": tp}, device_id_type=MESH)

    def greet_near(k, c):
        tell(barrier, a * inner + k)
        return c

    def greet_far(k, c):
        tell(barrier, k * inner + b)
        return c

    pl.semaphore_signal(barrier, inc=1, device_id=partner, device_id_type=MESH)
    lax.fori_loop(b + 1, inner, greet_near, 0)

    lax.fori_loop(a + 1, outer, greet_far, 0)

    in_copies = {}
    def fetch(i, src, dst):
        in_copies[i] = pltpu.make_async_copy(src, dst, in_sem.at[i])
        in_copies[i].start()

    w_hbm = (w0_hbm, w1_hbm, w2_hbm, w3_hbm)

    def fetch_weight(i, h, sem):
        part = (tp, other)[h]
        pltpu.make_async_copy(
            w_hbm[i].at[pl.ds(part * half, half), :], wv.at[i, pl.ds(h * half, half), :], sem
        ).start()

    def wait_weight(i):
        pltpu.make_async_copy(w_hbm[i], wv.at[i], wsem.at[i]).wait()

    fetch(0, x_hbm, x_ref)
    fetch(4, ld_hbm, ld_ref)
    fetch(2, rot_hbm, rot_ref)
    fetch(5, imap_hbm, imap_ref)
    fetch(1, gain_hbm, gain_ref)
    fetch_weight(0, 0, wsem.at[0])
    fetch_weight(0, 1, wsem.at[4])

    pl.semaphore_wait(barrier, 1 + b + a)

    def ready_near(k, c):
        tell(near_ready, a * inner + k)
        return c

    def ready_far(k, c):
        tell(far_ready, k * inner + b)
        return c

    lax.fori_loop(0, b, ready_near, 0)

    lax.fori_loop(0, a, ready_far, 0)

    when = lax.broadcasted_iota(jnp.int32, (rows, 2 * rows), 0)
    upto = lax.broadcasted_iota(jnp.int32, (rows, 2 * rows), 1)
    sums[...] = jnp.where(
        ((upto < rows) & (when <= upto)) | ((upto >= rows) & (when > upto - rows)), 1.0, 0.0
    ).astype(BF16)
    col = lax.broadcasted_iota(jnp.int32, (groups, chans), 1)
    row = lax.broadcasted_iota(jnp.int32, (groups, chans), 0)
    to_chan[...] = jnp.where((col >= row * gch) & (col < (row + 1) * gch), 1.0, 0.0).astype(BF16)

    def remote(src, dst, s, r, dev):
        return pltpu.make_async_remote_copy(
            src_ref=src, dst_ref=dst, send_sem=s, recv_sem=r, device_id=dev, device_id_type=MESH
        )

    in_copies[0].wait()
    x_copy = remote(x_ref, xr, x_sem.at[0], x_sem.at[1], partner)
    x_copy.start()

    fetch(3, init_hbm, init_ref)
    fetch(6, omap_hbm, omap_ref)
    fetch(7, skip_hbm, skip_ref)
    fetch(8, taps_hbm, taps_ref)
    for i in (1, 3, 2):
        for h in (0, 1):
            fetch_weight(i, h, wsem.at[i])
    for i, w, deep in ((1, co_hbm, cwide), (0, so_hbm, chans)):
        for h, part in ((0, tp), (1, other)):
            pltpu.make_async_copy(
                w.at[pl.ds(part * deep, deep), :], ov.at[i, pl.ds(h * deep, deep), :], osem.at[i]
            ).start()

    lane = lax.broadcasted_iota(jnp.int32, (1, LANES), 1)

    def pair_up(i, v):
        pairs[pl.ds(i * groups, groups), :] = v
        even = pairs[pl.ds(i * groups, prow, stride=2), :]
        odd = pairs[pl.ds(i * groups + 1, prow, stride=2), :]
        return jnp.where(lane < state, even, odd)

    def twice(v):
        return jnp.concatenate([v, v], axis=1)

    for i in (4, 2, 5, 1):
        in_copies[i].wait()
    ld = ld_ref[...]

    def time_sums(cols):
        added = jnp.dot(jnp.concatenate(split3(ld), axis=0), sums[:, cols], preferred_element_type=F32)
        return added[:groups] + added[groups : 2 * groups] + added[2 * groups :]

    def per_channel(v):
        hi, mid, _ = split3(v.T)
        return jnp.dot(hi, to_chan[...], preferred_element_type=F32) + jnp.dot(
            mid, to_chan[...], preferred_element_type=F32
        )

    gain = jnp.sqrt(minus_expm1(2.0 * ld))
    chan_end[...] = per_channel(gain * jnp.exp(time_sums(slice(rows, 2 * rows))))
    tot = pair_up(
        3, jnp.broadcast_to(jnp.exp(jnp.sum(ld, axis=1, keepdims=True)), (groups, LANES))
    )
    theta = pair_up(0, twice(rot_ref[...]))
    turn = jnp.cos(theta), jnp.sin(theta)
    step = turn
    for k in range(8):
        for i in (0, 1):
            powers[i, pl.ds(k * prow, prow), :] = step[i]
        step = cmul(step, turn) if k < 7 else step
    far_step16 = cmul(step, step)
    for i in (0, 1):
        powers[i, pl.ds(8 * prow, prow), :] = far_step16[i]
    whole = cpow(step, rows // 8)
    for r in range(prow):
        even = [powers[i, pl.ds(r, 8, stride=prow), :] for i in (0, 1)]
        eight = [powers[i, pl.ds(7 * prow + r, 1), :] for i in (0, 1)]
        sixteen = [powers[i, pl.ds(8 * prow + r, 1), :] for i in (0, 1)]
        odd = cmul(even, eight)
        for t in range(0, rows, 16):
            for i in (0, 1):
                tbl[t : t + 16, (2 * r + i) * LANES : (2 * r + i + 1) * LANES] = jnp.concatenate(
                    [even[i], odd[i]], axis=0
                ).astype(BF16)
            even = cmul(even, sixteen)
            odd = cmul(odd, sixteen)

    def spread_map(src, dst):
        dst[...] = jnp.zeros_like(dst)
        for b in range(blocks):
            for q in range(quads):
                g = b * per_block + 2 * q
                one = src[g].astype(F32)
                two = src[g + 1].astype(F32)
                one_r = jnp.concatenate([one[:, state:], one[:, :state]], axis=1)
                two_r = jnp.concatenate([two[:, state:], two[:, :state]], axis=1)
                low = lane < state
                re = jnp.concatenate([jnp.where(low, one, 0.0), jnp.where(low, 0.0, two_r)], axis=0)
                im = jnp.concatenate([jnp.where(low, one_r, 0.0), jnp.where(low, 0.0, two)], axis=0)
                at = pl.ds(b * LANES + q * 2 * gch, 2 * gch)
                dst[at, 2 * q * LANES : (2 * q + 1) * LANES] = re.astype(BF16)
                dst[at, (2 * q + 1) * LANES : (2 * q + 2) * LANES] = im.astype(BF16)

    spread_map(imap_ref, bd_in)
    own = x_ref[...].astype(F32)
    scaled = (own * gain_ref[:, pl.ds(pl.multiple_of(tp * half, LANES), half)]).astype(BF16)
    squares = jnp.sum(own * own, axis=1, keepdims=True)
    half_copy = pltpu.make_async_copy(w_hbm[0].at[pl.ds(0, half), :], wv.at[0, pl.ds(0, half), :], wsem.at[0])
    half_copy.wait()
    partial = jnp.dot(scaled, wv[0, :half], preferred_element_type=F32)
    acc[:, :half] = scaled

    x_copy.wait_recv()
    far_x = xr[...].astype(F32)
    scaled_far = (far_x * gain_ref[:, pl.ds(pl.multiple_of(other * half, LANES), half)]).astype(BF16)
    squares = squares + jnp.sum(far_x * far_x, axis=1, keepdims=True)
    scale = lax.rsqrt(squares / (2 * half) + EPS)

    acc[:, half:] = scaled_far
    rest_copy = pltpu.make_async_copy(
        w_hbm[0].at[pl.ds(0, half), :], wv.at[0, pl.ds(half, half), :], wsem.at[4]
    )
    rest_copy.wait()
    total = partial + jnp.dot(scaled_far, wv[0, half:], preferred_element_type=F32)
    drive_in = (total * scale).astype(BF16)
    din[...] = drive_in
    ends_in = (drive_in.astype(F32) * chan_end[...]).astype(BF16).T
    for r in range(prow):
        q = r % quads
        at = slice(r * 2 * gch, (r + 1) * 2 * gch)
        seen = jnp.dot(
            ends_in[at], tbl[:, 2 * r * LANES : (2 * r + 2) * LANES], preferred_element_type=F32
        )
        m_re = bd_in[at, 2 * q * LANES : (2 * q + 1) * LANES].astype(F32)
        m_im = bd_in[at, (2 * q + 1) * LANES : (2 * q + 2) * LANES].astype(F32)
        c, d = seen[:, :LANES], seen[:, LANES:]
        rowed[0, r : r + 1, :] = jnp.sum(c * m_re + d * m_im, axis=0, keepdims=True)
        rowed[1, r : r + 1, :] = jnp.sum(c * m_im - d * m_re, axis=0, keepdims=True)
    e_re, e_im = cmul(whole, (rowed[0], rowed[1]))

    near_in[b, pl.ds(0, prow), :] = e_re.astype(BF16)
    near_in[b, pl.ds(prow, prow), :] = e_im.astype(BF16)
    own_hi, own_lo, _ = split3(tot)
    near_in[b, pl.ds(2 * prow, prow), :] = own_hi
    near_in[b, pl.ds(3 * prow, prow), :] = own_lo

    def near_copy(k):
        return remote(
            near_in.at[b], near_in.at[b], near_send.at[k], near_recv.at[b], {"sp": a * inner + k, "tp": tp}
        )

    def far_copy(k):
        return remote(
            far_out, far_in.at[a], far_send.at[k], far_recv.at[a], {"sp": k * inner + b, "tp": tp}
        )

    near_from = jnp.where(a < last, 0, b + 1)
    near_upto = jnp.where(a < last, inner, b)
    after = inner - 1 - b

    @pl.when(after > 0)
    def _():
        pl.semaphore_wait(near_ready, after)

    def send_near(k, c):
        @pl.when(k != b)
        def _():
            near_copy(k).start()

        return c

    lax.fori_loop(near_from, inner, send_near, 0)

    def project(i):
        wait_weight(i)
        total = jnp.dot(acc[...], wv[i], preferred_element_type=F32)
        return (total * scale).astype(BF16)

    value = project(1)
    pre_gate = project(3)
    mixed = (pre_gate.astype(F32) * value.astype(F32)).astype(BF16).astype(F32)
    pad[pl.ds(8, rows), :] = mixed
    tail_copy = remote(
        pad.at[pl.ds(rows, 8), :],
        pad.at[pl.ds(0, 8), :],
        tail_sem.at[0],
        tail_sem.at[1],
        {"sp": lax.rem(sp + 1, n), "tp": tp},
    )

    @pl.when(hop_on)
    def _():
        pl.semaphore_wait(far_ready, last - a)

    @pl.when(sp < n - 1)
    def _():
        tail_copy.start()

    for i in (6, 7):
        in_copies[i].wait()
    spread_map(omap_ref, bd_out)
    for k in range(blocks):
        map_t[2 * k * bstates : 2 * (k + 1) * bstates, :] = bd_out[k * LANES : (k + 1) * LANES, :].T

    ld = ld_ref[...]
    gain = jnp.sqrt(minus_expm1(2.0 * ld))
    late = per_channel(jnp.concatenate([jnp.exp(time_sums(slice(0, rows))), gain], axis=1))
    chan_d[...] = late[:rows]
    chan_gain[...] = late[rows:]
    mags = split3(jnp.exp(ld).T)[:2]
    for k in range(blocks):
        col = lax.broadcasted_iota(jnp.int32, (groups, bstates), 1) + k * bstates
        row = lax.broadcasted_iota(jnp.int32, (groups, bstates), 0)
        spread = jnp.where(
            (col >= row * state) & (col < (row + 1) * state), 1.0, 0.0
        ).astype(BF16)
        m = jnp.dot(mags[0], spread, preferred_element_type=F32) + jnp.dot(
            mags[1], spread, preferred_element_type=F32
        )
        for q in range(quads):
            mag[pl.ds(k * quads + q, rows, stride=prow), :] = m[:, q * LANES : (q + 1) * LANES]

    hc[0] = project(2)
    gained = (din[...].astype(F32) * chan_gain[...]).astype(BF16)
    for k in range(blocks):
        blk = jnp.dot(
            gained[:, k * LANES : (k + 1) * LANES],
            bd_in[k * LANES : (k + 1) * LANES, :],
            preferred_element_type=F32,
        )
        for q in range(quads):
            r = k * quads + q
            drv[pl.ds(r, rows, stride=pitch), :] = blk[:, 2 * q * LANES : (2 * q + 1) * LANES]
            drv[pl.ds(prow + r, rows, stride=pitch), :] = blk[
                :, (2 * q + 1) * LANES : (2 * q + 2) * LANES
            ]

    def near_step(k, c):
        @pl.when(k != b)
        def _():
            remote(
                near_in.at[k], near_in.at[k], near_send.at[k], near_recv.at[k], {"sp": a * inner + k, "tp": tp}
            ).wait_recv()

        ends, mag_all, phase, mine = c[0:2], c[2], c[3:5], c[5:]
        k_mag = near_in[k, pl.ds(2 * prow, prow), :].astype(F32) + near_in[
            k, pl.ds(3 * prow, prow), :
        ].astype(F32)
        moved = cmul((whole[0] * k_mag, whole[1] * k_mag), ends)
        now = (
            moved[0] + near_in[k, pl.ds(0, prow), :].astype(F32),
            moved[1] + near_in[k, pl.ds(prow, prow), :].astype(F32),
            mag_all * k_mag,
        ) + cmul(whole, phase)
        return now + tuple(jnp.where(k < b, v, w) for v, w in zip(now, mine))

    def send_far(k, c):
        far_copy(k).start()
        return c

    def join_near():
        one = jnp.ones((prow, LANES), F32)
        first = pair_up(1, twice(init_ref[0])), pair_up(2, twice(init_ref[1]))
        begin = tuple(jnp.where(a == 0, v, zero) for v in first) + (one, one, zero)
        plane = lax.fori_loop(0, near_upto, near_step, begin + begin)
        for i in range(5):
            held[i] = plane[5 + i]

        @pl.when(a < last)
        def _():
            far_out[pl.ds(0, prow), :] = plane[0].astype(BF16)
            far_out[pl.ds(prow, prow), :] = plane[1].astype(BF16)
            all_hi, all_lo, _ = split3(plane[2])
            far_out[pl.ds(2 * prow, prow), :] = all_hi
            far_out[pl.ds(3 * prow, prow), :] = all_lo

            @pl.when(b < inner - 1)
            def _():
                pl.semaphore_wait(far_ready, last - a)

            lax.fori_loop(a + 1, outer, send_far, 0)

    zero = jnp.zeros((prow, LANES), F32)
    in_copies[3].wait()

    @pl.when(b > 0)
    def _():
        join_near()

    def scan(t, h):
        m = mag[pl.ds(pl.multiple_of(t * prow, prow), prow), :]
        base = pl.multiple_of(t * pitch, 8)
        d_re = drv[pl.ds(base, prow), :]
        d_im = drv[pl.ds(base + prow, prow), :]
        f_re, f_im = m * turn[0], m * turn[1]
        new_re = (f_re * h[0] + d_re) - f_im * h[1]
        new_im = (f_re * h[1] + d_im) + f_im * h[0]
        drv[pl.ds(base, prow), :] = new_re
        drv[pl.ds(base + prow, prow), :] = new_im
        return new_re, new_im

    lax.fori_loop(0, rows, scan, (zero, zero), unroll=8)
    for k in range(blocks):
        cols = slice(k * LANES, (k + 1) * LANES)
        at = [half_row + k * quads + q for q in range(quads) for half_row in (0, prow)]
        st = jnp.concatenate(
            [drv[pl.ds(r, rows, stride=pitch), :].astype(BF16) for r in at], axis=1
        )
        read = jnp.dot(
            st, map_t[2 * k * bstates : 2 * (k + 1) * bstates, :], preferred_element_type=F32
        )
        pre[:, cols] = read + skip_ref[:, cols] * din[:, cols].astype(F32)

    @pl.when(b == 0)
    def _():
        join_near()

    @pl.when(sp == 0)
    def _():
        pad[pl.ds(0, 8), :] = jnp.zeros((8, cwide), F32)

    in_copies[8].wait()

    @pl.when(sp > 0)
    def _():
        tail_copy.wait_recv()

    conv = jnp.zeros((rows, cwide), F32)
    for k in range(width):
        conv = conv + pad[pl.ds(8 + k - (width - 1), rows), :] * taps_ref[k : k + 1, :].astype(F32)
    hc[0] = (hc[0].astype(F32) * conv).astype(BF16)
    hc_copy = remote(hc.at[0], hc.at[1], hc_sem.at[0], hc_sem.at[1], partner)
    hc_copy.start()
    for i in (0, 1):
        pltpu.make_async_copy((so_hbm, co_hbm)[i], ov.at[i], osem.at[i]).wait()
    oacc[...] = jnp.dot(hc[0], ov[1, :cwide], preferred_element_type=F32)
    whole_plane = cpow(whole, inner)

    def far_step(k, h):
        remote(
            far_out, far_in.at[k], far_send.at[k], far_recv.at[k], {"sp": k * inner + b, "tp": tp}
        ).wait_recv()
        k_mag = far_in[k, pl.ds(2 * prow, prow), :].astype(F32) + far_in[
            k, pl.ds(3 * prow, prow), :
        ].astype(F32)
        moved = cmul((whole_plane[0] * k_mag, whole_plane[1] * k_mag), h)
        k_re = far_in[k, pl.ds(0, prow), :].astype(F32)
        k_im = far_in[k, pl.ds(prow, prow), :].astype(F32)
        return moved[0] + k_re, moved[1] + k_im

    before = lax.fori_loop(0, a, far_step, (zero, zero))
    mine = [held[i] for i in range(5)]
    moved = cmul((mine[3] * mine[2], mine[4] * mine[2]), before)
    enter = (mine[0] + moved[0], mine[1] + moved[1])

    rowed[0] = enter[0]
    rowed[1] = enter[1]
    hs_copies = []
    for k in range(blocks):
        cols = slice(k * LANES, (k + 1) * LANES)
        turned = []
        for r in range(k * quads, (k + 1) * quads):
            c = tbl[:, 2 * r * LANES : (2 * r + 1) * LANES].astype(F32)
            d = tbl[:, (2 * r + 1) * LANES : (2 * r + 2) * LANES].astype(F32)
            turned += cmul((c, d), (rowed[0, r : r + 1, :], rowed[1, r : r + 1, :]))
        moved = jnp.dot(
            jnp.concatenate([v.astype(BF16) for v in turned], axis=1),
            map_t[2 * k * bstates : 2 * (k + 1) * bstates, :],
            preferred_element_type=F32,
        )
        hs[0, :, cols] = gelu(pre[:, cols] + chan_d[:, cols] * moved).astype(BF16)
        copy = remote(hs.at[0, :, cols], hs.at[1, :, cols], hs_sem.at[0, k], hs_sem.at[1, k], partner)
        copy.start()
        hs_copies.append(copy)
    oacc[...] += jnp.dot(hs[0], ov[0, :chans], preferred_element_type=F32)
    hc_copy.wait_recv()
    oacc[...] += jnp.dot(hc[1], ov[1, cwide:], preferred_element_type=F32)
    for copy in hs_copies:
        copy.wait_recv()
    out_ref[...] = (oacc[...] + jnp.dot(hs[1], ov[0, chans:], preferred_element_type=F32)).astype(BF16)

    x_copy.wait_send()
    hc_copy.wait_send()
    for copy in hs_copies:
        copy.wait_send()

    @pl.when(sp < n - 1)
    def _():
        tail_copy.wait_send()

    def near_sent(k, c):
        @pl.when(k != b)
        def _():
            near_copy(k).wait_send()

        return c

    def far_sent(k, c):
        far_copy(k).wait_send()
        return c

    lax.fori_loop(near_from, inner, near_sent, 0)
    lax.fori_loop(a + 1, outer, far_sent, 0)


def on_device(
    activations,
    norm_gain,
    state_proj,
    value_proj,
    post_gate_proj,
    pre_gate_proj,
    input_map,
    output_map,
    skip_gain,
    rotation,
    log_decay,
    initial_state,
    conv_taps,
    state_out,
    conv_out,
):
    n = lax.axis_size("sp")
    rows, half = activations.shape
    groups, state = rotation.shape
    chans = state_proj.shape[1]
    cwide = value_proj.shape[1]
    outs = state_out.shape[1]
    states = groups * state
    prow = states // LANES
    inner = inner_of(n)
    bdw = 2 * states // (chans // LANES)
    vmem = pl.BlockSpec(memory_space=pltpu.VMEM)
    hbm = pl.BlockSpec(memory_space=pl.ANY)
    dma = pltpu.SemaphoreType.DMA
    return pl.pallas_call(
        functools.partial(kernel, n),
        out_shape=pltpu.VMEM((rows, outs), BF16),
        in_specs=[hbm] * 15,
        out_specs=vmem,
        scratch_shapes=[
            pltpu.VMEM((rows, half), BF16),
            pltpu.VMEM((1, 2 * half), F32),
            pltpu.VMEM(input_map.shape, BF16),
            pltpu.VMEM((groups, output_map.shape[2], output_map.shape[1]), F32),
            pltpu.VMEM((1, chans), F32),
            pltpu.VMEM((groups, state), F32),
            pltpu.VMEM((groups, rows), F32),
            pltpu.VMEM(initial_state.shape, F32),
            pltpu.VMEM(conv_taps.shape, BF16),
            pltpu.VMEM((4, 2 * half, chans), BF16),
            pltpu.VMEM((2, 2 * chans, outs), BF16),
            pltpu.VMEM((rows, half), BF16),
            pltpu.VMEM((rows, 2 * half), BF16),
            pltpu.VMEM((rows, chans), BF16),
            pltpu.VMEM((chans, bdw), BF16),
            pltpu.VMEM((chans, bdw), BF16),
            pltpu.VMEM((2 * states, LANES), BF16),
            pltpu.VMEM((rows, 2 * states), BF16),
            pltpu.VMEM((2, 9 * prow, LANES), F32),
            pltpu.VMEM((rows, chans), F32),
            pltpu.VMEM((rows, chans), F32),
            pltpu.VMEM((rows, chans), F32),
            pltpu.VMEM((2, prow, LANES), F32),
            pltpu.VMEM((rows, chans), F32),
            pltpu.VMEM((5, prow, LANES), F32),
            pltpu.VMEM((rows, 2 * rows), BF16),
            pltpu.VMEM((groups, chans), BF16),
            pltpu.VMEM((rows * prow, LANES), F32),
            pltpu.VMEM((rows * (2 * prow + 8), LANES), F32),
            pltpu.VMEM((4 * groups, LANES), F32),
            pltpu.VMEM((rows + 8, cwide), F32),
            pltpu.VMEM((inner, 4 * prow, LANES), BF16),
            pltpu.VMEM((n // inner, 4 * prow, LANES), BF16),
            pltpu.VMEM((4 * prow, LANES), BF16),
            pltpu.VMEM((2, rows, chans), BF16),
            pltpu.VMEM((2, rows, cwide), BF16),
            pltpu.VMEM((rows, outs), F32),
            dma((9,)),
            dma((5,)),
            dma((2,)),
            dma((2,)),
            dma((2,)),
            dma((2,)),
            dma((2, chans // LANES)),
            dma((inner,)),
            dma((inner,)),
            dma((n // inner,)),
            dma((n // inner,)),
            pltpu.SemaphoreType.REGULAR,
            pltpu.SemaphoreType.REGULAR,
        ],
        compiler_params=pltpu.CompilerParams(collective_id=0, has_side_effects=True),
    )(
        activations,
        norm_gain.reshape(1, -1),
        state_proj,
        value_proj,
        post_gate_proj,
        pre_gate_proj,
        input_map,
        jnp.swapaxes(output_map, 1, 2),
        skip_gain.reshape(1, -1),
        rotation,
        jnp.swapaxes(log_decay, 0, 1),
        initial_state,
        conv_taps,
        state_out,
        conv_out,
    )


def solution(mesh):
    return jax.shard_map(
        on_device,
        mesh=mesh,
        in_specs=(
            P("sp", "tp"),
            P(),
            P(None, "tp"),
            P(None, "tp"),
            P(None, "tp"),
            P(None, "tp"),
            P("tp", None, None),
            P("tp", None, None),
            P("tp"),
            P("tp", None),
            P("sp", "tp"),
            P(None, "tp", None),
            P(None, "tp"),
            P(None, "tp"),
            P(None, "tp"),
        ),
        out_specs=P("sp", "tp"),
        check_vma=False,
    )
```

```python
import functools

import jax
import jax.numpy as jnp
from jax import lax
from jax.experimental import pallas as pl
from jax.experimental.pallas import tpu as pltpu
from jax.sharding import PartitionSpec as P

EPS = 1e-06
LANES = 128
MESH = pl.DeviceIdType.MESH
F32 = jnp.float32
BF16 = jnp.bfloat16


def minus_expm1(y):
    poly = jnp.ones_like(y)
    for k in range(11, 1, -1):
        poly = 1.0 + poly * y * (1.0 / k)
    return jnp.where(y > -0.5, -y * poly, 1.0 - jnp.exp(y))


def split3(v):
    hi = v.astype(BF16)
    rest = v - hi.astype(F32)
    mid = rest.astype(BF16)
    low = (rest - mid.astype(F32)).astype(BF16)
    return hi, mid, low


def cmul(a, b):
    return a[0] * b[0] - a[1] * b[1], a[0] * b[1] + a[1] * b[0]


def cpow(base, count):
    result = None
    while count:
        if count & 1:
            result = base if result is None else cmul(result, base)
        count >>= 1
        if count:
            base = cmul(base, base)
    return result


def inner_of(n):
    return max(d for d in range(1, n + 1) if n % d == 0 and d * d <= n)


def gelu(x):
    return 0.5 * x * (1.0 + jnp.tanh(0.7978845608028654 * (x + 0.044715 * x * x * x)))


def kernel(
    n,
    x_hbm,
    gain_hbm,
    w0_hbm,
    w1_hbm,
    w2_hbm,
    w3_hbm,
    imap_hbm,
    omap_hbm,
    skip_hbm,
    rot_hbm,
    ld_hbm,
    init_hbm,
    taps_hbm,
    so_hbm,
    co_hbm,
    out_ref,
    x_ref,
    gain_ref,
    imap_ref,
    omap_ref,
    skip_ref,
    rot_ref,
    ld_ref,
    init_ref,
    taps_ref,
    wv,
    ov,
    xr,
    acc,
    din,
    bd_in,
    bd_out,
    map_t,
    tbl,
    powers,
    chan_end,
    chan_gain,
    rowed,
    post,
    table_far,
    map_far,
    post_far,
    aux,
    aux_far,
    held,
    enter,
    sums,
    to_chan,
    mag,
    drv,
    pairs,
    pad,
    near_in,
    far_in,
    far_out,
    hs,
    hc,
    oacc,
    in_sem,
    wsem,
    osem,
    x_sem,
    tail_sem,
    hc_sem,
    hs_sem,
    near_send,
    near_recv,
    far_send,
    far_recv,
    aux_sem,
    enter_sem,
    dup_sem,
    near_ready,
    far_ready,
):
    sp, tp = lax.axis_index("sp"), lax.axis_index("tp")
    other = 1 - tp
    rows, half = x_ref.shape
    groups, state = rot_ref.shape
    gch = imap_ref.shape[1]
    chans = groups * gch
    states = groups * state
    prow = states // LANES
    per_block = LANES // gch
    blocks = groups // per_block
    quads = prow // blocks
    pitch = drv.shape[0] // rows
    bstates = quads * LANES
    cwide = taps_ref.shape[1]
    width = taps_ref.shape[0]

    barrier = pltpu.get_barrier_semaphore()
    partner = {"sp": sp, "tp": other}

    inner = inner_of(n)
    outer = n // inner
    a, b = lax.div(sp, inner), lax.rem(sp, inner)
    last = outer - 1

    hop_on = (b == inner - 1) & (a < last)

    def tell(sem, j):
        for t in (0, 1):
            pl.semaphore_signal(sem, inc=1, device_id={"sp": j, "tp": t}, device_id_type=MESH)

    def greet_near(k, c):
        tell(barrier, a * inner + k)
        return c

    def greet_far(k, c):
        tell(barrier, k * inner + b)
        return c

    pl.semaphore_signal(barrier, inc=1, device_id=partner, device_id_type=MESH)
    lax.fori_loop(b + 1, inner, greet_near, 0)

    lax.fori_loop(a + 1, outer, greet_far, 0)

    in_copies = {}
    def fetch(i, src, dst):
        in_copies[i] = pltpu.make_async_copy(src, dst, in_sem.at[i])
        in_copies[i].start()

    w_hbm = (w0_hbm, w1_hbm, w2_hbm, w3_hbm)

    def fetch_weight(i, h, sem):
        part = (tp, other)[h]
        pltpu.make_async_copy(
            w_hbm[i].at[pl.ds(part * half, half), :], wv.at[i, pl.ds(h * half, half), :], sem
        ).start()

    def wait_weight(i):
        pltpu.make_async_copy(w_hbm[i], wv.at[i], wsem.at[i]).wait()

    fetch(0, x_hbm, x_ref)
    fetch(4, ld_hbm, ld_ref)
    fetch(2, rot_hbm, rot_ref)
    fetch(5, imap_hbm, imap_ref)
    fetch(1, gain_hbm, gain_ref)
    fetch_weight(0, 0, wsem.at[0])
    fetch_weight(0, 1, wsem.at[4])

    pl.semaphore_wait(barrier, 1 + 2 * (b + a))

    def ready_near(k, c):
        tell(near_ready, a * inner + k)
        return c

    def ready_far(k, c):
        tell(far_ready, k * inner + b)
        return c

    @pl.when(tp == 1)
    def _():
        lax.fori_loop(0, b, ready_near, 0)


    lax.fori_loop(0, a, ready_far, 0)

    when = lax.broadcasted_iota(jnp.int32, (rows, 2 * rows), 0)
    upto = lax.broadcasted_iota(jnp.int32, (rows, 2 * rows), 1)
    sums[...] = jnp.where(
        ((upto < rows) & (when <= upto)) | ((upto >= rows) & (when > upto - rows)), 1.0, 0.0
    ).astype(BF16)
    col = lax.broadcasted_iota(jnp.int32, (groups, chans), 1)
    row = lax.broadcasted_iota(jnp.int32, (groups, chans), 0)
    to_chan[...] = jnp.where((col >= row * gch) & (col < (row + 1) * gch), 1.0, 0.0).astype(BF16)

    def remote(src, dst, s, r, dev):
        return pltpu.make_async_remote_copy(
            src_ref=src, dst_ref=dst, send_sem=s, recv_sem=r, device_id=dev, device_id_type=MESH
        )

    in_copies[0].wait()
    x_copy = remote(x_ref, xr, x_sem.at[0], x_sem.at[1], partner)
    x_copy.start()

    fetch(3, init_hbm, init_ref)
    fetch(6, omap_hbm, omap_ref)
    fetch(7, skip_hbm, skip_ref)
    fetch(8, taps_hbm, taps_ref)
    for i in (1, 3, 2):
        for h in (0, 1):
            fetch_weight(i, h, wsem.at[i])
    for i, w, deep in ((1, co_hbm, cwide), (0, so_hbm, chans)):
        for h, part in ((0, tp), (1, other)):
            pltpu.make_async_copy(
                w.at[pl.ds(part * deep, deep), :], ov.at[i, pl.ds(h * deep, deep), :], osem.at[i]
            ).start()

    lane = lax.broadcasted_iota(jnp.int32, (1, LANES), 1)

    def pair_up(i, v):
        pairs[pl.ds(i * groups, groups), :] = v
        even = pairs[pl.ds(i * groups, prow, stride=2), :]
        odd = pairs[pl.ds(i * groups + 1, prow, stride=2), :]
        return jnp.where(lane < state, even, odd)

    def twice(v):
        return jnp.concatenate([v, v], axis=1)

    for i in (4, 2, 5, 1):
        in_copies[i].wait()
    ld = ld_ref[...]

    def time_sums(cols):
        added = jnp.dot(jnp.concatenate(split3(ld), axis=0), sums[:, cols], preferred_element_type=F32)
        return added[:groups] + added[groups : 2 * groups] + added[2 * groups :]

    def per_channel(v):
        hi, mid, _ = split3(v.T)
        return jnp.dot(hi, to_chan[...], preferred_element_type=F32) + jnp.dot(
            mid, to_chan[...], preferred_element_type=F32
        )

    gain = jnp.sqrt(minus_expm1(2.0 * ld))
    chan_end[...] = per_channel(gain * jnp.exp(time_sums(slice(rows, 2 * rows))))
    tot = pair_up(
        3, jnp.broadcast_to(jnp.exp(jnp.sum(ld, axis=1, keepdims=True)), (groups, LANES))
    )
    theta = pair_up(0, twice(rot_ref[...]))
    turn = jnp.cos(theta), jnp.sin(theta)
    step = turn
    for k in range(8):
        for i in (0, 1):
            powers[i, pl.ds(k * prow, prow), :] = step[i]
        step = cmul(step, turn) if k < 7 else step
    far_step16 = cmul(step, step)
    for i in (0, 1):
        powers[i, pl.ds(8 * prow, prow), :] = far_step16[i]
    whole = cpow(step, rows // 8)
    for r in range(prow):
        even = [powers[i, pl.ds(r, 8, stride=prow), :] for i in (0, 1)]
        eight = [powers[i, pl.ds(7 * prow + r, 1), :] for i in (0, 1)]
        sixteen = [powers[i, pl.ds(8 * prow + r, 1), :] for i in (0, 1)]
        odd = cmul(even, eight)
        for t in range(0, rows, 16):
            for i in (0, 1):
                tbl[t : t + 16, (2 * r + i) * LANES : (2 * r + i + 1) * LANES] = jnp.concatenate(
                    [even[i], odd[i]], axis=0
                ).astype(BF16)
            even = cmul(even, sixteen)
            odd = cmul(odd, sixteen)

    def spread_map(src, dst):
        dst[...] = jnp.zeros_like(dst)
        for b in range(blocks):
            for q in range(quads):
                g = b * per_block + 2 * q
                one = src[g].astype(F32)
                two = src[g + 1].astype(F32)
                one_r = jnp.concatenate([one[:, state:], one[:, :state]], axis=1)
                two_r = jnp.concatenate([two[:, state:], two[:, :state]], axis=1)
                low = lane < state
                re = jnp.concatenate([jnp.where(low, one, 0.0), jnp.where(low, 0.0, two_r)], axis=0)
                im = jnp.concatenate([jnp.where(low, one_r, 0.0), jnp.where(low, 0.0, two)], axis=0)
                at = pl.ds(b * LANES + q * 2 * gch, 2 * gch)
                dst[at, 2 * q * LANES : (2 * q + 1) * LANES] = re.astype(BF16)
                dst[at, (2 * q + 1) * LANES : (2 * q + 2) * LANES] = im.astype(BF16)

    spread_map(imap_ref, bd_in)
    own = x_ref[...].astype(F32)
    scaled = (own * gain_ref[:, pl.ds(pl.multiple_of(tp * half, LANES), half)]).astype(BF16)
    squares = jnp.sum(own * own, axis=1, keepdims=True)
    half_copy = pltpu.make_async_copy(w_hbm[0].at[pl.ds(0, half), :], wv.at[0, pl.ds(0, half), :], wsem.at[0])
    half_copy.wait()
    partial = jnp.dot(scaled, wv[0, :half], preferred_element_type=F32)
    acc[:, :half] = scaled

    x_copy.wait_recv()
    far_x = xr[...].astype(F32)
    scaled_far = (far_x * gain_ref[:, pl.ds(pl.multiple_of(other * half, LANES), half)]).astype(BF16)
    squares = squares + jnp.sum(far_x * far_x, axis=1, keepdims=True)
    scale = lax.rsqrt(squares / (2 * half) + EPS)

    acc[:, half:] = scaled_far
    rest_copy = pltpu.make_async_copy(
        w_hbm[0].at[pl.ds(0, half), :], wv.at[0, pl.ds(half, half), :], wsem.at[4]
    )
    rest_copy.wait()
    total = partial + jnp.dot(scaled_far, wv[0, half:], preferred_element_type=F32)
    drive_in = (total * scale).astype(BF16)
    din[...] = drive_in
    ends_in = (drive_in.astype(F32) * chan_end[...]).astype(BF16).T
    for r in range(prow):
        q = r % quads
        at = slice(r * 2 * gch, (r + 1) * 2 * gch)
        seen = jnp.dot(
            ends_in[at], tbl[:, 2 * r * LANES : (2 * r + 2) * LANES], preferred_element_type=F32
        )
        m_re = bd_in[at, 2 * q * LANES : (2 * q + 1) * LANES].astype(F32)
        m_im = bd_in[at, (2 * q + 1) * LANES : (2 * q + 2) * LANES].astype(F32)
        c, d = seen[:, :LANES], seen[:, LANES:]
        rowed[0, r : r + 1, :] = jnp.sum(c * m_re + d * m_im, axis=0, keepdims=True)
        rowed[1, r : r + 1, :] = jnp.sum(c * m_im - d * m_re, axis=0, keepdims=True)
    e_re, e_im = cmul(whole, (rowed[0], rowed[1]))

    near_in[tp, b, pl.ds(0, prow), :] = e_re.astype(BF16)
    near_in[tp, b, pl.ds(prow, prow), :] = e_im.astype(BF16)
    fore = lax.rem(lax.broadcasted_iota(jnp.int32, (prow, LANES), 1), state) < state // 2

    def packed(v):
        hi, mid, _ = split3(v)
        return jnp.where(fore, hi.astype(F32), mid.astype(F32)).astype(BF16)

    near_in[tp, b, pl.ds(2 * prow, prow), :] = packed(tot)

    def near_copy(k):
        return remote(
            near_in.at[tp, b],
            near_in.at[tp, b],
            near_send.at[k],
            near_recv.at[tp, b],
            {"sp": a * inner + k, "tp": 1},
        )

    def far_copy(k):
        return remote(
            far_out, far_in.at[a], far_send.at[k], far_recv.at[a], {"sp": k * inner + b, "tp": 1}
        )

    near_from = jnp.where(a < last, 0, b + 1)
    near_upto = jnp.where(a < last, inner, b)
    after = inner - 1 - b

    @pl.when(after > 0)
    def _():
        pl.semaphore_wait(near_ready, after)

    def send_near(k, c):
        @pl.when((k != b) | ((tp == 0) & (a < last)))
        def _():
            near_copy(k).start()

        return c

    lax.fori_loop(near_from, inner, send_near, 0)

    in_copies[3].wait()
    aux[0], aux[1] = whole
    aux[2] = pair_up(1, twice(init_ref[0]))
    aux[3] = pair_up(2, twice(init_ref[1]))
    aux_copy = remote(aux, aux_far, aux_sem.at[0], aux_sem.at[1], partner)
    dup_copies = [
        remote(src, dst, dup_sem.at[0, i], dup_sem.at[1, i], partner)
        for i, (src, dst) in enumerate(((tbl, table_far), (map_t, map_far), (post, post_far)))
    ]

    def give(copy):
        @pl.when(tp == 0)
        def _():
            copy.start()

    give(aux_copy)

    def project(i):
        wait_weight(i)
        total = jnp.dot(acc[...], wv[i], preferred_element_type=F32)
        return (total * scale).astype(BF16)

    value = project(1)
    pre_gate = project(3)
    mixed = (pre_gate.astype(F32) * value.astype(F32)).astype(BF16).astype(F32)
    pad[pl.ds(8, rows), :] = mixed
    tail_copy = remote(
        pad.at[pl.ds(rows, 8), :],
        pad.at[pl.ds(0, 8), :],
        tail_sem.at[0],
        tail_sem.at[1],
        {"sp": lax.rem(sp + 1, n), "tp": tp},
    )

    @pl.when(hop_on)
    def _():
        pl.semaphore_wait(far_ready, 2 * (last - a))

    @pl.when(sp < n - 1)
    def _():
        tail_copy.start()

    give(dup_copies[0])

    for i in (6, 7):
        in_copies[i].wait()
    spread_map(omap_ref, bd_out)
    for k in range(blocks):
        map_t[2 * k * bstates : 2 * (k + 1) * bstates, :] = bd_out[k * LANES : (k + 1) * LANES, :].T
    give(dup_copies[1])

    ld = ld_ref[...]
    gain = jnp.sqrt(minus_expm1(2.0 * ld))
    late = per_channel(jnp.concatenate([jnp.exp(time_sums(slice(0, rows))), gain], axis=1))
    post[1] = late[:rows]
    chan_gain[...] = late[rows:]
    mags = split3(jnp.exp(ld).T)[:2]
    for k in range(blocks):
        col = lax.broadcasted_iota(jnp.int32, (groups, bstates), 1) + k * bstates
        row = lax.broadcasted_iota(jnp.int32, (groups, bstates), 0)
        spread = jnp.where(
            (col >= row * state) & (col < (row + 1) * state), 1.0, 0.0
        ).astype(BF16)
        m = jnp.dot(mags[0], spread, preferred_element_type=F32) + jnp.dot(
            mags[1], spread, preferred_element_type=F32
        )
        for q in range(quads):
            mag[pl.ds(k * quads + q, rows, stride=prow), :] = m[:, q * LANES : (q + 1) * LANES]

    hc[0] = project(2)
    gained = (din[...].astype(F32) * chan_gain[...]).astype(BF16)
    for k in range(blocks):
        blk = jnp.dot(
            gained[:, k * LANES : (k + 1) * LANES],
            bd_in[k * LANES : (k + 1) * LANES, :],
            preferred_element_type=F32,
        )
        for q in range(quads):
            r = k * quads + q
            drv[pl.ds(r, rows, stride=pitch), :] = blk[:, 2 * q * LANES : (2 * q + 1) * LANES]
            drv[pl.ds(prow + r, rows, stride=pitch), :] = blk[
                :, (2 * q + 1) * LANES : (2 * q + 2) * LANES
            ]

    zero = jnp.zeros((prow, LANES), F32)

    def message(ref):
        v = ref[pl.ds(2 * prow, prow), :].astype(F32)
        mags = v + jnp.where(fore, pltpu.roll(v, LANES - state // 2, 1), pltpu.roll(v, state // 2, 1))
        return ref[pl.ds(0, prow), :].astype(F32), ref[pl.ds(prow, prow), :].astype(F32), mags

    def send_far(k, c):
        far_copy(outer + a - k).start()
        return c

    def join_half(h, turned, first):
        def near_step(k, c):
            @pl.when((k != b) | (h == 0))
            def _():
                remote(
                    near_in.at[h, k],
                    near_in.at[h, k],
                    near_send.at[k],
                    near_recv.at[h, k],
                    {"sp": a * inner + k, "tp": 0},
                ).wait_recv()

            ends, mag_all, phase, mine = c[0:2], c[2], c[3:5], c[5:]
            k_re, k_im, k_mag = message(near_in.at[h, k])
            moved = cmul((turned[0] * k_mag, turned[1] * k_mag), ends)
            now = (moved[0] + k_re, moved[1] + k_im, mag_all * k_mag) + cmul(turned, phase)
            return now + tuple(jnp.where(k < b, v, w) for v, w in zip(now, mine))

        one = jnp.ones((prow, LANES), F32)
        begin = tuple(jnp.where(a == 0, v, zero) for v in first) + (one, one, zero)
        plane = lax.fori_loop(0, near_upto, near_step, begin + begin)
        for i in range(5):
            held[h, i] = plane[5 + i]
        far_out[h, pl.ds(0, prow), :] = plane[0].astype(BF16)
        far_out[h, pl.ds(prow, prow), :] = plane[1].astype(BF16)
        far_out[h, pl.ds(2 * prow, prow), :] = packed(plane[2])

    def join_near():
        @pl.when(tp == 1)
        def _():
            join_half(1, whole, (aux[2], aux[3]))
            join_half(0, (aux_far[0], aux_far[1]), (aux_far[2], aux_far[3]))

        @pl.when((a < last) & (b < inner - 1))
        def _():
            pl.semaphore_wait(far_ready, 2 * (last - a))

        @pl.when((tp == 1) & (a < last))
        def _():
            lax.fori_loop(a + 1, outer, send_far, 0)

    @pl.when(tp == 1)
    def _():
        aux_copy.wait_recv()

    @pl.when(b > 0)
    def _():
        join_near()

    def scan(t, h):
        m = mag[pl.ds(pl.multiple_of(t * prow, prow), prow), :]
        base = pl.multiple_of(t * pitch, 8)
        d_re = drv[pl.ds(base, prow), :]
        d_im = drv[pl.ds(base + prow, prow), :]
        f_re, f_im = m * turn[0], m * turn[1]
        new_re = (f_re * h[0] + d_re) - f_im * h[1]
        new_im = (f_re * h[1] + d_im) + f_im * h[0]
        drv[pl.ds(base, prow), :] = new_re
        drv[pl.ds(base + prow, prow), :] = new_im
        return new_re, new_im

    lax.fori_loop(0, rows, scan, (zero, zero), unroll=8)
    for k in range(blocks):
        cols = slice(k * LANES, (k + 1) * LANES)
        at = [half_row + k * quads + q for q in range(quads) for half_row in (0, prow)]
        st = jnp.concatenate(
            [drv[pl.ds(r, rows, stride=pitch), :].astype(BF16) for r in at], axis=1
        )
        read = jnp.dot(
            st, map_t[2 * k * bstates : 2 * (k + 1) * bstates, :], preferred_element_type=F32
        )
        post[0, :, cols] = read + skip_ref[:, cols] * din[:, cols].astype(F32)

    give(dup_copies[2])

    @pl.when(b == 0)
    def _():
        join_near()

    @pl.when(sp == 0)
    def _():
        pad[pl.ds(0, 8), :] = jnp.zeros((8, cwide), F32)

    in_copies[8].wait()

    @pl.when(sp > 0)
    def _():
        tail_copy.wait_recv()

    conv = jnp.zeros((rows, cwide), F32)
    for k in range(width):
        conv = conv + pad[pl.ds(8 + k - (width - 1), rows), :] * taps_ref[k : k + 1, :].astype(F32)
    hc[0] = (hc[0].astype(F32) * conv).astype(BF16)
    hc_copy = remote(hc.at[0], hc.at[1], hc_sem.at[0], hc_sem.at[1], partner)
    hc_copy.start()
    for i in (0, 1):
        pltpu.make_async_copy((so_hbm, co_hbm)[i], ov.at[i], osem.at[i]).wait()
    oacc[...] = jnp.dot(hc[0], ov[1, :cwide], preferred_element_type=F32)
    hc_copy.wait_recv()
    oacc[...] += jnp.dot(hc[1], ov[1, cwide:], preferred_element_type=F32)
    def entering(h, turned):
        plane_turn = cpow(turned, inner)

        def far_step(k, c):
            k_re, k_im, k_mag = message(far_in.at[k, h])
            moved = cmul((plane_turn[0] * k_mag, plane_turn[1] * k_mag), c)
            return moved[0] + k_re, moved[1] + k_im

        before = lax.fori_loop(0, a, far_step, (zero, zero))
        moved = cmul((held[h, 3] * held[h, 2], held[h, 4] * held[h, 2]), before)
        return held[h, 0] + moved[0], held[h, 1] + moved[1]

    def correct(h, table, mapped, local, slot):
        moved = []
        for k in range(blocks):
            turned = []
            for r in range(k * quads, (k + 1) * quads):
                c, d = (
                    table[:, (2 * r + i) * LANES : (2 * r + i + 1) * LANES].reshape(rows // 16, 16, LANES)
                    for i in (0, 1)
                )
                h_re, h_im = (
                    jnp.broadcast_to(enter[h, i, r : r + 1, :], (16, LANES)).astype(BF16)[None]
                    for i in (0, 1)
                )
                turned += cmul((c, d), (h_re, h_im))
            moved.append(
                jnp.dot(
                    jnp.concatenate([v.reshape(rows, LANES) for v in turned], axis=1),
                    mapped[2 * k * bstates : 2 * (k + 1) * bstates, :],
                    preferred_element_type=F32,
                )
            )
        for k in range(blocks):
            cols = slice(k * LANES, (k + 1) * LANES)
            hs[slot, :, cols] = gelu(local[0, :, cols] + local[1, :, cols] * moved[k]).astype(BF16)

    def far_arrival(k, c):
        far_from = remote(
            far_in.at[k], far_in.at[k], far_send.at[k], far_recv.at[k], {"sp": k * inner + b, "tp": 0}
        )
        far_from.wait_recv()
        return c

    enter_copy = remote(enter.at[0], enter.at[0], enter_sem.at[0], enter_sem.at[1], partner)

    @pl.when(tp == 1)
    def _():
        lax.fori_loop(0, a, far_arrival, 0)
        enter[0, 0], enter[0, 1] = entering(0, (aux_far[0], aux_far[1]))
        enter_copy.start()
        enter[1, 0], enter[1, 1] = entering(1, whole)

    @pl.when(tp == 0)
    def _():
        enter_copy.wait_recv()

    correct(tp, tbl, map_t, post, 0)
    hs_copy = remote(hs.at[0], hs.at[1], hs_sem.at[0], hs_sem.at[1], partner)

    @pl.when(tp == 1)
    def _():
        hs_copy.start()
        for copy in dup_copies:
            copy.wait_recv()
        correct(0, table_far, map_far, post_far, 1)

    oacc[...] += jnp.dot(hs[0], ov[0, :chans], preferred_element_type=F32)

    @pl.when(tp == 0)
    def _():
        hs_copy.wait_recv()

    out_ref[...] = (oacc[...] + jnp.dot(hs[1], ov[0, chans:], preferred_element_type=F32)).astype(BF16)

    x_copy.wait_send()
    hc_copy.wait_send()

    @pl.when(tp == 1)
    def _():
        hs_copy.wait_send()
        enter_copy.wait_send()

    @pl.when(tp == 0)
    def _():
        aux_copy.wait_send()
        for copy in dup_copies:
            copy.wait_send()

    @pl.when(sp < n - 1)
    def _():
        tail_copy.wait_send()

    def near_sent(k, c):
        @pl.when((k != b) | ((tp == 0) & (a < last)))
        def _():
            near_copy(k).wait_send()

        return c

    def far_sent(k, c):
        far_copy(k).wait_send()
        return c

    lax.fori_loop(near_from, inner, near_sent, 0)

    @pl.when(tp == 1)
    def _():
        lax.fori_loop(a + 1, outer, far_sent, 0)


def on_device(
    activations,
    norm_gain,
    state_proj,
    value_proj,
    post_gate_proj,
    pre_gate_proj,
    input_map,
    output_map,
    skip_gain,
    rotation,
    log_decay,
    initial_state,
    conv_taps,
    state_out,
    conv_out,
):
    n = lax.axis_size("sp")
    rows, half = activations.shape
    groups, state = rotation.shape
    chans = state_proj.shape[1]
    cwide = value_proj.shape[1]
    outs = state_out.shape[1]
    states = groups * state
    prow = states // LANES
    inner = inner_of(n)
    bdw = 2 * states // (chans // LANES)
    vmem = pl.BlockSpec(memory_space=pltpu.VMEM)
    hbm = pl.BlockSpec(memory_space=pl.ANY)
    dma = pltpu.SemaphoreType.DMA
    return pl.pallas_call(
        functools.partial(kernel, n),
        out_shape=pltpu.VMEM((rows, outs), BF16),
        in_specs=[hbm] * 15,
        out_specs=vmem,
        scratch_shapes=[
            pltpu.VMEM((rows, half), BF16),
            pltpu.VMEM((1, 2 * half), F32),
            pltpu.VMEM(input_map.shape, BF16),
            pltpu.VMEM((groups, output_map.shape[2], output_map.shape[1]), F32),
            pltpu.VMEM((1, chans), F32),
            pltpu.VMEM((groups, state), F32),
            pltpu.VMEM((groups, rows), F32),
            pltpu.VMEM(initial_state.shape, F32),
            pltpu.VMEM(conv_taps.shape, BF16),
            pltpu.VMEM((4, 2 * half, chans), BF16),
            pltpu.VMEM((2, 2 * chans, outs), BF16),
            pltpu.VMEM((rows, half), BF16),
            pltpu.VMEM((rows, 2 * half), BF16),
            pltpu.VMEM((rows, chans), BF16),
            pltpu.VMEM((chans, bdw), BF16),
            pltpu.VMEM((chans, bdw), BF16),
            pltpu.VMEM((2 * states, LANES), BF16),
            pltpu.VMEM((rows, 2 * states), BF16),
            pltpu.VMEM((2, 9 * prow, LANES), F32),
            pltpu.VMEM((rows, chans), F32),
            pltpu.VMEM((rows, chans), F32),
            pltpu.VMEM((2, prow, LANES), F32),
            pltpu.VMEM((2, rows, chans), F32),
            pltpu.VMEM((rows, 2 * states), BF16),
            pltpu.VMEM((2 * states, LANES), BF16),
            pltpu.VMEM((2, rows, chans), F32),
            pltpu.VMEM((4, prow, LANES), F32),
            pltpu.VMEM((4, prow, LANES), F32),
            pltpu.VMEM((2, 5, prow, LANES), F32),
            pltpu.VMEM((2, 2, prow, LANES), F32),
            pltpu.VMEM((rows, 2 * rows), BF16),
            pltpu.VMEM((groups, chans), BF16),
            pltpu.VMEM((rows * prow, LANES), F32),
            pltpu.VMEM((rows * (2 * prow + 8), LANES), F32),
            pltpu.VMEM((4 * groups, LANES), F32),
            pltpu.VMEM((rows + 8, cwide), F32),
            pltpu.VMEM((2, inner, 3 * prow, LANES), BF16),
            pltpu.VMEM((n // inner, 2, 3 * prow, LANES), BF16),
            pltpu.VMEM((2, 3 * prow, LANES), BF16),
            pltpu.VMEM((2, rows, chans), BF16),
            pltpu.VMEM((2, rows, cwide), BF16),
            pltpu.VMEM((rows, outs), F32),
            dma((9,)),
            dma((5,)),
            dma((2,)),
            dma((2,)),
            dma((2,)),
            dma((2,)),
            dma((2,)),
            dma((inner,)),
            dma((2, inner)),
            dma((n // inner,)),
            dma((n // inner,)),
            dma((2,)),
            dma((2,)),
            dma((2, 3)),
            pltpu.SemaphoreType.REGULAR,
            pltpu.SemaphoreType.REGULAR,
        ],
        compiler_params=pltpu.CompilerParams(collective_id=0, has_side_effects=True),
    )(
        activations,
        norm_gain.reshape(1, -1),
        state_proj,
        value_proj,
        post_gate_proj,
        pre_gate_proj,
        input_map,
        jnp.swapaxes(output_map, 1, 2),
        skip_gain.reshape(1, -1),
        rotation,
        jnp.swapaxes(log_decay, 0, 1),
        initial_state,
        conv_taps,
        state_out,
        conv_out,
    )


def solution(mesh):
    return jax.shard_map(
        on_device,
        mesh=mesh,
        in_specs=(
            P("sp", "tp"),
            P(),
            P(None, "tp"),
            P(None, "tp"),
            P(None, "tp"),
            P(None, "tp"),
            P("tp", None, None),
            P("tp", None, None),
            P("tp"),
            P("tp", None),
            P("sp", "tp"),
            P(None, "tp", None),
            P(None, "tp"),
            P(None, "tp"),
            P(None, "tp"),
        ),
        out_specs=P("sp", "tp"),
        check_vma=False,
    )
```

```python
import functools

import jax
import jax.numpy as jnp
from jax import lax
from jax.experimental import pallas as pl
from jax.experimental.pallas import tpu as pltpu
from jax.sharding import PartitionSpec as P

EPS = 1e-06
LANES = 128
MESH = pl.DeviceIdType.MESH
F32 = jnp.float32
BF16 = jnp.bfloat16


def minus_expm1(y):
    poly = jnp.ones_like(y)
    for k in range(11, 1, -1):
        poly = 1.0 + poly * y * (1.0 / k)
    return jnp.where(y > -0.5, -y * poly, 1.0 - jnp.exp(y))


def split3(v):
    hi = v.astype(BF16)
    rest = v - hi.astype(F32)
    mid = rest.astype(BF16)
    low = (rest - mid.astype(F32)).astype(BF16)
    return hi, mid, low


def cmul(a, b):
    return a[0] * b[0] - a[1] * b[1], a[0] * b[1] + a[1] * b[0]


def cpow(base, count):
    result = None
    while count:
        if count & 1:
            result = base if result is None else cmul(result, base)
        count >>= 1
        if count:
            base = cmul(base, base)
    return result


def inner_of(n):
    return max(d for d in range(1, n + 1) if n % d == 0 and d * d <= n)


def gelu(x):
    return 0.5 * x * (1.0 + jnp.tanh(0.7978845608028654 * (x + 0.044715 * x * x * x)))


def kernel(
    n,
    x_hbm,
    gain_hbm,
    w0_hbm,
    w1_hbm,
    w2_hbm,
    w3_hbm,
    imap_hbm,
    omap_hbm,
    skip_hbm,
    rot_hbm,
    ld_hbm,
    init_hbm,
    taps_hbm,
    so_hbm,
    co_hbm,
    out_ref,
    x_ref,
    gain_ref,
    imap_ref,
    omap_ref,
    skip_ref,
    rot_ref,
    ld_ref,
    init_ref,
    taps_ref,
    wv,
    ov,
    xr,
    acc,
    din,
    bd_in,
    bd_out,
    map_t,
    tbl,
    powers,
    chan_end,
    chan_gain,
    rowed,
    post,
    table_far,
    map_far,
    post_far,
    aux,
    aux_far,
    mags_in,
    held,
    enter,
    sums,
    to_chan,
    mag,
    drv,
    pairs,
    pad,
    near_in,
    far_in,
    far_out,
    hs,
    hc,
    oacc,
    in_sem,
    wsem,
    osem,
    x_sem,
    tail_sem,
    hc_sem,
    hs_sem,
    near_send,
    near_recv,
    far_send,
    far_recv,
    aux_sem,
    enter_sem,
    dup_sem,
    near_ready,
    far_ready,
):
    sp, tp = lax.axis_index("sp"), lax.axis_index("tp")
    other = 1 - tp
    rows, half = x_ref.shape
    groups, state = rot_ref.shape
    gch = imap_ref.shape[1]
    chans = groups * gch
    states = groups * state
    prow = states // LANES
    per_block = LANES // gch
    blocks = groups // per_block
    quads = prow // blocks
    pitch = drv.shape[0] // rows
    bstates = quads * LANES
    cwide = taps_ref.shape[1]
    width = taps_ref.shape[0]

    barrier = pltpu.get_barrier_semaphore()
    partner = {"sp": sp, "tp": other}

    inner = inner_of(n)
    outer = n // inner
    a, b = lax.div(sp, inner), lax.rem(sp, inner)
    last = outer - 1

    hop_on = (b == inner - 1) & (a < last)

    def tell(sem, j):
        for t in (0, 1):
            pl.semaphore_signal(sem, inc=1, device_id={"sp": j, "tp": t}, device_id_type=MESH)

    def greet_near(k, c):
        tell(barrier, a * inner + k)
        return c

    def greet_far(k, c):
        tell(barrier, k * inner + b)
        return c

    pl.semaphore_signal(barrier, inc=1, device_id=partner, device_id_type=MESH)
    lax.fori_loop(b + 1, inner, greet_near, 0)

    lax.fori_loop(a + 1, outer, greet_far, 0)

    in_copies = {}
    def fetch(i, src, dst):
        in_copies[i] = pltpu.make_async_copy(src, dst, in_sem.at[i])
        in_copies[i].start()

    w_hbm = (w0_hbm, w1_hbm, w2_hbm, w3_hbm)

    def fetch_weight(i, h, sem):
        part = (tp, other)[h]
        pltpu.make_async_copy(
            w_hbm[i].at[pl.ds(part * half, half), :], wv.at[i, pl.ds(h * half, half), :], sem
        ).start()

    def wait_weight(i):
        pltpu.make_async_copy(w_hbm[i], wv.at[i], wsem.at[i]).wait()

    fetch(0, x_hbm, x_ref)
    fetch(4, ld_hbm, ld_ref)
    fetch(2, rot_hbm, rot_ref)
    fetch(5, imap_hbm, imap_ref)
    fetch(1, gain_hbm, gain_ref)
    fetch_weight(0, 0, wsem.at[0])
    fetch_weight(0, 1, wsem.at[4])

    pl.semaphore_wait(barrier, 1 + 2 * (b + a))

    def ready_near(k, c):
        tell(near_ready, a * inner + k)
        return c

    def ready_far(k, c):
        tell(far_ready, k * inner + b)
        return c

    @pl.when(tp == 1)
    def _():
        lax.fori_loop(0, b, ready_near, 0)


    lax.fori_loop(0, a, ready_far, 0)

    when = lax.broadcasted_iota(jnp.int32, (rows, 2 * rows), 0)
    upto = lax.broadcasted_iota(jnp.int32, (rows, 2 * rows), 1)
    sums[...] = jnp.where(
        ((upto < rows) & (when <= upto)) | ((upto >= rows) & (when > upto - rows)), 1.0, 0.0
    ).astype(BF16)
    col = lax.broadcasted_iota(jnp.int32, (groups, chans), 1)
    row = lax.broadcasted_iota(jnp.int32, (groups, chans), 0)
    to_chan[...] = jnp.where((col >= row * gch) & (col < (row + 1) * gch), 1.0, 0.0).astype(BF16)

    def remote(src, dst, s, r, dev):
        return pltpu.make_async_remote_copy(
            src_ref=src, dst_ref=dst, send_sem=s, recv_sem=r, device_id=dev, device_id_type=MESH
        )

    in_copies[0].wait()
    x_copy = remote(x_ref, xr, x_sem.at[0], x_sem.at[1], partner)
    x_copy.start()

    fetch(3, init_hbm, init_ref)
    fetch(6, omap_hbm, omap_ref)
    fetch(7, skip_hbm, skip_ref)
    fetch(8, taps_hbm, taps_ref)
    for i in (1, 3, 2):
        for h in (0, 1):
            fetch_weight(i, h, wsem.at[i])
    for i, w, deep in ((1, co_hbm, cwide), (0, so_hbm, chans)):
        for h, part in ((0, tp), (1, other)):
            pltpu.make_async_copy(
                w.at[pl.ds(part * deep, deep), :], ov.at[i, pl.ds(h * deep, deep), :], osem.at[i]
            ).start()

    lane = lax.broadcasted_iota(jnp.int32, (1, LANES), 1)

    def pair_up(i, v):
        pairs[pl.ds(i * groups, groups), :] = v
        even = pairs[pl.ds(i * groups, prow, stride=2), :]
        odd = pairs[pl.ds(i * groups + 1, prow, stride=2), :]
        return jnp.where(lane < state, even, odd)

    def twice(v):
        return jnp.concatenate([v, v], axis=1)

    for i in (4, 2, 5, 1):
        in_copies[i].wait()
    ld = ld_ref[...]

    def time_sums(cols):
        added = jnp.dot(jnp.concatenate(split3(ld), axis=0), sums[:, cols], preferred_element_type=F32)
        return added[:groups] + added[groups : 2 * groups] + added[2 * groups :]

    def per_channel(v):
        hi, mid, _ = split3(v.T)
        return jnp.dot(hi, to_chan[...], preferred_element_type=F32) + jnp.dot(
            mid, to_chan[...], preferred_element_type=F32
        )

    gain = jnp.sqrt(minus_expm1(2.0 * ld))
    chan_end[...] = per_channel(gain * jnp.exp(time_sums(slice(rows, 2 * rows))))
    tot = pair_up(
        3, jnp.broadcast_to(jnp.exp(jnp.sum(ld, axis=1, keepdims=True)), (groups, LANES))
    )
    theta = pair_up(0, twice(rot_ref[...]))
    turn = jnp.cos(theta), jnp.sin(theta)
    step = turn
    for k in range(8):
        for i in (0, 1):
            powers[i, pl.ds(k * prow, prow), :] = step[i]
        step = cmul(step, turn) if k < 7 else step
    far_step16 = cmul(step, step)
    for i in (0, 1):
        powers[i, pl.ds(8 * prow, prow), :] = far_step16[i]
    whole = cpow(step, rows // 8)
    for r in range(prow):
        even = [powers[i, pl.ds(r, 8, stride=prow), :] for i in (0, 1)]
        eight = [powers[i, pl.ds(7 * prow + r, 1), :] for i in (0, 1)]
        sixteen = [powers[i, pl.ds(8 * prow + r, 1), :] for i in (0, 1)]
        odd = cmul(even, eight)
        for t in range(0, rows, 16):
            for i in (0, 1):
                tbl[t : t + 16, (2 * r + i) * LANES : (2 * r + i + 1) * LANES] = jnp.concatenate(
                    [even[i], odd[i]], axis=0
                ).astype(BF16)
            even = cmul(even, sixteen)
            odd = cmul(odd, sixteen)

    def spread_map(src, dst):
        dst[...] = jnp.zeros_like(dst)
        for b in range(blocks):
            for q in range(quads):
                g = b * per_block + 2 * q
                one = src[g].astype(F32)
                two = src[g + 1].astype(F32)
                one_r = jnp.concatenate([one[:, state:], one[:, :state]], axis=1)
                two_r = jnp.concatenate([two[:, state:], two[:, :state]], axis=1)
                low = lane < state
                re = jnp.concatenate([jnp.where(low, one, 0.0), jnp.where(low, 0.0, two_r)], axis=0)
                im = jnp.concatenate([jnp.where(low, one_r, 0.0), jnp.where(low, 0.0, two)], axis=0)
                at = pl.ds(b * LANES + q * 2 * gch, 2 * gch)
                dst[at, 2 * q * LANES : (2 * q + 1) * LANES] = re.astype(BF16)
                dst[at, (2 * q + 1) * LANES : (2 * q + 2) * LANES] = im.astype(BF16)

    spread_map(imap_ref, bd_in)
    own = x_ref[...].astype(F32)
    scaled = (own * gain_ref[:, pl.ds(pl.multiple_of(tp * half, LANES), half)]).astype(BF16)
    squares = jnp.sum(own * own, axis=1, keepdims=True)
    half_copy = pltpu.make_async_copy(w_hbm[0].at[pl.ds(0, half), :], wv.at[0, pl.ds(0, half), :], wsem.at[0])
    half_copy.wait()
    partial = jnp.dot(scaled, wv[0, :half], preferred_element_type=F32)
    acc[:, :half] = scaled

    x_copy.wait_recv()
    far_x = xr[...].astype(F32)
    scaled_far = (far_x * gain_ref[:, pl.ds(pl.multiple_of(other * half, LANES), half)]).astype(BF16)
    squares = squares + jnp.sum(far_x * far_x, axis=1, keepdims=True)
    scale = lax.rsqrt(squares / (2 * half) + EPS)

    acc[:, half:] = scaled_far
    rest_copy = pltpu.make_async_copy(
        w_hbm[0].at[pl.ds(0, half), :], wv.at[0, pl.ds(half, half), :], wsem.at[4]
    )
    rest_copy.wait()
    total = partial + jnp.dot(scaled_far, wv[0, half:], preferred_element_type=F32)
    drive_in = (total * scale).astype(BF16)
    din[...] = drive_in
    ends_in = (drive_in.astype(F32) * chan_end[...]).astype(BF16).T
    for r in range(prow):
        q = r % quads
        at = slice(r * 2 * gch, (r + 1) * 2 * gch)
        seen = jnp.dot(
            ends_in[at], tbl[:, 2 * r * LANES : (2 * r + 2) * LANES], preferred_element_type=F32
        )
        m_re = bd_in[at, 2 * q * LANES : (2 * q + 1) * LANES].astype(F32)
        m_im = bd_in[at, (2 * q + 1) * LANES : (2 * q + 2) * LANES].astype(F32)
        c, d = seen[:, :LANES], seen[:, LANES:]
        rowed[0, r : r + 1, :] = jnp.sum(c * m_re + d * m_im, axis=0, keepdims=True)
        rowed[1, r : r + 1, :] = jnp.sum(c * m_im - d * m_re, axis=0, keepdims=True)
    e_re, e_im = cmul(whole, (rowed[0], rowed[1]))

    near_in[tp, b, pl.ds(0, prow), :] = e_re.astype(BF16)
    near_in[tp, b, pl.ds(prow, prow), :] = e_im.astype(BF16)
    fore = lax.rem(lax.broadcasted_iota(jnp.int32, (prow, LANES), 1), state) < state // 2

    def packed(v):
        hi, mid, _ = split3(v)
        return jnp.where(fore, hi.astype(F32), mid.astype(F32)).astype(BF16)

    near_in[tp, b, pl.ds(2 * prow, prow), :] = packed(tot)

    def near_copy(k):
        return remote(
            near_in.at[tp, b],
            near_in.at[tp, b],
            near_send.at[k],
            near_recv.at[tp, b],
            {"sp": a * inner + k, "tp": 1},
        )

    def far_copy(k):
        return remote(
            far_out, far_in.at[a], far_send.at[k], far_recv.at[a], {"sp": k * inner + b, "tp": 1}
        )

    near_from = jnp.where(a < last, 0, b + 1)
    near_upto = jnp.where(a < last, inner, b)
    after = inner - 1 - b

    @pl.when(after > 0)
    def _():
        pl.semaphore_wait(near_ready, after)

    def send_near(k, c):
        @pl.when((k != b) | ((tp == 0) & (a < last)))
        def _():
            near_copy(k).start()

        return c

    lax.fori_loop(near_from, inner, send_near, 0)

    in_copies[3].wait()
    aux[0], aux[1] = whole
    aux[2] = pair_up(1, twice(init_ref[0]))
    aux[3] = pair_up(2, twice(init_ref[1]))
    aux_copy = remote(aux, aux_far, aux_sem.at[0], aux_sem.at[1], partner)
    dup_copies = [
        remote(src, dst, dup_sem.at[0, i], dup_sem.at[1, i], partner)
        for i, (src, dst) in enumerate(
            (
                (tbl, table_far),
                (map_t, map_far),
                (post.at[1], post_far.at[1]),
                (post.at[0], post_far.at[0]),
            )
        )
    ]

    def give(copy):
        @pl.when(tp == 0)
        def _():
            copy.start()

    give(aux_copy)

    def project(i):
        wait_weight(i)
        total = jnp.dot(acc[...], wv[i], preferred_element_type=F32)
        return (total * scale).astype(BF16)

    value = project(1)
    pre_gate = project(3)
    mixed = (pre_gate.astype(F32) * value.astype(F32)).astype(BF16).astype(F32)
    pad[pl.ds(8, rows), :] = mixed
    tail_copy = remote(
        pad.at[pl.ds(rows, 8), :],
        pad.at[pl.ds(0, 8), :],
        tail_sem.at[0],
        tail_sem.at[1],
        {"sp": lax.rem(sp + 1, n), "tp": tp},
    )

    @pl.when(hop_on)
    def _():
        pl.semaphore_wait(far_ready, 2 * (last - a))

    @pl.when(sp < n - 1)
    def _():
        tail_copy.start()

    give(dup_copies[0])

    for i in (6, 7):
        in_copies[i].wait()
    spread_map(omap_ref, bd_out)
    for k in range(blocks):
        map_t[2 * k * bstates : 2 * (k + 1) * bstates, :] = bd_out[k * LANES : (k + 1) * LANES, :].T
    give(dup_copies[1])

    ld = ld_ref[...]
    gain = jnp.sqrt(minus_expm1(2.0 * ld))
    late = per_channel(jnp.concatenate([jnp.exp(time_sums(slice(0, rows))), gain], axis=1))
    post[1] = late[:rows]
    give(dup_copies[2])
    chan_gain[...] = late[rows:]
    mags = split3(jnp.exp(ld).T)[:2]
    for k in range(blocks):
        col = lax.broadcasted_iota(jnp.int32, (groups, bstates), 1) + k * bstates
        row = lax.broadcasted_iota(jnp.int32, (groups, bstates), 0)
        spread = jnp.where(
            (col >= row * state) & (col < (row + 1) * state), 1.0, 0.0
        ).astype(BF16)
        m = jnp.dot(mags[0], spread, preferred_element_type=F32) + jnp.dot(
            mags[1], spread, preferred_element_type=F32
        )
        for q in range(quads):
            mag[pl.ds(k * quads + q, rows, stride=prow), :] = m[:, q * LANES : (q + 1) * LANES]

    zero = jnp.zeros((prow, LANES), F32)

    def unpacked(v):
        v = v.astype(F32)
        keep = lax.rem(lax.broadcasted_iota(jnp.int32, v.shape, 1), state) < state // 2
        return v + jnp.where(keep, pltpu.roll(v, LANES - state // 2, 1), pltpu.roll(v, state // 2, 1))

    def unpack_all(ref, h, count, index):
        packs = jnp.concatenate([ref[index(h, k) + (pl.ds(2 * prow, prow),)] for k in range(count)], axis=0)
        mags_in[h, : count * prow, :] = unpacked(packs)

    def message(ref, h, k):
        return (
            ref[pl.ds(0, prow), :].astype(F32),
            ref[pl.ds(prow, prow), :].astype(F32),
            mags_in[h, pl.ds(pl.multiple_of(k * prow, prow), prow), :],
        )

    def send_far(k, c):
        far_copy(outer + a - k).start()
        return c

    def near_arrival(h):
        def arrival(k, c):
            @pl.when((k != b) | (h == 0))
            def _():
                remote(
                    near_in.at[h, k],
                    near_in.at[h, k],
                    near_send.at[k],
                    near_recv.at[h, k],
                    {"sp": a * inner + k, "tp": 0},
                ).wait_recv()

            return c

        lax.fori_loop(0, near_upto, arrival, 0)

    def join_half(h, turned, first):
        unpack_all(near_in, h, inner, lambda h, k: (h, k))

        def near_step(k, c):
            ends, mag_all, phase, mine = c[0:2], c[2], c[3:5], c[5:]
            k_re, k_im, k_mag = message(near_in.at[h, k], h, k)
            moved = cmul((turned[0] * k_mag, turned[1] * k_mag), ends)
            now = (moved[0] + k_re, moved[1] + k_im, mag_all * k_mag) + cmul(turned, phase)
            return now + tuple(jnp.where(k < b, v, w) for v, w in zip(now, mine))

        one = jnp.ones((prow, LANES), F32)
        begin = tuple(jnp.where(a == 0, v, zero) for v in first) + (one, one, zero)
        plane = lax.fori_loop(0, near_upto, near_step, begin + begin)
        for i in range(5):
            held[h, i] = plane[5 + i]
        far_out[h, pl.ds(0, prow), :] = plane[0].astype(BF16)
        far_out[h, pl.ds(prow, prow), :] = plane[1].astype(BF16)
        far_out[h, pl.ds(2 * prow, prow), :] = packed(plane[2])

    def join_near():
        @pl.when(tp == 1)
        def _():
            near_arrival(1)
            near_arrival(0)
            join_half(1, whole, (aux[2], aux[3]))
            join_half(0, (aux_far[0], aux_far[1]), (aux_far[2], aux_far[3]))

        @pl.when((a < last) & (b < inner - 1))
        def _():
            pl.semaphore_wait(far_ready, 2 * (last - a))

        @pl.when((tp == 1) & (a < last))
        def _():
            lax.fori_loop(a + 1, outer, send_far, 0)

    @pl.when(tp == 1)
    def _():
        aux_copy.wait_recv()

    @pl.when(b > 1)
    def _():
        join_near()

    hc[0] = project(2)
    gained = (din[...].astype(F32) * chan_gain[...]).astype(BF16)
    for k in range(blocks):
        blk = jnp.dot(
            gained[:, k * LANES : (k + 1) * LANES],
            bd_in[k * LANES : (k + 1) * LANES, :],
            preferred_element_type=F32,
        )
        for q in range(quads):
            r = k * quads + q
            drv[pl.ds(r, rows, stride=pitch), :] = blk[:, 2 * q * LANES : (2 * q + 1) * LANES]
            drv[pl.ds(prow + r, rows, stride=pitch), :] = blk[
                :, (2 * q + 1) * LANES : (2 * q + 2) * LANES
            ]

    @pl.when(b == 1)
    def _():
        join_near()

    def scan(t, h):
        m = mag[pl.ds(pl.multiple_of(t * prow, prow), prow), :]
        base = pl.multiple_of(t * pitch, 8)
        d_re = drv[pl.ds(base, prow), :]
        d_im = drv[pl.ds(base + prow, prow), :]
        f_re, f_im = m * turn[0], m * turn[1]
        new_re = (f_re * h[0] + d_re) - f_im * h[1]
        new_im = (f_re * h[1] + d_im) + f_im * h[0]
        drv[pl.ds(base, prow), :] = new_re
        drv[pl.ds(base + prow, prow), :] = new_im
        return new_re, new_im

    lax.fori_loop(0, rows, scan, (zero, zero), unroll=8)
    for k in range(blocks):
        cols = slice(k * LANES, (k + 1) * LANES)
        at = [half_row + k * quads + q for q in range(quads) for half_row in (0, prow)]
        st = jnp.concatenate(
            [drv[pl.ds(r, rows, stride=pitch), :].astype(BF16) for r in at], axis=1
        )
        read = jnp.dot(
            st, map_t[2 * k * bstates : 2 * (k + 1) * bstates, :], preferred_element_type=F32
        )
        post[0, :, cols] = read + skip_ref[:, cols] * din[:, cols].astype(F32)

    @pl.when(b == 0)
    def _():
        give(dup_copies[3])

    @pl.when(b == 0)
    def _():
        join_near()

    @pl.when(sp == 0)
    def _():
        pad[pl.ds(0, 8), :] = jnp.zeros((8, cwide), F32)

    in_copies[8].wait()

    @pl.when(sp > 0)
    def _():
        tail_copy.wait_recv()

    conv = jnp.zeros((rows, cwide), F32)
    for k in range(width):
        conv = conv + pad[pl.ds(8 + k - (width - 1), rows), :] * taps_ref[k : k + 1, :].astype(F32)
    hc[0] = (hc[0].astype(F32) * conv).astype(BF16)
    hc_copy = remote(hc.at[0], hc.at[1], hc_sem.at[0], hc_sem.at[1], partner)
    hc_copy.start()

    @pl.when(b > 0)
    def _():
        give(dup_copies[3])

    for i in (0, 1):
        pltpu.make_async_copy((so_hbm, co_hbm)[i], ov.at[i], osem.at[i]).wait()
    oacc[...] = jnp.dot(hc[0], ov[1, :cwide], preferred_element_type=F32)

    def add_far_conv():
        hc_copy.wait_recv()
        oacc[...] += jnp.dot(hc[1], ov[1, cwide:], preferred_element_type=F32)

    @pl.when(b > 0)
    def _():
        add_far_conv()

    def entering(h, turned):
        plane_turn = cpow(turned, inner)

        unpack_all(far_in, h, last, lambda h, k: (k, h))

        def far_step(k, c):
            k_re, k_im, k_mag = message(far_in.at[k, h], h, k)
            moved = cmul((plane_turn[0] * k_mag, plane_turn[1] * k_mag), c)
            return moved[0] + k_re, moved[1] + k_im

        before = lax.fori_loop(0, a, far_step, (zero, zero))
        moved = cmul((held[h, 3] * held[h, 2], held[h, 4] * held[h, 2]), before)
        return held[h, 0] + moved[0], held[h, 1] + moved[1]

    def correct(h, table, mapped, local, slot):
        moved = []
        for k in range(blocks):
            turned = []
            for r in range(k * quads, (k + 1) * quads):
                c, d = (
                    table[:, (2 * r + i) * LANES : (2 * r + i + 1) * LANES].reshape(rows // 16, 16, LANES)
                    for i in (0, 1)
                )
                h_re, h_im = (
                    jnp.broadcast_to(enter[h, i, r : r + 1, :], (16, LANES)).astype(BF16)[None]
                    for i in (0, 1)
                )
                turned += cmul((c, d), (h_re, h_im))
            moved.append(
                jnp.dot(
                    jnp.concatenate([v.reshape(rows, LANES) for v in turned], axis=1),
                    mapped[2 * k * bstates : 2 * (k + 1) * bstates, :],
                    preferred_element_type=F32,
                )
            )
        for k in range(blocks):
            cols = slice(k * LANES, (k + 1) * LANES)
            hs[slot, :, cols] = gelu(local[0, :, cols] + local[1, :, cols] * moved[k]).astype(BF16)

    def far_arrival(k, c):
        far_from = remote(
            far_in.at[k], far_in.at[k], far_send.at[k], far_recv.at[k], {"sp": k * inner + b, "tp": 0}
        )
        far_from.wait_recv()
        return c

    enter_copy = remote(enter.at[0], enter.at[0], enter_sem.at[0], enter_sem.at[1], partner)

    @pl.when(tp == 1)
    def _():
        lax.fori_loop(0, a, far_arrival, 0)
        enter[0, 0], enter[0, 1] = entering(0, (aux_far[0], aux_far[1]))
        enter_copy.start()
        enter[1, 0], enter[1, 1] = entering(1, whole)

    @pl.when(tp == 0)
    def _():
        enter_copy.wait_recv()

    correct(tp, tbl, map_t, post, 0)
    hs_copy = remote(hs.at[0], hs.at[1], hs_sem.at[0], hs_sem.at[1], partner)

    @pl.when(tp == 1)
    def _():
        hs_copy.start()
        for copy in dup_copies:
            copy.wait_recv()
        correct(0, table_far, map_far, post_far, 1)

    oacc[...] += jnp.dot(hs[0], ov[0, :chans], preferred_element_type=F32)

    @pl.when(b == 0)
    def _():
        add_far_conv()

    @pl.when(tp == 0)
    def _():
        hs_copy.wait_recv()

    out_ref[...] = (oacc[...] + jnp.dot(hs[1], ov[0, chans:], preferred_element_type=F32)).astype(BF16)

    x_copy.wait_send()
    hc_copy.wait_send()

    @pl.when(tp == 1)
    def _():
        hs_copy.wait_send()
        enter_copy.wait_send()

    @pl.when(tp == 0)
    def _():
        aux_copy.wait_send()
        for copy in dup_copies:
            copy.wait_send()

    @pl.when(sp < n - 1)
    def _():
        tail_copy.wait_send()

    def near_sent(k, c):
        @pl.when((k != b) | ((tp == 0) & (a < last)))
        def _():
            near_copy(k).wait_send()

        return c

    def far_sent(k, c):
        far_copy(k).wait_send()
        return c

    lax.fori_loop(near_from, inner, near_sent, 0)

    @pl.when(tp == 1)
    def _():
        lax.fori_loop(a + 1, outer, far_sent, 0)


def on_device(
    activations,
    norm_gain,
    state_proj,
    value_proj,
    post_gate_proj,
    pre_gate_proj,
    input_map,
    output_map,
    skip_gain,
    rotation,
    log_decay,
    initial_state,
    conv_taps,
    state_out,
    conv_out,
):
    n = lax.axis_size("sp")
    rows, half = activations.shape
    groups, state = rotation.shape
    chans = state_proj.shape[1]
    cwide = value_proj.shape[1]
    outs = state_out.shape[1]
    states = groups * state
    prow = states // LANES
    inner = inner_of(n)
    bdw = 2 * states // (chans // LANES)
    vmem = pl.BlockSpec(memory_space=pltpu.VMEM)
    hbm = pl.BlockSpec(memory_space=pl.ANY)
    dma = pltpu.SemaphoreType.DMA
    return pl.pallas_call(
        functools.partial(kernel, n),
        out_shape=pltpu.VMEM((rows, outs), BF16),
        in_specs=[hbm] * 15,
        out_specs=vmem,
        scratch_shapes=[
            pltpu.VMEM((rows, half), BF16),
            pltpu.VMEM((1, 2 * half), F32),
            pltpu.VMEM(input_map.shape, BF16),
            pltpu.VMEM((groups, output_map.shape[2], output_map.shape[1]), F32),
            pltpu.VMEM((1, chans), F32),
            pltpu.VMEM((groups, state), F32),
            pltpu.VMEM((groups, rows), F32),
            pltpu.VMEM(initial_state.shape, F32),
            pltpu.VMEM(conv_taps.shape, BF16),
            pltpu.VMEM((4, 2 * half, chans), BF16),
            pltpu.VMEM((2, 2 * chans, outs), BF16),
            pltpu.VMEM((rows, half), BF16),
            pltpu.VMEM((rows, 2 * half), BF16),
            pltpu.VMEM((rows, chans), BF16),
            pltpu.VMEM((chans, bdw), BF16),
            pltpu.VMEM((chans, bdw), BF16),
            pltpu.VMEM((2 * states, LANES), BF16),
            pltpu.VMEM((rows, 2 * states), BF16),
            pltpu.VMEM((2, 9 * prow, LANES), F32),
            pltpu.VMEM((rows, chans), F32),
            pltpu.VMEM((rows, chans), F32),
            pltpu.VMEM((2, prow, LANES), F32),
            pltpu.VMEM((2, rows, chans), F32),
            pltpu.VMEM((rows, 2 * states), BF16),
            pltpu.VMEM((2 * states, LANES), BF16),
            pltpu.VMEM((2, rows, chans), F32),
            pltpu.VMEM((4, prow, LANES), F32),
            pltpu.VMEM((4, prow, LANES), F32),
            pltpu.VMEM((2, max(inner, n // inner) * prow, LANES), F32),
            pltpu.VMEM((2, 5, prow, LANES), F32),
            pltpu.VMEM((2, 2, prow, LANES), F32),
            pltpu.VMEM((rows, 2 * rows), BF16),
            pltpu.VMEM((groups, chans), BF16),
            pltpu.VMEM((rows * prow, LANES), F32),
            pltpu.VMEM((rows * (2 * prow + 8), LANES), F32),
            pltpu.VMEM((4 * groups, LANES), F32),
            pltpu.VMEM((rows + 8, cwide), F32),
            pltpu.VMEM((2, inner, 3 * prow, LANES), BF16),
            pltpu.VMEM((n // inner, 2, 3 * prow, LANES), BF16),
            pltpu.VMEM((2, 3 * prow, LANES), BF16),
            pltpu.VMEM((2, rows, chans), BF16),
            pltpu.VMEM((2, rows, cwide), BF16),
            pltpu.VMEM((rows, outs), F32),
            dma((9,)),
            dma((5,)),
            dma((2,)),
            dma((2,)),
            dma((2,)),
            dma((2,)),
            dma((2,)),
            dma((inner,)),
            dma((2, inner)),
            dma((n // inner,)),
            dma((n // inner,)),
            dma((2,)),
            dma((2,)),
            dma((2, 4)),
            pltpu.SemaphoreType.REGULAR,
            pltpu.SemaphoreType.REGULAR,
        ],
        compiler_params=pltpu.CompilerParams(collective_id=0, has_side_effects=True),
    )(
        activations,
        norm_gain.reshape(1, -1),
        state_proj,
        value_proj,
        post_gate_proj,
        pre_gate_proj,
        input_map,
        jnp.swapaxes(output_map, 1, 2),
        skip_gain.reshape(1, -1),
        rotation,
        jnp.swapaxes(log_decay, 0, 1),
        initial_state,
        conv_taps,
        state_out,
        conv_out,
    )


def solution(mesh):
    return jax.shard_map(
        on_device,
        mesh=mesh,
        in_specs=(
            P("sp", "tp"),
            P(),
            P(None, "tp"),
            P(None, "tp"),
            P(None, "tp"),
            P(None, "tp"),
            P("tp", None, None),
            P("tp", None, None),
            P("tp"),
            P("tp", None),
            P("sp", "tp"),
            P(None, "tp", None),
            P(None, "tp"),
            P(None, "tp"),
            P(None, "tp"),
        ),
        out_specs=P("sp", "tp"),
        check_vma=False,
    )
```

```python
import functools

import jax
import jax.numpy as jnp
from jax import lax
from jax.experimental import pallas as pl
from jax.experimental.pallas import tpu as pltpu
from jax.sharding import PartitionSpec as P

EPS = 1e-06
LANES = 128
MESH = pl.DeviceIdType.MESH
F32 = jnp.float32
BF16 = jnp.bfloat16


def minus_expm1(y):
    poly = jnp.ones_like(y)
    for k in range(11, 1, -1):
        poly = 1.0 + poly * y * (1.0 / k)
    return jnp.where(y > -0.5, -y * poly, 1.0 - jnp.exp(y))


def split3(v):
    hi = v.astype(BF16)
    rest = v - hi.astype(F32)
    mid = rest.astype(BF16)
    low = (rest - mid.astype(F32)).astype(BF16)
    return hi, mid, low


def cmul(a, b):
    return a[0] * b[0] - a[1] * b[1], a[0] * b[1] + a[1] * b[0]


def cpow(base, count):
    result = None
    while count:
        if count & 1:
            result = base if result is None else cmul(result, base)
        count >>= 1
        if count:
            base = cmul(base, base)
    return result


def inner_of(n):
    return max(d for d in range(1, n + 1) if n % d == 0 and d * d <= n)


def gelu(x):
    return 0.5 * x * (1.0 + jnp.tanh(0.7978845608028654 * (x + 0.044715 * x * x * x)))


def kernel(
    n,
    x_hbm,
    gain_hbm,
    w0_hbm,
    w1_hbm,
    w2_hbm,
    w3_hbm,
    imap_hbm,
    omap_hbm,
    skip_hbm,
    rot_hbm,
    ld_hbm,
    init_hbm,
    taps_hbm,
    so_hbm,
    co_hbm,
    out_ref,
    x_ref,
    gain_ref,
    imap_ref,
    omap_ref,
    skip_ref,
    rot_ref,
    ld_ref,
    init_ref,
    taps_ref,
    wv,
    ov,
    xr,
    acc,
    din,
    bd_in,
    bd_out,
    map_t,
    tbl,
    powers,
    chan_end,
    chan_gain,
    rowed,
    post,
    table_far,
    map_far,
    post_far,
    aux,
    aux_far,
    mags_in,
    held,
    enter,
    sums,
    to_chan,
    mag,
    drv,
    pairs,
    pad,
    near_in,
    far_in,
    far_out,
    hs,
    hc,
    oacc,
    in_sem,
    wsem,
    osem,
    x_sem,
    tail_sem,
    hc_sem,
    hs_sem,
    near_sem,
    far_sem,
    aux_sem,
    enter_sem,
    dup_sem,
    near_ready,
    far_ready,
):
    sp, tp = lax.axis_index("sp"), lax.axis_index("tp")
    other = 1 - tp
    rows, half = x_ref.shape
    groups, state = rot_ref.shape
    gch = imap_ref.shape[1]
    chans = groups * gch
    states = groups * state
    prow = states // LANES
    per_block = LANES // gch
    blocks = groups // per_block
    quads = prow // blocks
    pitch = drv.shape[0] // rows
    bstates = quads * LANES
    cwide = taps_ref.shape[1]
    width = taps_ref.shape[0]

    barrier = pltpu.get_barrier_semaphore()
    partner = {"sp": sp, "tp": other}

    inner = inner_of(n)
    outer = n // inner
    a, b = lax.div(sp, inner), lax.rem(sp, inner)
    last = outer - 1

    hop_on = (b == inner - 1) & (a < last)

    def tell(sem, j):
        for t in (0, 1):
            pl.semaphore_signal(sem, inc=1, device_id={"sp": j, "tp": t}, device_id_type=MESH)

    def greet_near(k, c):
        tell(barrier, a * inner + k)
        return c

    def greet_far(k, c):
        tell(barrier, k * inner + b)
        return c

    pl.semaphore_signal(barrier, inc=1, device_id=partner, device_id_type=MESH)
    lax.fori_loop(b + 1, inner, greet_near, 0)

    lax.fori_loop(a + 1, outer, greet_far, 0)

    in_copies = {}
    def fetch(i, src, dst):
        in_copies[i] = pltpu.make_async_copy(src, dst, in_sem.at[i])
        in_copies[i].start()

    w_hbm = (w0_hbm, w1_hbm, w2_hbm, w3_hbm)

    def fetch_weight(i, h, sem):
        part = (tp, other)[h]
        pltpu.make_async_copy(
            w_hbm[i].at[pl.ds(part * half, half), :], wv.at[i, pl.ds(h * half, half), :], sem
        ).start()

    def wait_weight(i):
        pltpu.make_async_copy(w_hbm[i], wv.at[i], wsem.at[i]).wait()

    fetch(0, x_hbm, x_ref)
    fetch(4, ld_hbm, ld_ref)
    fetch(2, rot_hbm, rot_ref)
    fetch(5, imap_hbm, imap_ref)
    fetch(1, gain_hbm, gain_ref)
    fetch_weight(0, 0, wsem.at[0])
    fetch_weight(0, 1, wsem.at[0])

    pl.semaphore_wait(barrier, 1 + 2 * (b + a))

    def ready_near(k, c):
        tell(near_ready, a * inner + k)
        return c

    def ready_far(k, c):
        tell(far_ready, k * inner + b)
        return c

    @pl.when(tp == 1)
    def _():
        lax.fori_loop(0, b, ready_near, 0)


    lax.fori_loop(0, a, ready_far, 0)

    when = lax.broadcasted_iota(jnp.int32, (rows, 2 * rows), 0)
    upto = lax.broadcasted_iota(jnp.int32, (rows, 2 * rows), 1)
    sums[...] = jnp.where(
        ((upto < rows) & (when <= upto)) | ((upto >= rows) & (when > upto - rows)), 1.0, 0.0
    ).astype(BF16)
    col = lax.broadcasted_iota(jnp.int32, (groups, chans), 1)
    row = lax.broadcasted_iota(jnp.int32, (groups, chans), 0)
    to_chan[...] = jnp.where((col >= row * gch) & (col < (row + 1) * gch), 1.0, 0.0).astype(BF16)

    def remote(src, dst, s, r, dev):
        return pltpu.make_async_remote_copy(
            src_ref=src, dst_ref=dst, send_sem=s, recv_sem=r, device_id=dev, device_id_type=MESH
        )

    in_copies[0].wait()
    x_copy = remote(x_ref, xr, x_sem.at[0], x_sem.at[1], partner)
    x_copy.start()

    fetch(3, init_hbm, init_ref)
    fetch(6, omap_hbm, omap_ref)
    fetch(7, skip_hbm, skip_ref)
    fetch(8, taps_hbm, taps_ref)
    for i in (1, 3, 2):
        for h in (0, 1):
            fetch_weight(i, h, wsem.at[i])
    for i, w, deep in ((1, co_hbm, cwide), (0, so_hbm, chans)):
        for h, part in ((0, tp), (1, other)):
            pltpu.make_async_copy(
                w.at[pl.ds(part * deep, deep), :], ov.at[pl.ds(2 * i * chans + h * deep, deep), :], osem.at[0]
            ).start()

    lane = lax.broadcasted_iota(jnp.int32, (1, LANES), 1)

    def pair_up(i, v):
        pairs[pl.ds(i * groups, groups), :] = v
        even = pairs[pl.ds(i * groups, prow, stride=2), :]
        odd = pairs[pl.ds(i * groups + 1, prow, stride=2), :]
        return jnp.where(lane < state, even, odd)

    def twice(v):
        return jnp.concatenate([v, v], axis=1)

    for i in (4, 2, 5, 1):
        in_copies[i].wait()
    ld = ld_ref[...]

    def time_sums(cols):
        added = jnp.dot(jnp.concatenate(split3(ld), axis=0), sums[:, cols], preferred_element_type=F32)
        return added[:groups] + added[groups : 2 * groups] + added[2 * groups :]

    def per_channel(v):
        hi, mid, _ = split3(v.T)
        return jnp.dot(hi, to_chan[...], preferred_element_type=F32) + jnp.dot(
            mid, to_chan[...], preferred_element_type=F32
        )

    gain = jnp.sqrt(minus_expm1(2.0 * ld))
    chan_end[...] = per_channel(gain * jnp.exp(time_sums(slice(rows, 2 * rows))))
    tot = pair_up(
        3, jnp.broadcast_to(jnp.exp(jnp.sum(ld, axis=1, keepdims=True)), (groups, LANES))
    )
    theta = pair_up(0, twice(rot_ref[...]))
    turn = jnp.cos(theta), jnp.sin(theta)
    step = turn
    for k in range(8):
        for i in (0, 1):
            powers[i, pl.ds(k * prow, prow), :] = step[i]
        step = cmul(step, turn) if k < 7 else step
    far_step16 = cmul(step, step)
    for i in (0, 1):
        powers[i, pl.ds(8 * prow, prow), :] = far_step16[i]
    whole = cpow(step, rows // 8)
    for r in range(prow):
        even = [powers[i, pl.ds(r, 8, stride=prow), :] for i in (0, 1)]
        eight = [powers[i, pl.ds(7 * prow + r, 1), :] for i in (0, 1)]
        sixteen = [powers[i, pl.ds(8 * prow + r, 1), :] for i in (0, 1)]
        odd = cmul(even, eight)
        for t in range(0, rows, 16):
            for i in (0, 1):
                tbl[t : t + 16, (2 * r + i) * LANES : (2 * r + i + 1) * LANES] = jnp.concatenate(
                    [even[i], odd[i]], axis=0
                ).astype(BF16)
            even = cmul(even, sixteen)
            odd = cmul(odd, sixteen)

    def spread_map(src, dst):
        dst[...] = jnp.zeros_like(dst)
        for b in range(blocks):
            for q in range(quads):
                g = b * per_block + 2 * q
                one = src[g].astype(F32)
                two = src[g + 1].astype(F32)
                one_r = jnp.concatenate([one[:, state:], one[:, :state]], axis=1)
                two_r = jnp.concatenate([two[:, state:], two[:, :state]], axis=1)
                low = lane < state
                re = jnp.concatenate([jnp.where(low, one, 0.0), jnp.where(low, 0.0, two_r)], axis=0)
                im = jnp.concatenate([jnp.where(low, one_r, 0.0), jnp.where(low, 0.0, two)], axis=0)
                at = pl.ds(b * LANES + q * 2 * gch, 2 * gch)
                dst[at, 2 * q * LANES : (2 * q + 1) * LANES] = re.astype(BF16)
                dst[at, (2 * q + 1) * LANES : (2 * q + 2) * LANES] = im.astype(BF16)

    spread_map(imap_ref, bd_in)
    own = x_ref[...].astype(F32)
    scaled = (own * gain_ref[:, pl.ds(pl.multiple_of(tp * half, LANES), half)]).astype(BF16)
    squares = jnp.sum(own * own, axis=1, keepdims=True)
    wait_weight(0)
    partial = jnp.dot(scaled, wv[0, :half], preferred_element_type=F32)
    acc[:, :half] = scaled

    x_copy.wait_recv()
    far_x = xr[...].astype(F32)
    scaled_far = (far_x * gain_ref[:, pl.ds(pl.multiple_of(other * half, LANES), half)]).astype(BF16)
    squares = squares + jnp.sum(far_x * far_x, axis=1, keepdims=True)
    scale = lax.rsqrt(squares / (2 * half) + EPS)

    acc[:, half:] = scaled_far
    total = partial + jnp.dot(scaled_far, wv[0, half:], preferred_element_type=F32)
    drive_in = (total * scale).astype(BF16)
    din[...] = drive_in
    ends_in = (drive_in.astype(F32) * chan_end[...]).astype(BF16).T
    for r in range(prow):
        q = r % quads
        at = slice(r * 2 * gch, (r + 1) * 2 * gch)
        seen = jnp.dot(
            ends_in[at], tbl[:, 2 * r * LANES : (2 * r + 2) * LANES], preferred_element_type=F32
        )
        m_re = bd_in[at, 2 * q * LANES : (2 * q + 1) * LANES].astype(F32)
        m_im = bd_in[at, (2 * q + 1) * LANES : (2 * q + 2) * LANES].astype(F32)
        c, d = seen[:, :LANES], seen[:, LANES:]
        rowed[0, r : r + 1, :] = jnp.sum(c * m_re + d * m_im, axis=0, keepdims=True)
        rowed[1, r : r + 1, :] = jnp.sum(c * m_im - d * m_re, axis=0, keepdims=True)
    e_re, e_im = cmul(whole, (rowed[0], rowed[1]))

    near_in[tp, b, pl.ds(0, prow), :] = e_re.astype(BF16)
    near_in[tp, b, pl.ds(prow, prow), :] = e_im.astype(BF16)
    fore = lax.rem(lax.broadcasted_iota(jnp.int32, (prow, LANES), 1), state) < state // 2

    def packed(v):
        hi, mid, _ = split3(v)
        return jnp.where(fore, hi.astype(F32), mid.astype(F32)).astype(BF16)

    near_in[tp, b, pl.ds(2 * prow, prow), :] = packed(tot)

    def wait_many(ref, sems, count, upto, sent):
        for j in range(1, upto + 1):
            @pl.when(count == j)
            def _():
                part = ref.at[pl.ds(0, j)]
                copy = remote(part, part, sems[0], sems[1], partner)
                copy.wait_send() if sent else copy.wait_recv()

    def near_copy(k):
        return remote(
            near_in.at[tp, b],
            near_in.at[tp, b],
            near_sem.at[2],
            near_sem.at[tp],
            {"sp": a * inner + k, "tp": 1},
        )

    def far_copy(k):
        return remote(
            far_out, far_in.at[a], far_sem.at[0], far_sem.at[1], {"sp": k * inner + b, "tp": 1}
        )

    near_from = jnp.where(a < last, 0, b + 1)
    near_upto = jnp.where(a < last, inner, b)
    after = inner - 1 - b

    @pl.when(after > 0)
    def _():
        pl.semaphore_wait(near_ready, after)

    def send_near(k, c):
        @pl.when((k != b) | ((tp == 0) & (a < last)))
        def _():
            near_copy(k).start()

        return c

    lax.fori_loop(near_from, inner, send_near, 0)

    in_copies[3].wait()
    aux[0], aux[1] = whole
    aux[2] = pair_up(1, twice(init_ref[0]))
    aux[3] = pair_up(2, twice(init_ref[1]))
    aux_copy = remote(aux, aux_far, aux_sem.at[0], aux_sem.at[1], partner)
    dup_copies = [
        remote(src, dst, dup_sem.at[0, min(i, 2)], dup_sem.at[1, min(i, 2)], partner)
        for i, (src, dst) in enumerate(
            (
                (tbl, table_far),
                (map_t, map_far),
                (post.at[1], post_far.at[1]),
                (post.at[0], post_far.at[0]),
            )
        )
    ]

    def give(copy):
        @pl.when(tp == 0)
        def _():
            copy.start()

    waited = dup_copies[:2] + [
        remote(post, post_far, dup_sem.at[0, 2], dup_sem.at[1, 2], partner)
    ]

    give(aux_copy)

    def project(i):
        wait_weight(i)
        total = jnp.dot(acc[...], wv[i], preferred_element_type=F32)
        return (total * scale).astype(BF16)

    value = project(1)
    pre_gate = project(3)
    mixed = (pre_gate.astype(F32) * value.astype(F32)).astype(BF16).astype(F32)
    pad[pl.ds(8, rows), :] = mixed
    tail_copy = remote(
        pad.at[pl.ds(rows, 8), :],
        pad.at[pl.ds(0, 8), :],
        tail_sem.at[0],
        tail_sem.at[1],
        {"sp": lax.rem(sp + 1, n), "tp": tp},
    )

    @pl.when(hop_on)
    def _():
        pl.semaphore_wait(far_ready, 2 * (last - a))

    @pl.when(sp < n - 1)
    def _():
        tail_copy.start()

    give(dup_copies[0])

    for i in (6, 7):
        in_copies[i].wait()
    spread_map(omap_ref, bd_out)
    for k in range(blocks):
        map_t[2 * k * bstates : 2 * (k + 1) * bstates, :] = bd_out[k * LANES : (k + 1) * LANES, :].T
    give(dup_copies[1])

    ld = ld_ref[...]
    gain = jnp.sqrt(minus_expm1(2.0 * ld))
    late = per_channel(jnp.concatenate([jnp.exp(time_sums(slice(0, rows))), gain], axis=1))
    post[1] = late[:rows]
    give(dup_copies[2])
    chan_gain[...] = late[rows:]
    mags = split3(jnp.exp(ld).T)[:2]
    for k in range(blocks):
        col = lax.broadcasted_iota(jnp.int32, (groups, bstates), 1) + k * bstates
        row = lax.broadcasted_iota(jnp.int32, (groups, bstates), 0)
        spread = jnp.where(
            (col >= row * state) & (col < (row + 1) * state), 1.0, 0.0
        ).astype(BF16)
        m = jnp.dot(mags[0], spread, preferred_element_type=F32) + jnp.dot(
            mags[1], spread, preferred_element_type=F32
        )
        for q in range(quads):
            mag[pl.ds(k * quads + q, rows, stride=prow), :] = m[:, q * LANES : (q + 1) * LANES]

    zero = jnp.zeros((prow, LANES), F32)

    def unpacked(v):
        v = v.astype(F32)
        keep = lax.rem(lax.broadcasted_iota(jnp.int32, v.shape, 1), state) < state // 2
        return v + jnp.where(keep, pltpu.roll(v, LANES - state // 2, 1), pltpu.roll(v, state // 2, 1))

    def unpack_all(ref, h, count, index):
        packs = jnp.concatenate([ref[index(h, k) + (pl.ds(2 * prow, prow),)] for k in range(count)], axis=0)
        mags_in[h, : count * prow, :] = unpacked(packs)

    def message(ref, h, k):
        return (
            ref[pl.ds(0, prow), :].astype(F32),
            ref[pl.ds(prow, prow), :].astype(F32),
            mags_in[h, pl.ds(pl.multiple_of(k * prow, prow), prow), :],
        )

    def send_far(k, c):
        far_copy(outer + a - k).start()
        return c

    def join_half(h, turned, first):
        unpack_all(near_in, h, inner, lambda h, k: (h, k))

        def near_step(k, c):
            ends, mag_all, phase, mine = c[0:2], c[2], c[3:5], c[5:]
            k_re, k_im, k_mag = message(near_in.at[h, k], h, k)
            moved = cmul((turned[0] * k_mag, turned[1] * k_mag), ends)
            now = (moved[0] + k_re, moved[1] + k_im, mag_all * k_mag) + cmul(turned, phase)
            return now + tuple(jnp.where(k < b, v, w) for v, w in zip(now, mine))

        one = jnp.ones((prow, LANES), F32)
        begin = tuple(jnp.where(a == 0, v, zero) for v in first) + (one, one, zero)
        plane = lax.fori_loop(0, near_upto, near_step, begin + begin)
        for i in range(5):
            held[h, i] = plane[5 + i]
        far_out[h, pl.ds(0, prow), :] = plane[0].astype(BF16)
        far_out[h, pl.ds(prow, prow), :] = plane[1].astype(BF16)
        far_out[h, pl.ds(2 * prow, prow), :] = packed(plane[2])

    def join_near():
        @pl.when(tp == 1)
        def _():
            for h in (1, 0):
                wait_many(
                    near_in.at[h],
                    (near_sem.at[2], near_sem.at[h]),
                    jnp.where(a < last, inner - h, b),
                    inner,
                    False,
                )
            join_half(1, whole, (aux[2], aux[3]))
            join_half(0, (aux_far[0], aux_far[1]), (aux_far[2], aux_far[3]))

        @pl.when((a < last) & (b < inner - 1))
        def _():
            pl.semaphore_wait(far_ready, 2 * (last - a))

        @pl.when((tp == 1) & (a < last))
        def _():
            lax.fori_loop(a + 1, outer, send_far, 0)

    @pl.when(tp == 1)
    def _():
        aux_copy.wait_recv()

    @pl.when(b > 1)
    def _():
        join_near()

    hc[0] = project(2)
    gained = (din[...].astype(F32) * chan_gain[...]).astype(BF16)
    for k in range(blocks):
        blk = jnp.dot(
            gained[:, k * LANES : (k + 1) * LANES],
            bd_in[k * LANES : (k + 1) * LANES, :],
            preferred_element_type=F32,
        )
        for q in range(quads):
            r = k * quads + q
            drv[pl.ds(r, rows, stride=pitch), :] = blk[:, 2 * q * LANES : (2 * q + 1) * LANES]
            drv[pl.ds(prow + r, rows, stride=pitch), :] = blk[
                :, (2 * q + 1) * LANES : (2 * q + 2) * LANES
            ]

    @pl.when(b == 1)
    def _():
        join_near()

    hc_copy = remote(hc.at[0], hc.at[1], hc_sem.at[0], hc_sem.at[1], partner)

    def convolve():
        @pl.when(sp == 0)
        def _():
            pad[pl.ds(0, 8), :] = jnp.zeros((8, cwide), F32)

        in_copies[8].wait()

        @pl.when(sp > 0)
        def _():
            tail_copy.wait_recv()

        conv = jnp.zeros((rows, cwide), F32)
        for k in range(width):
            conv = conv + pad[pl.ds(8 + k - (width - 1), rows), :] * taps_ref[k : k + 1, :].astype(F32)
        hc[0] = (hc[0].astype(F32) * conv).astype(BF16)
        hc_copy.start()

    @pl.when(b > 0)
    def _():
        convolve()

    def scan(t, h):
        m = mag[pl.ds(pl.multiple_of(t * prow, prow), prow), :]
        base = pl.multiple_of(t * pitch, 8)
        d_re = drv[pl.ds(base, prow), :]
        d_im = drv[pl.ds(base + prow, prow), :]
        f_re, f_im = m * turn[0], m * turn[1]
        new_re = (f_re * h[0] + d_re) - f_im * h[1]
        new_im = (f_re * h[1] + d_im) + f_im * h[0]
        drv[pl.ds(base, prow), :] = new_re
        drv[pl.ds(base + prow, prow), :] = new_im
        return new_re, new_im

    lax.fori_loop(0, rows, scan, (zero, zero), unroll=8)
    for k in range(blocks):
        cols = slice(k * LANES, (k + 1) * LANES)
        at = [half_row + k * quads + q for q in range(quads) for half_row in (0, prow)]
        st = jnp.concatenate(
            [drv[pl.ds(r, rows, stride=pitch), :].astype(BF16) for r in at], axis=1
        )
        read = jnp.dot(
            st, map_t[2 * k * bstates : 2 * (k + 1) * bstates, :], preferred_element_type=F32
        )
        post[0, :, cols] = read + skip_ref[:, cols] * din[:, cols].astype(F32)

    give(dup_copies[3])

    @pl.when(b == 0)
    def _():
        join_near()

    @pl.when(b == 0)
    def _():
        convolve()

    pltpu.make_async_copy(ov, ov, osem.at[0]).wait()
    oacc[...] = jnp.dot(hc[0], ov[2 * chans : 2 * chans + cwide], preferred_element_type=F32)

    def add_far_conv():
        hc_copy.wait_recv()
        oacc[...] += jnp.dot(hc[1], ov[2 * chans + cwide :], preferred_element_type=F32)

    @pl.when(b > 0)
    def _():
        add_far_conv()

    def entering(h, turned):
        plane_turn = cpow(turned, inner)

        unpack_all(far_in, h, last, lambda h, k: (k, h))

        def far_step(k, c):
            k_re, k_im, k_mag = message(far_in.at[k, h], h, k)
            moved = cmul((plane_turn[0] * k_mag, plane_turn[1] * k_mag), c)
            return moved[0] + k_re, moved[1] + k_im

        before = lax.fori_loop(0, a, far_step, (zero, zero))
        moved = cmul((held[h, 3] * held[h, 2], held[h, 4] * held[h, 2]), before)
        return held[h, 0] + moved[0], held[h, 1] + moved[1]

    def correct(h, table, mapped, local, slot):
        moved = []
        for k in range(blocks):
            turned = []
            for r in range(k * quads, (k + 1) * quads):
                c, d = (
                    table[:, (2 * r + i) * LANES : (2 * r + i + 1) * LANES].reshape(rows // 16, 16, LANES)
                    for i in (0, 1)
                )
                h_re, h_im = (
                    jnp.broadcast_to(enter[h, i, r : r + 1, :], (16, LANES)).astype(BF16)[None]
                    for i in (0, 1)
                )
                turned += cmul((c, d), (h_re, h_im))
            moved.append(
                jnp.dot(
                    jnp.concatenate([v.reshape(rows, LANES) for v in turned], axis=1),
                    mapped[2 * k * bstates : 2 * (k + 1) * bstates, :],
                    preferred_element_type=F32,
                )
            )
        for k in range(blocks):
            cols = slice(k * LANES, (k + 1) * LANES)
            hs[slot, :, cols] = gelu(local[0, :, cols] + local[1, :, cols] * moved[k]).astype(BF16)

    enter_copy = remote(enter.at[0], enter.at[0], enter_sem.at[0], enter_sem.at[1], partner)

    @pl.when(tp == 1)
    def _():
        wait_many(far_in, (far_sem.at[0], far_sem.at[1]), a, last, False)
        enter[0, 0], enter[0, 1] = entering(0, (aux_far[0], aux_far[1]))
        enter_copy.start()
        enter[1, 0], enter[1, 1] = entering(1, whole)

    @pl.when(tp == 0)
    def _():
        enter_copy.wait_recv()

    correct(tp, tbl, map_t, post, 0)
    hs_copy = remote(hs.at[0], hs.at[1], hs_sem.at[0], hs_sem.at[1], partner)

    @pl.when(tp == 1)
    def _():
        hs_copy.start()
        for copy in waited:
            copy.wait_recv()
        correct(0, table_far, map_far, post_far, 1)

    oacc[...] += jnp.dot(hs[0], ov[:chans], preferred_element_type=F32)

    @pl.when(b == 0)
    def _():
        add_far_conv()

    @pl.when(tp == 0)
    def _():
        hs_copy.wait_recv()

    out_ref[...] = (oacc[...] + jnp.dot(hs[1], ov[chans : 2 * chans], preferred_element_type=F32)).astype(BF16)

    x_copy.wait_send()
    hc_copy.wait_send()

    @pl.when(tp == 1)
    def _():
        hs_copy.wait_send()
        enter_copy.wait_send()

    @pl.when(tp == 0)
    def _():
        aux_copy.wait_send()
        for copy in waited:
            copy.wait_send()

    @pl.when(sp < n - 1)
    def _():
        tail_copy.wait_send()

    wait_many(
        near_in.at[0],
        (near_sem.at[2], near_sem.at[0]),
        jnp.where(a < last, inner - tp, inner - 1 - b),
        inner,
        True,
    )

    @pl.when(tp == 1)
    def _():
        wait_many(far_in, (far_sem.at[0], far_sem.at[1]), last - a, last, True)


def on_device(
    activations,
    norm_gain,
    state_proj,
    value_proj,
    post_gate_proj,
    pre_gate_proj,
    input_map,
    output_map,
    skip_gain,
    rotation,
    log_decay,
    initial_state,
    conv_taps,
    state_out,
    conv_out,
):
    n = lax.axis_size("sp")
    rows, half = activations.shape
    groups, state = rotation.shape
    chans = state_proj.shape[1]
    cwide = value_proj.shape[1]
    outs = state_out.shape[1]
    states = groups * state
    prow = states // LANES
    inner = inner_of(n)
    bdw = 2 * states // (chans // LANES)
    vmem = pl.BlockSpec(memory_space=pltpu.VMEM)
    hbm = pl.BlockSpec(memory_space=pl.ANY)
    dma = pltpu.SemaphoreType.DMA
    return pl.pallas_call(
        functools.partial(kernel, n),
        out_shape=pltpu.VMEM((rows, outs), BF16),
        in_specs=[hbm] * 15,
        out_specs=vmem,
        scratch_shapes=[
            pltpu.VMEM((rows, half), BF16),
            pltpu.VMEM((1, 2 * half), F32),
            pltpu.VMEM(input_map.shape, BF16),
            pltpu.VMEM((groups, output_map.shape[2], output_map.shape[1]), F32),
            pltpu.VMEM((1, chans), F32),
            pltpu.VMEM((groups, state), F32),
            pltpu.VMEM((groups, rows), F32),
            pltpu.VMEM(initial_state.shape, F32),
            pltpu.VMEM(conv_taps.shape, BF16),
            pltpu.VMEM((4, 2 * half, chans), BF16),
            pltpu.VMEM((2 * chans + 2 * cwide, outs), BF16),
            pltpu.VMEM((rows, half), BF16),
            pltpu.VMEM((rows, 2 * half), BF16),
            pltpu.VMEM((rows, chans), BF16),
            pltpu.VMEM((chans, bdw), BF16),
            pltpu.VMEM((chans, bdw), BF16),
            pltpu.VMEM((2 * states, LANES), BF16),
            pltpu.VMEM((rows, 2 * states), BF16),
            pltpu.VMEM((2, 9 * prow, LANES), F32),
            pltpu.VMEM((rows, chans), F32),
            pltpu.VMEM((rows, chans), F32),
            pltpu.VMEM((2, prow, LANES), F32),
            pltpu.VMEM((2, rows, chans), F32),
            pltpu.VMEM((rows, 2 * states), BF16),
            pltpu.VMEM((2 * states, LANES), BF16),
            pltpu.VMEM((2, rows, chans), F32),
            pltpu.VMEM((4, prow, LANES), F32),
            pltpu.VMEM((4, prow, LANES), F32),
            pltpu.VMEM((2, max(inner, n // inner) * prow, LANES), F32),
            pltpu.VMEM((2, 5, prow, LANES), F32),
            pltpu.VMEM((2, 2, prow, LANES), F32),
            pltpu.VMEM((rows, 2 * rows), BF16),
            pltpu.VMEM((groups, chans), BF16),
            pltpu.VMEM((rows * prow, LANES), F32),
            pltpu.VMEM((rows * (2 * prow + 8), LANES), F32),
            pltpu.VMEM((4 * groups, LANES), F32),
            pltpu.VMEM((rows + 8, cwide), F32),
            pltpu.VMEM((2, inner, 3 * prow, LANES), BF16),
            pltpu.VMEM((n // inner, 2, 3 * prow, LANES), BF16),
            pltpu.VMEM((2, 3 * prow, LANES), BF16),
            pltpu.VMEM((2, rows, chans), BF16),
            pltpu.VMEM((2, rows, cwide), BF16),
            pltpu.VMEM((rows, outs), F32),
            dma((9,)),
            dma((4,)),
            dma((1,)),
            dma((2,)),
            dma((2,)),
            dma((2,)),
            dma((2,)),
            dma((3,)),
            dma((2,)),
            dma((2,)),
            dma((2,)),
            dma((2, 3)),
            pltpu.SemaphoreType.REGULAR,
            pltpu.SemaphoreType.REGULAR,
        ],
        compiler_params=pltpu.CompilerParams(collective_id=0, has_side_effects=True),
    )(
        activations,
        norm_gain.reshape(1, -1),
        state_proj,
        value_proj,
        post_gate_proj,
        pre_gate_proj,
        input_map,
        jnp.swapaxes(output_map, 1, 2),
        skip_gain.reshape(1, -1),
        rotation,
        jnp.swapaxes(log_decay, 0, 1),
        initial_state,
        conv_taps,
        state_out,
        conv_out,
    )


def solution(mesh):
    return jax.shard_map(
        on_device,
        mesh=mesh,
        in_specs=(
            P("sp", "tp"),
            P(),
            P(None, "tp"),
            P(None, "tp"),
            P(None, "tp"),
            P(None, "tp"),
            P("tp", None, None),
            P("tp", None, None),
            P("tp"),
            P("tp", None),
            P("sp", "tp"),
            P(None, "tp", None),
            P(None, "tp"),
            P(None, "tp"),
            P(None, "tp"),
        ),
        out_specs=P("sp", "tp"),
        check_vma=False,
    )
```

```python
import functools

import jax
import jax.numpy as jnp
from jax import lax
from jax.experimental import pallas as pl
from jax.experimental.pallas import tpu as pltpu
from jax.sharding import PartitionSpec as P

EPS = 1e-06
LANES = 128
MESH = pl.DeviceIdType.MESH
F32 = jnp.float32
BF16 = jnp.bfloat16


def minus_expm1(y):
    poly = jnp.ones_like(y)
    for k in range(11, 1, -1):
        poly = 1.0 + poly * y * (1.0 / k)
    return jnp.where(y > -0.5, -y * poly, 1.0 - jnp.exp(y))


def split3(v):
    hi = v.astype(BF16)
    rest = v - hi.astype(F32)
    mid = rest.astype(BF16)
    low = (rest - mid.astype(F32)).astype(BF16)
    return hi, mid, low


def cmul(a, b):
    return a[0] * b[0] - a[1] * b[1], a[0] * b[1] + a[1] * b[0]


def cpow(base, count):
    result = None
    while count:
        if count & 1:
            result = base if result is None else cmul(result, base)
        count >>= 1
        if count:
            base = cmul(base, base)
    return result


def inner_of(n):
    return max(d for d in range(1, n + 1) if n % d == 0 and d * d <= n)


def gelu(x):
    return 0.5 * x * (1.0 + jnp.tanh(0.7978845608028654 * (x + 0.044715 * x * x * x)))


def kernel(
    n,
    x_hbm,
    gain_hbm,
    w0_hbm,
    w1_hbm,
    w2_hbm,
    w3_hbm,
    imap_hbm,
    omap_hbm,
    skip_hbm,
    rot_hbm,
    ld_hbm,
    init_hbm,
    taps_hbm,
    so_hbm,
    co_hbm,
    out_ref,
    x_ref,
    gain_ref,
    imap_ref,
    omap_ref,
    skip_ref,
    rot_ref,
    ld_ref,
    init_ref,
    taps_ref,
    wv,
    ov,
    xr,
    acc,
    din,
    bd_in,
    bd_out,
    map_t,
    tbl,
    powers,
    chan_end,
    chan_gain,
    rowed,
    post,
    table_far,
    map_far,
    post_far,
    aux,
    aux_far,
    mags_in,
    held,
    enter,
    sums,
    to_chan,
    mag,
    drv,
    pairs,
    pad,
    near_in,
    far_in,
    far_out,
    hs,
    hc,
    oacc,
    in_sem,
    wsem,
    osem,
    x_sem,
    tail_sem,
    hc_sem,
    hs_sem,
    near_sem,
    far_sem,
    aux_sem,
    enter_sem,
    dup_sem,
    near_ready,
    far_ready,
):
    sp, tp = lax.axis_index("sp"), lax.axis_index("tp")
    other = 1 - tp
    rows, half = x_ref.shape
    groups, state = rot_ref.shape
    gch = imap_ref.shape[1]
    chans = groups * gch
    states = groups * state
    prow = states // LANES
    per_block = LANES // gch
    blocks = groups // per_block
    quads = prow // blocks
    pitch = drv.shape[0] // rows
    bstates = quads * LANES
    cwide = taps_ref.shape[1]
    width = taps_ref.shape[0]

    barrier = pltpu.get_barrier_semaphore()
    partner = {"sp": sp, "tp": other}

    inner = inner_of(n)
    outer = n // inner
    a, b = lax.div(sp, inner), lax.rem(sp, inner)
    last = outer - 1

    hop_on = (b == inner - 1) & (a < last)

    def tell(sem, j):
        for t in (0, 1):
            pl.semaphore_signal(sem, inc=1, device_id={"sp": j, "tp": t}, device_id_type=MESH)

    def greet_far(k, c):
        tell(barrier, k * inner + b)
        return c

    pl.semaphore_signal(barrier, inc=1, device_id=partner, device_id_type=MESH)

    @pl.when(b < inner - 1)
    def _():
        tell(barrier, sp + inner - 1 - b)

    lax.fori_loop(a + 1, outer, greet_far, 0)

    in_copies = {}
    def fetch(i, src, dst):
        in_copies[i] = pltpu.make_async_copy(src, dst, in_sem.at[i])
        in_copies[i].start()

    w_hbm = (w0_hbm, w1_hbm, w2_hbm, w3_hbm)

    def fetch_weight(i, h, sem):
        part = (tp, other)[h]
        pltpu.make_async_copy(
            w_hbm[i].at[pl.ds(part * half, half), :], wv.at[i, pl.ds(h * half, half), :], sem
        ).start()

    def wait_weight(i):
        pltpu.make_async_copy(w_hbm[i], wv.at[i], wsem.at[i]).wait()

    fetch(0, x_hbm, x_ref)
    fetch(4, ld_hbm, ld_ref)
    fetch(2, rot_hbm, rot_ref)
    fetch(5, imap_hbm, imap_ref)
    fetch(1, gain_hbm, gain_ref)
    fetch_weight(0, 0, wsem.at[0])
    fetch_weight(0, 1, wsem.at[0])

    pl.semaphore_wait(barrier, 1 + 2 * (a + jnp.where(b == inner - 1, b, 0)))

    def ready_near(k, c):
        tell(near_ready, a * inner + k)
        return c

    def ready_far(k, c):
        tell(far_ready, k * inner + b)
        return c

    @pl.when((tp == 1) & (b == inner - 1))
    def _():
        lax.fori_loop(0, b, ready_near, 0)


    lax.fori_loop(0, a, ready_far, 0)

    when = lax.broadcasted_iota(jnp.int32, (rows, 2 * rows), 0)
    upto = lax.broadcasted_iota(jnp.int32, (rows, 2 * rows), 1)
    sums[...] = jnp.where(
        ((upto < rows) & (when <= upto)) | ((upto >= rows) & (when > upto - rows)), 1.0, 0.0
    ).astype(BF16)
    col = lax.broadcasted_iota(jnp.int32, (groups, chans), 1)
    row = lax.broadcasted_iota(jnp.int32, (groups, chans), 0)
    to_chan[...] = jnp.where((col >= row * gch) & (col < (row + 1) * gch), 1.0, 0.0).astype(BF16)

    def remote(src, dst, s, r, dev):
        return pltpu.make_async_remote_copy(
            src_ref=src, dst_ref=dst, send_sem=s, recv_sem=r, device_id=dev, device_id_type=MESH
        )

    in_copies[0].wait()
    x_copy = remote(x_ref, xr, x_sem.at[0], x_sem.at[1], partner)
    x_copy.start()

    fetch(3, init_hbm, init_ref)
    fetch(6, omap_hbm, omap_ref)
    fetch(7, skip_hbm, skip_ref)
    fetch(8, taps_hbm, taps_ref)
    for i in (1, 3, 2):
        for h in (0, 1):
            fetch_weight(i, h, wsem.at[i])
    for i, w, deep in ((1, co_hbm, cwide), (0, so_hbm, chans)):
        for h, part in ((0, tp), (1, other)):
            pltpu.make_async_copy(
                w.at[pl.ds(part * deep, deep), :], ov.at[pl.ds(2 * i * chans + h * deep, deep), :], osem.at[0]
            ).start()

    lane = lax.broadcasted_iota(jnp.int32, (1, LANES), 1)

    def pair_up(i, v):
        pairs[pl.ds(i * groups, groups), :] = v
        even = pairs[pl.ds(i * groups, prow, stride=2), :]
        odd = pairs[pl.ds(i * groups + 1, prow, stride=2), :]
        return jnp.where(lane < state, even, odd)

    def twice(v):
        return jnp.concatenate([v, v], axis=1)

    for i in (4, 2, 5, 1):
        in_copies[i].wait()
    ld = ld_ref[...]

    def time_sums(cols):
        added = jnp.dot(jnp.concatenate(split3(ld), axis=0), sums[:, cols], preferred_element_type=F32)
        return added[:groups] + added[groups : 2 * groups] + added[2 * groups :]

    def per_channel(v):
        hi, mid, _ = split3(v.T)
        return jnp.dot(hi, to_chan[...], preferred_element_type=F32) + jnp.dot(
            mid, to_chan[...], preferred_element_type=F32
        )

    gain = jnp.sqrt(minus_expm1(2.0 * ld))
    chan_end[...] = per_channel(gain * jnp.exp(time_sums(slice(rows, 2 * rows))))
    tot = pair_up(
        3, jnp.broadcast_to(jnp.exp(jnp.sum(ld, axis=1, keepdims=True)), (groups, LANES))
    )
    theta = pair_up(0, twice(rot_ref[...]))
    turn = jnp.cos(theta), jnp.sin(theta)
    step = turn
    for k in range(8):
        for i in (0, 1):
            powers[i, pl.ds(k * prow, prow), :] = step[i]
        step = cmul(step, turn) if k < 7 else step
    far_step16 = cmul(step, step)
    for i in (0, 1):
        powers[i, pl.ds(8 * prow, prow), :] = far_step16[i]
    whole = cpow(step, rows // 8)
    for r in range(prow):
        even = [powers[i, pl.ds(r, 8, stride=prow), :] for i in (0, 1)]
        eight = [powers[i, pl.ds(7 * prow + r, 1), :] for i in (0, 1)]
        sixteen = [powers[i, pl.ds(8 * prow + r, 1), :] for i in (0, 1)]
        odd = cmul(even, eight)
        for t in range(0, rows, 16):
            for i in (0, 1):
                tbl[t : t + 16, (2 * r + i) * LANES : (2 * r + i + 1) * LANES] = jnp.concatenate(
                    [even[i], odd[i]], axis=0
                ).astype(BF16)
            even = cmul(even, sixteen)
            odd = cmul(odd, sixteen)

    def spread_map(src, dst):
        dst[...] = jnp.zeros_like(dst)
        for b in range(blocks):
            for q in range(quads):
                g = b * per_block + 2 * q
                one = src[g].astype(F32)
                two = src[g + 1].astype(F32)
                one_r = jnp.concatenate([one[:, state:], one[:, :state]], axis=1)
                two_r = jnp.concatenate([two[:, state:], two[:, :state]], axis=1)
                low = lane < state
                re = jnp.concatenate([jnp.where(low, one, 0.0), jnp.where(low, 0.0, two_r)], axis=0)
                im = jnp.concatenate([jnp.where(low, one_r, 0.0), jnp.where(low, 0.0, two)], axis=0)
                at = pl.ds(b * LANES + q * 2 * gch, 2 * gch)
                dst[at, 2 * q * LANES : (2 * q + 1) * LANES] = re.astype(BF16)
                dst[at, (2 * q + 1) * LANES : (2 * q + 2) * LANES] = im.astype(BF16)

    spread_map(imap_ref, bd_in)
    own = x_ref[...].astype(F32)
    scaled = (own * gain_ref[:, pl.ds(pl.multiple_of(tp * half, LANES), half)]).astype(BF16)
    squares = jnp.sum(own * own, axis=1, keepdims=True)
    wait_weight(0)
    partial = jnp.dot(scaled, wv[0, :half], preferred_element_type=F32)
    acc[:, :half] = scaled

    x_copy.wait_recv()
    far_x = xr[...].astype(F32)
    scaled_far = (far_x * gain_ref[:, pl.ds(pl.multiple_of(other * half, LANES), half)]).astype(BF16)
    squares = squares + jnp.sum(far_x * far_x, axis=1, keepdims=True)
    scale = lax.rsqrt(squares / (2 * half) + EPS)

    acc[:, half:] = scaled_far
    total = partial + jnp.dot(scaled_far, wv[0, half:], preferred_element_type=F32)
    drive_in = (total * scale).astype(BF16)
    din[...] = drive_in
    ends_in = (drive_in.astype(F32) * chan_end[...]).astype(BF16).T
    for r in range(prow):
        q = r % quads
        at = slice(r * 2 * gch, (r + 1) * 2 * gch)
        seen = jnp.dot(
            ends_in[at], tbl[:, 2 * r * LANES : (2 * r + 2) * LANES], preferred_element_type=F32
        )
        m_re = bd_in[at, 2 * q * LANES : (2 * q + 1) * LANES].astype(F32)
        m_im = bd_in[at, (2 * q + 1) * LANES : (2 * q + 2) * LANES].astype(F32)
        c, d = seen[:, :LANES], seen[:, LANES:]
        rowed[0, r : r + 1, :] = jnp.sum(c * m_re + d * m_im, axis=0, keepdims=True)
        rowed[1, r : r + 1, :] = jnp.sum(c * m_im - d * m_re, axis=0, keepdims=True)
    e_re, e_im = cmul(whole, (rowed[0], rowed[1]))

    near_in[tp, b, pl.ds(0, prow), :] = e_re.astype(BF16)
    near_in[tp, b, pl.ds(prow, prow), :] = e_im.astype(BF16)
    fore = lax.rem(lax.broadcasted_iota(jnp.int32, (prow, LANES), 1), state) < state // 2

    def packed(v):
        hi, mid, _ = split3(v)
        return jnp.where(fore, hi.astype(F32), mid.astype(F32)).astype(BF16)

    near_in[tp, b, pl.ds(2 * prow, prow), :] = packed(tot)

    def wait_many(ref, sems, count, upto, sent):
        for j in range(1, upto + 1):
            @pl.when(count == j)
            def _():
                part = ref.at[pl.ds(0, j)]
                copy = remote(part, part, sems[0], sems[1], partner)
                copy.wait_send() if sent else copy.wait_recv()

    def near_copy(k):
        return remote(
            near_in.at[tp, b],
            near_in.at[tp, b],
            near_sem.at[2],
            near_sem.at[tp],
            {"sp": a * inner + k, "tp": 1},
        )

    def far_copy(k):
        return remote(
            far_out, far_in.at[a], far_sem.at[0], far_sem.at[1], {"sp": k * inner + b, "tp": 1}
        )

    near_from = jnp.where(a < last, 0, b + 1)
    near_upto = jnp.where(a < last, inner, b)
    @pl.when(b < inner - 1)
    def _():
        pl.semaphore_wait(near_ready, 1)

    def send_near(k, c):
        @pl.when((k != b) | ((tp == 0) & (a < last)))
        def _():
            near_copy(k).start()

        return c

    lax.fori_loop(near_from, inner, send_near, 0)

    in_copies[3].wait()
    aux[0], aux[1] = whole
    aux[2] = pair_up(1, twice(init_ref[0]))
    aux[3] = pair_up(2, twice(init_ref[1]))
    aux_copy = remote(aux, aux_far, aux_sem.at[0], aux_sem.at[1], partner)
    dup_copies = [
        remote(src, dst, dup_sem.at[0, (0, 1, 2, 2, 1)[i]], dup_sem.at[1, (0, 1, 2, 2, 1)[i]], partner)
        for i, (src, dst) in enumerate(
            (
                (tbl, table_far),
                (map_t.at[pl.ds(0, states), :], map_far.at[pl.ds(0, states), :]),
                (post.at[1], post_far.at[1]),
                (post.at[0], post_far.at[0]),
                (map_t.at[pl.ds(states, states), :], map_far.at[pl.ds(states, states), :]),
            )
        )
    ]

    def give(copy):
        @pl.when(tp == 0)
        def _():
            copy.start()

    waited = [
        remote(src, dst, dup_sem.at[0, i], dup_sem.at[1, i], partner)
        for i, (src, dst) in enumerate(((tbl, table_far), (map_t, map_far), (post, post_far)))
    ]

    give(aux_copy)

    def project(i):
        wait_weight(i)
        total = jnp.dot(acc[...], wv[i], preferred_element_type=F32)
        return (total * scale).astype(BF16)

    value = project(1)
    pre_gate = project(3)
    mixed = (pre_gate.astype(F32) * value.astype(F32)).astype(BF16).astype(F32)
    pad[pl.ds(8, rows), :] = mixed
    tail_copy = remote(
        pad.at[pl.ds(rows, 8), :],
        pad.at[pl.ds(0, 8), :],
        tail_sem.at[0],
        tail_sem.at[1],
        {"sp": lax.rem(sp + 1, n), "tp": tp},
    )

    @pl.when(hop_on)
    def _():
        pl.semaphore_wait(far_ready, 2 * (last - a))

    @pl.when(sp < n - 1)
    def _():
        tail_copy.start()

    give(dup_copies[0])

    for i in (6, 7):
        in_copies[i].wait()
    spread_map(omap_ref, bd_out)
    for k in range(blocks):
        map_t[2 * k * bstates : 2 * (k + 1) * bstates, :] = bd_out[k * LANES : (k + 1) * LANES, :].T
    give(dup_copies[1])

    ld = ld_ref[...]
    gain = jnp.sqrt(minus_expm1(2.0 * ld))
    late = per_channel(jnp.concatenate([jnp.exp(time_sums(slice(0, rows))), gain], axis=1))
    post[1] = late[:rows]
    give(dup_copies[2])
    chan_gain[...] = late[rows:]
    mags = split3(jnp.exp(ld).T)[:2]
    for k in range(blocks):
        col = lax.broadcasted_iota(jnp.int32, (groups, bstates), 1) + k * bstates
        row = lax.broadcasted_iota(jnp.int32, (groups, bstates), 0)
        spread = jnp.where(
            (col >= row * state) & (col < (row + 1) * state), 1.0, 0.0
        ).astype(BF16)
        m = jnp.dot(mags[0], spread, preferred_element_type=F32) + jnp.dot(
            mags[1], spread, preferred_element_type=F32
        )
        for q in range(quads):
            mag[pl.ds(k * quads + q, rows, stride=prow), :] = m[:, q * LANES : (q + 1) * LANES]

    zero = jnp.zeros((prow, LANES), F32)

    def unpacked(v):
        v = v.astype(F32)
        keep = lax.rem(lax.broadcasted_iota(jnp.int32, v.shape, 1), state) < state // 2
        return v + jnp.where(keep, pltpu.roll(v, LANES - state // 2, 1), pltpu.roll(v, state // 2, 1))

    def unpack_all(ref, count, index):
        packs = [
            ref[index(h, k) + (pl.ds(2 * prow, prow),)] for h in (0, 1) for k in range(count)
        ]
        v = unpacked(jnp.concatenate(packs, axis=0))
        for h in (0, 1):
            mags_in[h, : count * prow, :] = v[h * count * prow : (h + 1) * count * prow]

    def message(ref, h, k):
        return (
            ref[pl.ds(0, prow), :].astype(F32),
            ref[pl.ds(prow, prow), :].astype(F32),
            mags_in[h, pl.ds(pl.multiple_of(k * prow, prow), prow), :],
        )

    def send_far(k, c):
        far_copy(outer + a - k).start()
        return c

    def join_halves(turned, first):
        unpack_all(near_in, inner, lambda h, k: (h, k))

        def half_step(h, k, c):
            ends, mag_all, phase, mine = c[0:2], c[2], c[3:5], c[5:]
            k_re, k_im, k_mag = message(near_in.at[h, k], h, k)
            moved = cmul((turned[h][0] * k_mag, turned[h][1] * k_mag), ends)
            now = (moved[0] + k_re, moved[1] + k_im, mag_all * k_mag) + cmul(turned[h], phase)
            return now + tuple(jnp.where(k < b, v, w) for v, w in zip(now, mine))

        def near_step(k, c):
            return tuple(half_step(h, k, c[h]) for h in (0, 1))

        one = jnp.ones((prow, LANES), F32)
        begin = [tuple(jnp.where(a == 0, v, zero) for v in f) + (one, one, zero) for f in first]
        planes = lax.fori_loop(0, near_upto, near_step, tuple(v + v for v in begin))
        for h, plane in enumerate(planes):
            far_out[h, pl.ds(0, prow), :] = plane[0].astype(BF16)
            far_out[h, pl.ds(prow, prow), :] = plane[1].astype(BF16)
            far_out[h, pl.ds(2 * prow, prow), :] = packed(plane[2])
            for i in range(5):
                held[h, i] = plane[5 + i]

    def join_near():
        @pl.when(tp == 1)
        def _():
            for h in (1, 0):
                wait_many(
                    near_in.at[h],
                    (near_sem.at[2], near_sem.at[h]),
                    jnp.where(a < last, inner - h, b),
                    inner,
                    False,
                )
            join_halves(
                ((aux_far[0], aux_far[1]), whole), ((aux_far[2], aux_far[3]), (aux[2], aux[3]))
            )

        @pl.when((a < last) & (b < inner - 1))
        def _():
            pl.semaphore_wait(far_ready, 2 * (last - a))

        @pl.when((tp == 1) & (a < last))
        def _():
            lax.fori_loop(a + 1, outer, send_far, 0)

    @pl.when(tp == 1)
    def _():
        aux_copy.wait_recv()

    @pl.when(b > 1)
    def _():
        join_near()

    hc[0] = project(2)
    gained = (din[...].astype(F32) * chan_gain[...]).astype(BF16)
    for k in range(blocks):
        blk = jnp.dot(
            gained[:, k * LANES : (k + 1) * LANES],
            bd_in[k * LANES : (k + 1) * LANES, :],
            preferred_element_type=F32,
        )
        for q in range(quads):
            r = k * quads + q
            drv[pl.ds(r, rows, stride=pitch), :] = blk[:, 2 * q * LANES : (2 * q + 1) * LANES]
            drv[pl.ds(prow + r, rows, stride=pitch), :] = blk[
                :, (2 * q + 1) * LANES : (2 * q + 2) * LANES
            ]

    @pl.when(b == 1)
    def _():
        join_near()

    hc_copy = remote(hc.at[0], hc.at[1], hc_sem.at[0], hc_sem.at[1], partner)

    def convolve():
        @pl.when(sp == 0)
        def _():
            pad[pl.ds(0, 8), :] = jnp.zeros((8, cwide), F32)

        in_copies[8].wait()

        @pl.when(sp > 0)
        def _():
            tail_copy.wait_recv()

        conv = jnp.zeros((rows, cwide), F32)
        for k in range(width):
            conv = conv + pad[pl.ds(8 + k - (width - 1), rows), :] * taps_ref[k : k + 1, :].astype(F32)
        hc[0] = (hc[0].astype(F32) * conv).astype(BF16)
        hc_copy.start()

    @pl.when(b > 0)
    def _():
        convolve()

    give(dup_copies[4])

    def scan(t, h):
        m = mag[pl.ds(pl.multiple_of(t * prow, prow), prow), :]
        base = pl.multiple_of(t * pitch, 8)
        d_re = drv[pl.ds(base, prow), :]
        d_im = drv[pl.ds(base + prow, prow), :]
        f_re, f_im = m * turn[0], m * turn[1]
        new_re = (f_re * h[0] + d_re) - f_im * h[1]
        new_im = (f_re * h[1] + d_im) + f_im * h[0]
        drv[pl.ds(base, prow), :] = new_re
        drv[pl.ds(base + prow, prow), :] = new_im
        return new_re, new_im

    lax.fori_loop(0, rows, scan, (zero, zero), unroll=8)

    @pl.when(b == 0)
    def _():
        join_near()

    for k in range(blocks):
        cols = slice(k * LANES, (k + 1) * LANES)
        at = [half_row + k * quads + q for q in range(quads) for half_row in (0, prow)]
        st = jnp.concatenate(
            [drv[pl.ds(r, rows, stride=pitch), :].astype(BF16) for r in at], axis=1
        )
        read = jnp.dot(
            st, map_t[2 * k * bstates : 2 * (k + 1) * bstates, :], preferred_element_type=F32
        )
        post[0, :, cols] = read + skip_ref[:, cols] * din[:, cols].astype(F32)

    give(dup_copies[3])

    @pl.when(b == 0)
    def _():
        convolve()

    pltpu.make_async_copy(ov, ov, osem.at[0]).wait()
    oacc[...] = jnp.dot(hc[0], ov[2 * chans : 2 * chans + cwide], preferred_element_type=F32)

    def add_far_conv():
        hc_copy.wait_recv()
        oacc[...] += jnp.dot(hc[1], ov[2 * chans + cwide :], preferred_element_type=F32)

    @pl.when(b > 0)
    def _():
        add_far_conv()

    def entering(h, turned):
        plane_turn = cpow(turned, inner)

        def far_step(k, c):
            k_re, k_im, k_mag = message(far_in.at[k, h], h, k)
            moved = cmul((plane_turn[0] * k_mag, plane_turn[1] * k_mag), c)
            return moved[0] + k_re, moved[1] + k_im

        before = lax.fori_loop(0, a, far_step, (zero, zero))
        moved = cmul((held[h, 3] * held[h, 2], held[h, 4] * held[h, 2]), before)
        return held[h, 0] + moved[0], held[h, 1] + moved[1]

    def correct(h, table, mapped, local, slot):
        moved = []
        for k in range(blocks):
            turned = []
            for r in range(k * quads, (k + 1) * quads):
                c, d = (
                    table[:, (2 * r + i) * LANES : (2 * r + i + 1) * LANES].reshape(rows // 16, 16, LANES)
                    for i in (0, 1)
                )
                h_re, h_im = (
                    jnp.broadcast_to(enter[h, i, r : r + 1, :], (16, LANES)).astype(BF16)[None]
                    for i in (0, 1)
                )
                turned += cmul((c, d), (h_re, h_im))
            moved.append(
                jnp.dot(
                    jnp.concatenate([v.reshape(rows, LANES) for v in turned], axis=1),
                    mapped[2 * k * bstates : 2 * (k + 1) * bstates, :],
                    preferred_element_type=F32,
                )
            )
        made = []
        for k in range(blocks):
            cols = slice(k * LANES, (k + 1) * LANES)
            made.append(gelu(local[0, :, cols] + local[1, :, cols] * moved[k]).astype(BF16))
            hs[slot, :, cols] = made[k]
        return made

    enter_copy = remote(enter.at[0], enter.at[0], enter_sem.at[0], enter_sem.at[1], partner)

    @pl.when(tp == 1)
    def _():
        wait_many(far_in, (far_sem.at[0], far_sem.at[1]), a, last, False)
        unpack_all(far_in, last, lambda h, k: (k, h))
        enter[0, 0], enter[0, 1] = entering(0, (aux_far[0], aux_far[1]))
        enter_copy.start()
        enter[1, 0], enter[1, 1] = entering(1, whole)

    @pl.when(tp == 0)
    def _():
        enter_copy.wait_recv()

    hs_copy = remote(hs.at[0], hs.at[1], hs_sem.at[0], hs_sem.at[1], partner)

    def add_own(blks):
        oacc[...] += jnp.dot(
            jnp.concatenate(blks, axis=1), ov[:chans], preferred_element_type=F32
        )

    @pl.when(tp == 1)
    def _():
        correct(1, tbl, map_t, post, 0)
        hs_copy.start()
        for copy in waited:
            copy.wait_recv()
        correct(0, table_far, map_far, post_far, 1)
        oacc[...] += jnp.dot(hs[0], ov[:chans], preferred_element_type=F32)

    @pl.when(tp == 0)
    def _():
        add_own(correct(0, tbl, map_t, post, 0))

    @pl.when(b == 0)
    def _():
        add_far_conv()

    @pl.when(tp == 0)
    def _():
        hs_copy.wait_recv()

    out_ref[...] = (oacc[...] + jnp.dot(hs[1], ov[chans : 2 * chans], preferred_element_type=F32)).astype(BF16)

    x_copy.wait_send()
    hc_copy.wait_send()

    @pl.when(tp == 1)
    def _():
        hs_copy.wait_send()
        enter_copy.wait_send()

    @pl.when(tp == 0)
    def _():
        aux_copy.wait_send()
        for copy in waited:
            copy.wait_send()

    @pl.when(sp < n - 1)
    def _():
        tail_copy.wait_send()

    wait_many(
        near_in.at[0],
        (near_sem.at[2], near_sem.at[0]),
        jnp.where(a < last, inner - tp, inner - 1 - b),
        inner,
        True,
    )

    @pl.when(tp == 1)
    def _():
        wait_many(far_in, (far_sem.at[0], far_sem.at[1]), last - a, last, True)


def on_device(
    activations,
    norm_gain,
    state_proj,
    value_proj,
    post_gate_proj,
    pre_gate_proj,
    input_map,
    output_map,
    skip_gain,
    rotation,
    log_decay,
    initial_state,
    conv_taps,
    state_out,
    conv_out,
):
    n = lax.axis_size("sp")
    rows, half = activations.shape
    groups, state = rotation.shape
    chans = state_proj.shape[1]
    cwide = value_proj.shape[1]
    outs = state_out.shape[1]
    states = groups * state
    prow = states // LANES
    inner = inner_of(n)
    bdw = 2 * states // (chans // LANES)
    vmem = pl.BlockSpec(memory_space=pltpu.VMEM)
    hbm = pl.BlockSpec(memory_space=pl.ANY)
    dma = pltpu.SemaphoreType.DMA
    return pl.pallas_call(
        functools.partial(kernel, n),
        out_shape=pltpu.VMEM((rows, outs), BF16),
        in_specs=[hbm] * 15,
        out_specs=vmem,
        scratch_shapes=[
            pltpu.VMEM((rows, half), BF16),
            pltpu.VMEM((1, 2 * half), F32),
            pltpu.VMEM(input_map.shape, BF16),
            pltpu.VMEM((groups, output_map.shape[2], output_map.shape[1]), F32),
            pltpu.VMEM((1, chans), F32),
            pltpu.VMEM((groups, state), F32),
            pltpu.VMEM((groups, rows), F32),
            pltpu.VMEM(initial_state.shape, F32),
            pltpu.VMEM(conv_taps.shape, BF16),
            pltpu.VMEM((4, 2 * half, chans), BF16),
            pltpu.VMEM((2 * chans + 2 * cwide, outs), BF16),
            pltpu.VMEM((rows, half), BF16),
            pltpu.VMEM((rows, 2 * half), BF16),
            pltpu.VMEM((rows, chans), BF16),
            pltpu.VMEM((chans, bdw), BF16),
            pltpu.VMEM((chans, bdw), BF16),
            pltpu.VMEM((2 * states, LANES), BF16),
            pltpu.VMEM((rows, 2 * states), BF16),
            pltpu.VMEM((2, 9 * prow, LANES), F32),
            pltpu.VMEM((rows, chans), F32),
            pltpu.VMEM((rows, chans), F32),
            pltpu.VMEM((2, prow, LANES), F32),
            pltpu.VMEM((2, rows, chans), F32),
            pltpu.VMEM((rows, 2 * states), BF16),
            pltpu.VMEM((2 * states, LANES), BF16),
            pltpu.VMEM((2, rows, chans), F32),
            pltpu.VMEM((4, prow, LANES), F32),
            pltpu.VMEM((4, prow, LANES), F32),
            pltpu.VMEM((2, max(inner, n // inner) * prow, LANES), F32),
            pltpu.VMEM((2, 5, prow, LANES), F32),
            pltpu.VMEM((2, 2, prow, LANES), F32),
            pltpu.VMEM((rows, 2 * rows), BF16),
            pltpu.VMEM((groups, chans), BF16),
            pltpu.VMEM((rows * prow, LANES), F32),
            pltpu.VMEM((rows * (2 * prow + 8), LANES), F32),
            pltpu.VMEM((4 * groups, LANES), F32),
            pltpu.VMEM((rows + 8, cwide), F32),
            pltpu.VMEM((2, inner, 3 * prow, LANES), BF16),
            pltpu.VMEM((n // inner, 2, 3 * prow, LANES), BF16),
            pltpu.VMEM((2, 3 * prow, LANES), BF16),
            pltpu.VMEM((2, rows, chans), BF16),
            pltpu.VMEM((2, rows, cwide), BF16),
            pltpu.VMEM((rows, outs), F32),
            dma((9,)),
            dma((4,)),
            dma((1,)),
            dma((2,)),
            dma((2,)),
            dma((2,)),
            dma((2,)),
            dma((3,)),
            dma((2,)),
            dma((2,)),
            dma((2,)),
            dma((2, 3)),
            pltpu.SemaphoreType.REGULAR,
            pltpu.SemaphoreType.REGULAR,
        ],
        compiler_params=pltpu.CompilerParams(collective_id=0, has_side_effects=True),
    )(
        activations,
        norm_gain.reshape(1, -1),
        state_proj,
        value_proj,
        post_gate_proj,
        pre_gate_proj,
        input_map,
        jnp.swapaxes(output_map, 1, 2),
        skip_gain.reshape(1, -1),
        rotation,
        jnp.swapaxes(log_decay, 0, 1),
        initial_state,
        conv_taps,
        state_out,
        conv_out,
    )


def solution(mesh):
    return jax.shard_map(
        on_device,
        mesh=mesh,
        in_specs=(
            P("sp", "tp"),
            P(),
            P(None, "tp"),
            P(None, "tp"),
            P(None, "tp"),
            P(None, "tp"),
            P("tp", None, None),
            P("tp", None, None),
            P("tp"),
            P("tp", None),
            P("sp", "tp"),
            P(None, "tp", None),
            P(None, "tp"),
            P(None, "tp"),
            P(None, "tp"),
        ),
        out_specs=P("sp", "tp"),
        check_vma=False,
    )
```

```python
import functools

import jax
import jax.numpy as jnp
from jax import lax
from jax.experimental import pallas as pl
from jax.experimental.pallas import tpu as pltpu
from jax.sharding import PartitionSpec as P

EPS = 1e-06
LANES = 128
MESH = pl.DeviceIdType.MESH
F32 = jnp.float32
BF16 = jnp.bfloat16


def minus_expm1(y):
    poly = jnp.ones_like(y)
    for k in range(11, 1, -1):
        poly = 1.0 + poly * y * (1.0 / k)
    return jnp.where(y > -0.5, -y * poly, 1.0 - jnp.exp(y))


def split3(v):
    hi = v.astype(BF16)
    rest = v - hi.astype(F32)
    mid = rest.astype(BF16)
    low = (rest - mid.astype(F32)).astype(BF16)
    return hi, mid, low


def cmul(a, b):
    return a[0] * b[0] - a[1] * b[1], a[0] * b[1] + a[1] * b[0]


def cpow(base, count):
    result = None
    while count:
        if count & 1:
            result = base if result is None else cmul(result, base)
        count >>= 1
        if count:
            base = cmul(base, base)
    return result


def inner_of(n):
    return max(d for d in range(1, n + 1) if n % d == 0 and d * d <= n)


def gelu(x):
    return 0.5 * x * (1.0 + jnp.tanh(0.7978845608028654 * (x + 0.044715 * x * x * x)))


def kernel(
    n,
    x_hbm,
    gain_hbm,
    w0_hbm,
    w1_hbm,
    w2_hbm,
    w3_hbm,
    imap_hbm,
    omap_hbm,
    skip_hbm,
    rot_hbm,
    ld_hbm,
    init_hbm,
    taps_hbm,
    so_hbm,
    co_hbm,
    out_ref,
    x_ref,
    gain_ref,
    imap_ref,
    omap_ref,
    skip_ref,
    rot_ref,
    ld_ref,
    init_ref,
    taps_ref,
    wv,
    ov,
    xr,
    acc,
    din,
    bd_in,
    bd_out,
    map_t,
    tbl,
    powers,
    chan_end,
    chan_gain,
    rowed,
    post,
    table_far,
    map_far,
    post_far,
    aux,
    aux_far,
    mags_in,
    held,
    enter,
    sums,
    to_chan,
    mag,
    drv,
    pairs,
    pad,
    near_in,
    far_in,
    far_out,
    hs,
    hc,
    oacc,
    in_sem,
    wsem,
    osem,
    x_sem,
    tail_sem,
    hc_sem,
    hs_sem,
    near_sem,
    far_sem,
    aux_sem,
    enter_sem,
    dup_sem,
    near_ready,
    far_ready,
):
    sp, tp = lax.axis_index("sp"), lax.axis_index("tp")
    other = 1 - tp
    rows, half = x_ref.shape
    groups, state = rot_ref.shape
    gch = imap_ref.shape[1]
    chans = groups * gch
    states = groups * state
    prow = states // LANES
    per_block = LANES // gch
    blocks = groups // per_block
    quads = prow // blocks
    pitch = drv.shape[0] // rows
    bstates = quads * LANES
    cwide = taps_ref.shape[1]
    width = taps_ref.shape[0]

    barrier = pltpu.get_barrier_semaphore()
    partner = {"sp": sp, "tp": other}

    inner = inner_of(n)
    outer = n // inner
    a, b = lax.div(sp, inner), lax.rem(sp, inner)
    last = outer - 1

    hop_on = (b == inner - 1) & (a < last)

    def tell(sem, j):
        for t in (0, 1):
            pl.semaphore_signal(sem, inc=1, device_id={"sp": j, "tp": t}, device_id_type=MESH)

    def greet_far(k, c):
        tell(barrier, k * inner + b)
        return c

    pl.semaphore_signal(barrier, inc=1, device_id=partner, device_id_type=MESH)

    @pl.when(b < inner - 1)
    def _():
        tell(barrier, sp + inner - 1 - b)

    lax.fori_loop(a + 1, outer, greet_far, 0)

    in_copies = {}
    def fetch(i, src, dst):
        in_copies[i] = pltpu.make_async_copy(src, dst, in_sem.at[i])
        in_copies[i].start()

    w_hbm = (w0_hbm, w1_hbm, w2_hbm, w3_hbm)

    def fetch_weight(i, h, sem):
        part = (tp, other)[h]
        pltpu.make_async_copy(
            w_hbm[i].at[pl.ds(part * half, half), :], wv.at[i, pl.ds(h * half, half), :], sem
        ).start()

    def wait_weight(i):
        pltpu.make_async_copy(w_hbm[i], wv.at[i], wsem.at[i]).wait()

    fetch(0, x_hbm, x_ref)
    fetch(4, ld_hbm, ld_ref)
    fetch(2, rot_hbm, rot_ref)
    fetch(5, imap_hbm, imap_ref)
    fetch(1, gain_hbm, gain_ref)
    fetch_weight(0, 0, wsem.at[0])
    fetch_weight(0, 1, wsem.at[0])

    pl.semaphore_wait(barrier, 1 + 2 * (a + jnp.where(b == inner - 1, b, 0)))

    def ready_near(k, c):
        tell(near_ready, a * inner + k)
        return c

    def ready_far(k, c):
        tell(far_ready, k * inner + b)
        return c

    @pl.when((tp == 1) & (b == inner - 1))
    def _():
        lax.fori_loop(0, b, ready_near, 0)


    lax.fori_loop(0, a, ready_far, 0)

    when = lax.broadcasted_iota(jnp.int32, (rows, 2 * rows), 0)
    upto = lax.broadcasted_iota(jnp.int32, (rows, 2 * rows), 1)
    sums[...] = jnp.where(
        ((upto < rows) & (when <= upto)) | ((upto >= rows) & (when > upto - rows)), 1.0, 0.0
    ).astype(BF16)
    col = lax.broadcasted_iota(jnp.int32, (groups, chans), 1)
    row = lax.broadcasted_iota(jnp.int32, (groups, chans), 0)
    to_chan[...] = jnp.where((col >= row * gch) & (col < (row + 1) * gch), 1.0, 0.0).astype(BF16)

    def remote(src, dst, s, r, dev):
        return pltpu.make_async_remote_copy(
            src_ref=src, dst_ref=dst, send_sem=s, recv_sem=r, device_id=dev, device_id_type=MESH
        )

    in_copies[0].wait()
    x_copy = remote(x_ref, xr, x_sem.at[0], x_sem.at[1], partner)
    x_copy.start()

    fetch(3, init_hbm, init_ref)
    fetch(6, omap_hbm, omap_ref)
    fetch(7, skip_hbm, skip_ref)
    fetch(8, taps_hbm, taps_ref)
    for i in (1, 3, 2):
        for h in (0, 1):
            fetch_weight(i, h, wsem.at[i])
    for i, w, deep in ((1, co_hbm, cwide), (0, so_hbm, chans)):
        for h, part in ((0, tp), (1, other)):
            pltpu.make_async_copy(
                w.at[pl.ds(part * deep, deep), :], ov.at[pl.ds(2 * i * chans + h * deep, deep), :], osem.at[0]
            ).start()

    lane = lax.broadcasted_iota(jnp.int32, (1, LANES), 1)

    def pair_up(i, v):
        pairs[pl.ds(i * groups, groups), :] = v
        even = pairs[pl.ds(i * groups, prow, stride=2), :]
        odd = pairs[pl.ds(i * groups + 1, prow, stride=2), :]
        return jnp.where(lane < state, even, odd)

    def twice(v):
        return jnp.concatenate([v, v], axis=1)

    for i in (4, 2, 5, 1):
        in_copies[i].wait()
    ld = ld_ref[...]

    def time_sums(cols):
        added = jnp.dot(jnp.concatenate(split3(ld), axis=0), sums[:, cols], preferred_element_type=F32)
        return added[:groups] + added[groups : 2 * groups] + added[2 * groups :]

    def per_channel(v):
        hi, mid, _ = split3(v.T)
        return jnp.dot(hi, to_chan[...], preferred_element_type=F32) + jnp.dot(
            mid, to_chan[...], preferred_element_type=F32
        )

    gain = jnp.sqrt(minus_expm1(2.0 * ld))
    chan_end[...] = per_channel(gain * jnp.exp(time_sums(slice(rows, 2 * rows))))
    tot = pair_up(
        3, jnp.broadcast_to(jnp.exp(jnp.sum(ld, axis=1, keepdims=True)), (groups, LANES))
    )
    theta = pair_up(0, twice(rot_ref[...]))
    turn = jnp.cos(theta), jnp.sin(theta)
    step = turn
    for k in range(8):
        for i in (0, 1):
            powers[i, pl.ds(k * prow, prow), :] = step[i]
        step = cmul(step, turn) if k < 7 else step
    far_step16 = cmul(step, step)
    for i in (0, 1):
        powers[i, pl.ds(8 * prow, prow), :] = far_step16[i]
    whole = cpow(step, rows // 8)
    for r in range(prow):
        even = [powers[i, pl.ds(r, 8, stride=prow), :] for i in (0, 1)]
        eight = [powers[i, pl.ds(7 * prow + r, 1), :] for i in (0, 1)]
        sixteen = [powers[i, pl.ds(8 * prow + r, 1), :] for i in (0, 1)]
        odd = cmul(even, eight)
        for t in range(0, rows, 16):
            for i in (0, 1):
                tbl[t : t + 16, (2 * r + i) * LANES : (2 * r + i + 1) * LANES] = jnp.concatenate(
                    [even[i], odd[i]], axis=0
                ).astype(BF16)
            even = cmul(even, sixteen)
            odd = cmul(odd, sixteen)

    def spread_map(src, dst):
        dst[...] = jnp.zeros_like(dst)
        for b in range(blocks):
            for q in range(quads):
                g = b * per_block + 2 * q
                one = src[g].astype(F32)
                two = src[g + 1].astype(F32)
                one_r = jnp.concatenate([one[:, state:], one[:, :state]], axis=1)
                two_r = jnp.concatenate([two[:, state:], two[:, :state]], axis=1)
                low = lane < state
                re = jnp.concatenate([jnp.where(low, one, 0.0), jnp.where(low, 0.0, two_r)], axis=0)
                im = jnp.concatenate([jnp.where(low, one_r, 0.0), jnp.where(low, 0.0, two)], axis=0)
                at = pl.ds(b * LANES + q * 2 * gch, 2 * gch)
                dst[at, 2 * q * LANES : (2 * q + 1) * LANES] = re.astype(BF16)
                dst[at, (2 * q + 1) * LANES : (2 * q + 2) * LANES] = im.astype(BF16)

    spread_map(imap_ref, bd_in)
    own = x_ref[...].astype(F32)
    scaled = (own * gain_ref[:, pl.ds(pl.multiple_of(tp * half, LANES), half)]).astype(BF16)
    squares = jnp.sum(own * own, axis=1, keepdims=True)
    wait_weight(0)
    partial = jnp.dot(scaled, wv[0, :half], preferred_element_type=F32)
    acc[:, :half] = scaled

    x_copy.wait_recv()
    far_x = xr[...].astype(F32)
    scaled_far = (far_x * gain_ref[:, pl.ds(pl.multiple_of(other * half, LANES), half)]).astype(BF16)
    squares = squares + jnp.sum(far_x * far_x, axis=1, keepdims=True)
    scale = lax.rsqrt(squares / (2 * half) + EPS)

    acc[:, half:] = scaled_far
    total = partial + jnp.dot(scaled_far, wv[0, half:], preferred_element_type=F32)
    drive_in = (total * scale).astype(BF16)
    din[...] = drive_in
    ends_in = (drive_in.astype(F32) * chan_end[...]).astype(BF16).T
    for r in range(prow):
        q = r % quads
        at = slice(r * 2 * gch, (r + 1) * 2 * gch)
        seen = jnp.dot(
            ends_in[at], tbl[:, 2 * r * LANES : (2 * r + 2) * LANES], preferred_element_type=F32
        )
        m_re = bd_in[at, 2 * q * LANES : (2 * q + 1) * LANES].astype(F32)
        m_im = bd_in[at, (2 * q + 1) * LANES : (2 * q + 2) * LANES].astype(F32)
        c, d = seen[:, :LANES], seen[:, LANES:]
        rowed[0, r : r + 1, :] = jnp.sum(c * m_re + d * m_im, axis=0, keepdims=True)
        rowed[1, r : r + 1, :] = jnp.sum(c * m_im - d * m_re, axis=0, keepdims=True)
    e_re, e_im = cmul(whole, (rowed[0], rowed[1]))

    near_in[tp, b, pl.ds(0, prow), :] = e_re.astype(BF16)
    near_in[tp, b, pl.ds(prow, prow), :] = e_im.astype(BF16)
    fore = lax.rem(lax.broadcasted_iota(jnp.int32, (prow, LANES), 1), state) < state // 2

    def packed(v):
        hi, mid, _ = split3(v)
        return jnp.where(fore, hi.astype(F32), mid.astype(F32)).astype(BF16)

    near_in[tp, b, pl.ds(2 * prow, prow), :] = packed(tot)

    def wait_many(ref, sems, count, upto, sent):
        for j in range(1, upto + 1):
            @pl.when(count == j)
            def _():
                part = ref.at[pl.ds(0, j)]
                copy = remote(part, part, sems[0], sems[1], partner)
                copy.wait_send() if sent else copy.wait_recv()

    def near_copy(k):
        return remote(
            near_in.at[tp, b],
            near_in.at[tp, b],
            near_sem.at[2],
            near_sem.at[tp],
            {"sp": a * inner + k, "tp": 1},
        )

    def far_copy(k):
        return remote(
            far_out, far_in.at[a], far_sem.at[0], far_sem.at[1], {"sp": k * inner + b, "tp": 1}
        )

    near_from = jnp.where(a < last, 0, b + 1)
    near_upto = jnp.where(a < last, inner, b)
    @pl.when(b < inner - 1)
    def _():
        pl.semaphore_wait(near_ready, 1)

    def send_near(k, c):
        @pl.when((k != b) | ((tp == 0) & (a < last)))
        def _():
            near_copy(k).start()

        return c

    lax.fori_loop(near_from, inner, send_near, 0)

    in_copies[3].wait()
    aux[0], aux[1] = whole
    aux[2] = pair_up(1, twice(init_ref[0]))
    aux[3] = pair_up(2, twice(init_ref[1]))
    aux_copy = remote(aux, aux_far, aux_sem.at[0], aux_sem.at[1], partner)
    dup_copies = [
        remote(src, dst, dup_sem.at[0, (0, 1, 2, 2, 1)[i]], dup_sem.at[1, (0, 1, 2, 2, 1)[i]], partner)
        for i, (src, dst) in enumerate(
            (
                (tbl, table_far),
                (map_t.at[pl.ds(0, states), :], map_far.at[pl.ds(0, states), :]),
                (post.at[1], post_far.at[1]),
                (post.at[0], post_far.at[0]),
                (map_t.at[pl.ds(states, states), :], map_far.at[pl.ds(states, states), :]),
            )
        )
    ]

    def give(copy):
        @pl.when(tp == 0)
        def _():
            copy.start()

    waited = [
        remote(src, dst, dup_sem.at[0, i], dup_sem.at[1, i], partner)
        for i, (src, dst) in enumerate(((tbl, table_far), (map_t, map_far), (post, post_far)))
    ]

    give(aux_copy)

    def project(i):
        wait_weight(i)
        total = jnp.dot(acc[...], wv[i], preferred_element_type=F32)
        return (total * scale).astype(BF16)

    value = project(1)
    pre_gate = project(3)
    mixed = (pre_gate.astype(F32) * value.astype(F32)).astype(BF16).astype(F32)
    pad[pl.ds(8, rows), :] = mixed
    tail_copy = remote(
        pad.at[pl.ds(rows, 8), :],
        pad.at[pl.ds(0, 8), :],
        tail_sem.at[0],
        tail_sem.at[1],
        {"sp": lax.rem(sp + 1, n), "tp": tp},
    )

    @pl.when(hop_on)
    def _():
        pl.semaphore_wait(far_ready, 2 * (last - a))

    @pl.when(sp < n - 1)
    def _():
        tail_copy.start()

    give(dup_copies[0])

    for i in (6, 7):
        in_copies[i].wait()
    spread_map(omap_ref, bd_out)
    for k in range(blocks):
        map_t[2 * k * bstates : 2 * (k + 1) * bstates, :] = bd_out[k * LANES : (k + 1) * LANES, :].T
    give(dup_copies[1])

    ld = ld_ref[...]
    gain = jnp.sqrt(minus_expm1(2.0 * ld))
    late = per_channel(jnp.concatenate([jnp.exp(time_sums(slice(0, rows))), gain], axis=1))
    post[1] = late[:rows]
    give(dup_copies[2])
    chan_gain[...] = late[rows:]
    mags = split3(jnp.exp(ld).T)[:2]
    for k in range(blocks):
        col = lax.broadcasted_iota(jnp.int32, (groups, bstates), 1) + k * bstates
        row = lax.broadcasted_iota(jnp.int32, (groups, bstates), 0)
        spread = jnp.where(
            (col >= row * state) & (col < (row + 1) * state), 1.0, 0.0
        ).astype(BF16)
        m = jnp.dot(mags[0], spread, preferred_element_type=F32) + jnp.dot(
            mags[1], spread, preferred_element_type=F32
        )
        for q in range(quads):
            mag[pl.ds(k * quads + q, rows, stride=prow), :] = m[:, q * LANES : (q + 1) * LANES]

    zero = jnp.zeros((prow, LANES), F32)

    def unpacked(v):
        v = v.astype(F32)
        keep = lax.rem(lax.broadcasted_iota(jnp.int32, v.shape, 1), state) < state // 2
        return v + jnp.where(keep, pltpu.roll(v, LANES - state // 2, 1), pltpu.roll(v, state // 2, 1))

    def unpack_all(ref, count, index):
        packs = [
            ref[index(h, k) + (pl.ds(2 * prow, prow),)] for h in (0, 1) for k in range(count)
        ]
        v = unpacked(jnp.concatenate(packs, axis=0))
        for h in (0, 1):
            mags_in[h, : count * prow, :] = v[h * count * prow : (h + 1) * count * prow]

    def message(ref, h, k):
        return (
            ref[pl.ds(0, prow), :].astype(F32),
            ref[pl.ds(prow, prow), :].astype(F32),
            mags_in[h, pl.ds(pl.multiple_of(k * prow, prow), prow), :],
        )

    def send_far(k, c):
        far_copy(outer + a - k).start()
        return c

    def join_halves(turned, first):
        unpack_all(near_in, inner, lambda h, k: (h, k))

        def half_step(h, k, c):
            ends, mag_all, phase, mine = c[0:2], c[2], c[3:5], c[5:]
            k_re, k_im, k_mag = message(near_in.at[h, k], h, k)
            moved = cmul((turned[h][0] * k_mag, turned[h][1] * k_mag), ends)
            now = (moved[0] + k_re, moved[1] + k_im, mag_all * k_mag) + cmul(turned[h], phase)
            return now + tuple(jnp.where(k < b, v, w) for v, w in zip(now, mine))

        def near_step(k, c):
            return tuple(half_step(h, k, c[h]) for h in (0, 1))

        one = jnp.ones((prow, LANES), F32)
        begin = [tuple(jnp.where(a == 0, v, zero) for v in f) + (one, one, zero) for f in first]
        planes = lax.fori_loop(0, near_upto, near_step, tuple(v + v for v in begin))
        for h, plane in enumerate(planes):
            far_out[h, pl.ds(0, prow), :] = plane[0].astype(BF16)
            far_out[h, pl.ds(prow, prow), :] = plane[1].astype(BF16)
            far_out[h, pl.ds(2 * prow, prow), :] = packed(plane[2])
            for i in range(5):
                held[h, i] = plane[5 + i]

    def join_near():
        @pl.when(tp == 1)
        def _():
            for h in (1, 0):
                wait_many(
                    near_in.at[h],
                    (near_sem.at[2], near_sem.at[h]),
                    jnp.where(a < last, inner - h, b),
                    inner,
                    False,
                )
            join_halves(
                ((aux_far[0], aux_far[1]), whole), ((aux_far[2], aux_far[3]), (aux[2], aux[3]))
            )

        @pl.when((a < last) & (b < inner - 1))
        def _():
            pl.semaphore_wait(far_ready, 2 * (last - a))

        @pl.when((tp == 1) & (a < last))
        def _():
            lax.fori_loop(a + 1, outer, send_far, 0)

    @pl.when(tp == 1)
    def _():
        aux_copy.wait_recv()

    @pl.when(b > 1)
    def _():
        join_near()

    hc[0] = project(2)
    gained = (din[...].astype(F32) * chan_gain[...]).astype(BF16)
    for k in range(blocks):
        blk = jnp.dot(
            gained[:, k * LANES : (k + 1) * LANES],
            bd_in[k * LANES : (k + 1) * LANES, :],
            preferred_element_type=F32,
        )
        for q in range(quads):
            r = k * quads + q
            drv[pl.ds(r, rows, stride=pitch), :] = blk[:, 2 * q * LANES : (2 * q + 1) * LANES]
            drv[pl.ds(prow + r, rows, stride=pitch), :] = blk[
                :, (2 * q + 1) * LANES : (2 * q + 2) * LANES
            ]

    @pl.when(b == 1)
    def _():
        join_near()

    hc_copy = remote(hc.at[0], hc.at[1], hc_sem.at[0], hc_sem.at[1], partner)

    def convolve():
        @pl.when(sp == 0)
        def _():
            pad[pl.ds(0, 8), :] = jnp.zeros((8, cwide), F32)

        in_copies[8].wait()

        @pl.when(sp > 0)
        def _():
            tail_copy.wait_recv()

        conv = jnp.zeros((rows, cwide), F32)
        for k in range(width):
            conv = conv + pad[pl.ds(8 + k - (width - 1), rows), :] * taps_ref[k : k + 1, :].astype(F32)
        hc[0] = (hc[0].astype(F32) * conv).astype(BF16)
        hc_copy.start()

    even = lax.rem(b, 2) == 0

    @pl.when(jnp.logical_not(even))
    def _():
        convolve()

    give(dup_copies[4])

    def scan(t, h):
        m = mag[pl.ds(pl.multiple_of(t * prow, prow), prow), :]
        base = pl.multiple_of(t * pitch, 8)
        d_re = drv[pl.ds(base, prow), :]
        d_im = drv[pl.ds(base + prow, prow), :]
        f_re, f_im = m * turn[0], m * turn[1]
        new_re = (f_re * h[0] + d_re) - f_im * h[1]
        new_im = (f_re * h[1] + d_im) + f_im * h[0]
        drv[pl.ds(base, prow), :] = new_re
        drv[pl.ds(base + prow, prow), :] = new_im
        return new_re, new_im

    lax.fori_loop(0, rows, scan, (zero, zero), unroll=8)

    @pl.when(b == 0)
    def _():
        join_near()

    for k in range(blocks):
        cols = slice(k * LANES, (k + 1) * LANES)
        at = [half_row + k * quads + q for q in range(quads) for half_row in (0, prow)]
        st = jnp.concatenate(
            [drv[pl.ds(r, rows, stride=pitch), :].astype(BF16) for r in at], axis=1
        )
        read = jnp.dot(
            st, map_t[2 * k * bstates : 2 * (k + 1) * bstates, :], preferred_element_type=F32
        )
        post[0, :, cols] = read + skip_ref[:, cols] * din[:, cols].astype(F32)

    give(dup_copies[3])

    @pl.when(even)
    def _():
        convolve()

    pltpu.make_async_copy(ov, ov, osem.at[0]).wait()
    oacc[...] = jnp.dot(hc[0], ov[2 * chans : 2 * chans + cwide], preferred_element_type=F32)

    def add_far_conv():
        hc_copy.wait_recv()
        oacc[...] += jnp.dot(hc[1], ov[2 * chans + cwide :], preferred_element_type=F32)

    @pl.when(tp == 0)
    def _():
        add_far_conv()

    def entering(h, turned):
        plane_turn = cpow(turned, inner)

        def far_step(k, c):
            k_re, k_im, k_mag = message(far_in.at[k, h], h, k)
            moved = cmul((plane_turn[0] * k_mag, plane_turn[1] * k_mag), c)
            return moved[0] + k_re, moved[1] + k_im

        before = lax.fori_loop(0, a, far_step, (zero, zero))
        moved = cmul((held[h, 3] * held[h, 2], held[h, 4] * held[h, 2]), before)
        return held[h, 0] + moved[0], held[h, 1] + moved[1]

    def correct(h, table, mapped, local, slot):
        moved = []
        for k in range(blocks):
            turned = []
            for r in range(k * quads, (k + 1) * quads):
                c, d = (
                    table[:, (2 * r + i) * LANES : (2 * r + i + 1) * LANES].reshape(rows // 16, 16, LANES)
                    for i in (0, 1)
                )
                h_re, h_im = (
                    jnp.broadcast_to(enter[h, i, r : r + 1, :], (16, LANES)).astype(BF16)[None]
                    for i in (0, 1)
                )
                turned += cmul((c, d), (h_re, h_im))
            moved.append(
                jnp.dot(
                    jnp.concatenate([v.reshape(rows, LANES) for v in turned], axis=1),
                    mapped[2 * k * bstates : 2 * (k + 1) * bstates, :],
                    preferred_element_type=F32,
                )
            )
        made = []
        for k in range(blocks):
            cols = slice(k * LANES, (k + 1) * LANES)
            made.append(gelu(local[0, :, cols] + local[1, :, cols] * moved[k]).astype(BF16))
            hs[slot, :, cols] = made[k]
        return made

    enter_copy = remote(enter.at[0], enter.at[0], enter_sem.at[0], enter_sem.at[1], partner)

    @pl.when(tp == 1)
    def _():
        wait_many(far_in, (far_sem.at[0], far_sem.at[1]), a, last, False)
        unpack_all(far_in, last, lambda h, k: (k, h))
        enter[0, 0], enter[0, 1] = entering(0, (aux_far[0], aux_far[1]))

        @pl.when(sp > 0)
        def _():
            enter_copy.start()

        enter[1, 0], enter[1, 1] = entering(1, whole)

    @pl.when((tp == 0) & (sp > 0))
    def _():
        enter_copy.wait_recv()

    @pl.when((tp == 0) & (sp == 0))
    def _():
        enter[0, 0], enter[0, 1] = aux[2], aux[3]

    hs_copy = remote(hs.at[0], hs.at[1], hs_sem.at[0], hs_sem.at[1], partner)

    def add_own(blks):
        oacc[...] += jnp.dot(
            jnp.concatenate(blks, axis=1), ov[:chans], preferred_element_type=F32
        )

    @pl.when(tp == 1)
    def _():
        correct(1, tbl, map_t, post, 0)
        hs_copy.start()
        for copy in waited:
            copy.wait_recv()
        hc_copy.wait_recv()
        correct(0, table_far, map_far, post_far, 1)
        oacc[...] += jnp.dot(hs[0], ov[:chans], preferred_element_type=F32) + jnp.dot(
            hc[1], ov[2 * chans + cwide :], preferred_element_type=F32
        )

    @pl.when(tp == 0)
    def _():
        add_own(correct(0, tbl, map_t, post, 0))

    @pl.when(tp == 0)
    def _():
        hs_copy.wait_recv()

    out_ref[...] = (oacc[...] + jnp.dot(hs[1], ov[chans : 2 * chans], preferred_element_type=F32)).astype(BF16)

    x_copy.wait_send()
    hc_copy.wait_send()

    @pl.when(tp == 1)
    def _():
        hs_copy.wait_send()

    @pl.when((tp == 1) & (sp > 0))
    def _():
        enter_copy.wait_send()

    @pl.when(tp == 0)
    def _():
        aux_copy.wait_send()
        for copy in waited:
            copy.wait_send()

    @pl.when(sp < n - 1)
    def _():
        tail_copy.wait_send()

    wait_many(
        near_in.at[0],
        (near_sem.at[2], near_sem.at[0]),
        jnp.where(a < last, inner - tp, inner - 1 - b),
        inner,
        True,
    )

    @pl.when(tp == 1)
    def _():
        wait_many(far_in, (far_sem.at[0], far_sem.at[1]), last - a, last, True)


def on_device(
    activations,
    norm_gain,
    state_proj,
    value_proj,
    post_gate_proj,
    pre_gate_proj,
    input_map,
    output_map,
    skip_gain,
    rotation,
    log_decay,
    initial_state,
    conv_taps,
    state_out,
    conv_out,
):
    n = lax.axis_size("sp")
    rows, half = activations.shape
    groups, state = rotation.shape
    chans = state_proj.shape[1]
    cwide = value_proj.shape[1]
    outs = state_out.shape[1]
    states = groups * state
    prow = states // LANES
    inner = inner_of(n)
    bdw = 2 * states // (chans // LANES)
    vmem = pl.BlockSpec(memory_space=pltpu.VMEM)
    hbm = pl.BlockSpec(memory_space=pl.ANY)
    dma = pltpu.SemaphoreType.DMA
    return pl.pallas_call(
        functools.partial(kernel, n),
        out_shape=pltpu.VMEM((rows, outs), BF16),
        in_specs=[hbm] * 15,
        out_specs=vmem,
        scratch_shapes=[
            pltpu.VMEM((rows, half), BF16),
            pltpu.VMEM((1, 2 * half), F32),
            pltpu.VMEM(input_map.shape, BF16),
            pltpu.VMEM((groups, output_map.shape[2], output_map.shape[1]), F32),
            pltpu.VMEM((1, chans), F32),
            pltpu.VMEM((groups, state), F32),
            pltpu.VMEM((groups, rows), F32),
            pltpu.VMEM(initial_state.shape, F32),
            pltpu.VMEM(conv_taps.shape, BF16),
            pltpu.VMEM((4, 2 * half, chans), BF16),
            pltpu.VMEM((2 * chans + 2 * cwide, outs), BF16),
            pltpu.VMEM((rows, half), BF16),
            pltpu.VMEM((rows, 2 * half), BF16),
            pltpu.VMEM((rows, chans), BF16),
            pltpu.VMEM((chans, bdw), BF16),
            pltpu.VMEM((chans, bdw), BF16),
            pltpu.VMEM((2 * states, LANES), BF16),
            pltpu.VMEM((rows, 2 * states), BF16),
            pltpu.VMEM((2, 9 * prow, LANES), F32),
            pltpu.VMEM((rows, chans), F32),
            pltpu.VMEM((rows, chans), F32),
            pltpu.VMEM((2, prow, LANES), F32),
            pltpu.VMEM((2, rows, chans), F32),
            pltpu.VMEM((rows, 2 * states), BF16),
            pltpu.VMEM((2 * states, LANES), BF16),
            pltpu.VMEM((2, rows, chans), F32),
            pltpu.VMEM((4, prow, LANES), F32),
            pltpu.VMEM((4, prow, LANES), F32),
            pltpu.VMEM((2, max(inner, n // inner) * prow, LANES), F32),
            pltpu.VMEM((2, 5, prow, LANES), F32),
            pltpu.VMEM((2, 2, prow, LANES), F32),
            pltpu.VMEM((rows, 2 * rows), BF16),
            pltpu.VMEM((groups, chans), BF16),
            pltpu.VMEM((rows * prow, LANES), F32),
            pltpu.VMEM((rows * (2 * prow + 8), LANES), F32),
            pltpu.VMEM((4 * groups, LANES), F32),
            pltpu.VMEM((rows + 8, cwide), F32),
            pltpu.VMEM((2, inner, 3 * prow, LANES), BF16),
            pltpu.VMEM((n // inner, 2, 3 * prow, LANES), BF16),
            pltpu.VMEM((2, 3 * prow, LANES), BF16),
            pltpu.VMEM((2, rows, chans), BF16),
            pltpu.VMEM((2, rows, cwide), BF16),
            pltpu.VMEM((rows, outs), F32),
            dma((9,)),
            dma((4,)),
            dma((1,)),
            dma((2,)),
            dma((2,)),
            dma((2,)),
            dma((2,)),
            dma((3,)),
            dma((2,)),
            dma((2,)),
            dma((2,)),
            dma((2, 3)),
            pltpu.SemaphoreType.REGULAR,
            pltpu.SemaphoreType.REGULAR,
        ],
        compiler_params=pltpu.CompilerParams(collective_id=0, has_side_effects=True),
    )(
        activations,
        norm_gain.reshape(1, -1),
        state_proj,
        value_proj,
        post_gate_proj,
        pre_gate_proj,
        input_map,
        jnp.swapaxes(output_map, 1, 2),
        skip_gain.reshape(1, -1),
        rotation,
        jnp.swapaxes(log_decay, 0, 1),
        initial_state,
        conv_taps,
        state_out,
        conv_out,
    )


def solution(mesh):
    return jax.shard_map(
        on_device,
        mesh=mesh,
        in_specs=(
            P("sp", "tp"),
            P(),
            P(None, "tp"),
            P(None, "tp"),
            P(None, "tp"),
            P(None, "tp"),
            P("tp", None, None),
            P("tp", None, None),
            P("tp"),
            P("tp", None),
            P("sp", "tp"),
            P(None, "tp", None),
            P(None, "tp"),
            P(None, "tp"),
            P(None, "tp"),
        ),
        out_specs=P("sp", "tp"),
        check_vma=False,
    )
```

```python
import functools

import jax
import jax.numpy as jnp
from jax import lax
from jax.experimental import pallas as pl
from jax.experimental.pallas import tpu as pltpu
from jax.sharding import PartitionSpec as P

EPS = 1e-06
LANES = 128
MESH = pl.DeviceIdType.MESH
F32 = jnp.float32
BF16 = jnp.bfloat16


def minus_expm1(y):
    poly = jnp.ones_like(y)
    for k in range(11, 1, -1):
        poly = 1.0 + poly * y * (1.0 / k)
    return jnp.where(y > -0.5, -y * poly, 1.0 - jnp.exp(y))


def split3(v):
    hi = v.astype(BF16)
    rest = v - hi.astype(F32)
    mid = rest.astype(BF16)
    low = (rest - mid.astype(F32)).astype(BF16)
    return hi, mid, low


def cmul(a, b):
    return a[0] * b[0] - a[1] * b[1], a[0] * b[1] + a[1] * b[0]


def cpow(base, count):
    result = None
    while count:
        if count & 1:
            result = base if result is None else cmul(result, base)
        count >>= 1
        if count:
            base = cmul(base, base)
    return result


def inner_of(n):
    return max(d for d in range(1, n + 1) if n % d == 0 and d * d <= n)


def gelu(x):
    return 0.5 * x * (1.0 + jnp.tanh(0.7978845608028654 * (x + 0.044715 * x * x * x)))


def kernel(
    n,
    x_hbm,
    gain_hbm,
    w0_hbm,
    w1_hbm,
    w2_hbm,
    w3_hbm,
    imap_hbm,
    omap_hbm,
    skip_hbm,
    rot_hbm,
    ld_hbm,
    init_hbm,
    taps_hbm,
    so_hbm,
    co_hbm,
    out_ref,
    x_ref,
    gain_ref,
    imap_ref,
    omap_ref,
    skip_ref,
    rot_ref,
    ld_ref,
    init_ref,
    taps_ref,
    wv,
    ov,
    xr,
    acc,
    din,
    bd_in,
    bd_out,
    map_t,
    tbl,
    powers,
    chan_end,
    chan_gain,
    rowed,
    post,
    table_far,
    map_far,
    post_far,
    aux,
    aux_far,
    mags_in,
    held,
    enter,
    sums,
    to_chan,
    mag,
    drv,
    pairs,
    pad,
    near_in,
    far_in,
    far_out,
    hs,
    hc,
    oacc,
    in_sem,
    wsem,
    osem,
    x_sem,
    tail_sem,
    hc_sem,
    hs_sem,
    near_sem,
    far_sem,
    aux_sem,
    enter_sem,
    dup_sem,
    near_ready,
    far_ready,
):
    sp, tp = lax.axis_index("sp"), lax.axis_index("tp")
    other = 1 - tp
    rows, half = x_ref.shape
    groups, state = rot_ref.shape
    gch = imap_ref.shape[1]
    chans = groups * gch
    states = groups * state
    prow = states // LANES
    per_block = LANES // gch
    blocks = groups // per_block
    quads = prow // blocks
    pitch = drv.shape[0] // rows
    bstates = quads * LANES
    cwide = taps_ref.shape[1]
    width = taps_ref.shape[0]

    barrier = pltpu.get_barrier_semaphore()
    partner = {"sp": sp, "tp": other}

    inner = inner_of(n)
    outer = n // inner
    a, b = lax.div(sp, inner), lax.rem(sp, inner)
    last = outer - 1

    hop_on = (b == inner - 1) & (a < last)

    def tell(sem, j):
        for t in (0, 1):
            pl.semaphore_signal(sem, inc=1, device_id={"sp": j, "tp": t}, device_id_type=MESH)

    def greet_far(k, c):
        tell(barrier, k * inner + b)
        return c

    pl.semaphore_signal(barrier, inc=1, device_id=partner, device_id_type=MESH)

    @pl.when(b < inner - 1)
    def _():
        tell(barrier, sp + inner - 1 - b)

    lax.fori_loop(a + 1, outer, greet_far, 0)

    in_copies = {}
    def fetch(i, src, dst):
        in_copies[i] = pltpu.make_async_copy(src, dst, in_sem.at[i])
        in_copies[i].start()

    w_hbm = (w0_hbm, w1_hbm, w2_hbm, w3_hbm)

    def fetch_weight(i, h, sem):
        part = (tp, other)[h]
        pltpu.make_async_copy(
            w_hbm[i].at[pl.ds(part * half, half), :], wv.at[i, pl.ds(h * half, half), :], sem
        ).start()

    def wait_weight(i):
        pltpu.make_async_copy(w_hbm[i], wv.at[i], wsem.at[i]).wait()

    fetch(0, x_hbm, x_ref)
    fetch(4, ld_hbm, ld_ref)
    fetch(2, rot_hbm, rot_ref)
    fetch(5, imap_hbm, imap_ref)
    fetch(1, gain_hbm, gain_ref)
    fetch_weight(0, 0, wsem.at[0])
    fetch_weight(0, 1, wsem.at[0])

    pl.semaphore_wait(barrier, 1 + 2 * (a + jnp.where(b == inner - 1, b, 0)))

    def ready_near(k, c):
        tell(near_ready, a * inner + k)
        return c

    def ready_far(k, c):
        tell(far_ready, k * inner + b)
        return c

    @pl.when((tp == 1) & (b == inner - 1))
    def _():
        lax.fori_loop(0, b, ready_near, 0)


    lax.fori_loop(0, a, ready_far, 0)

    bd_in[...] = jnp.zeros_like(bd_in)
    bd_out[...] = jnp.zeros_like(bd_out)
    when = lax.broadcasted_iota(jnp.int32, (rows, 2 * rows), 0)
    upto = lax.broadcasted_iota(jnp.int32, (rows, 2 * rows), 1)
    sums[...] = jnp.where(
        ((upto < rows) & (when <= upto)) | ((upto >= rows) & (when > upto - rows)), 1.0, 0.0
    ).astype(BF16)
    col = lax.broadcasted_iota(jnp.int32, (groups, chans), 1)
    row = lax.broadcasted_iota(jnp.int32, (groups, chans), 0)
    to_chan[...] = jnp.where((col >= row * gch) & (col < (row + 1) * gch), 1.0, 0.0).astype(BF16)

    def remote(src, dst, s, r, dev):
        return pltpu.make_async_remote_copy(
            src_ref=src, dst_ref=dst, send_sem=s, recv_sem=r, device_id=dev, device_id_type=MESH
        )

    in_copies[0].wait()
    x_copy = remote(x_ref, xr, x_sem.at[0], x_sem.at[1], partner)
    x_copy.start()

    fetch(3, init_hbm, init_ref)
    fetch(6, omap_hbm, omap_ref)
    fetch(7, skip_hbm, skip_ref)
    fetch(8, taps_hbm, taps_ref)
    for i in (1, 3, 2):
        for h in (0, 1):
            fetch_weight(i, h, wsem.at[i])
    for i, w, deep in ((1, co_hbm, cwide), (0, so_hbm, chans)):
        for h, part in ((0, tp), (1, other)):
            pltpu.make_async_copy(
                w.at[pl.ds(part * deep, deep), :], ov.at[pl.ds(2 * i * chans + h * deep, deep), :], osem.at[0]
            ).start()

    lane = lax.broadcasted_iota(jnp.int32, (1, LANES), 1)

    def pair_up(i, v):
        pairs[pl.ds(i * groups, groups), :] = v
        even = pairs[pl.ds(i * groups, prow, stride=2), :]
        odd = pairs[pl.ds(i * groups + 1, prow, stride=2), :]
        return jnp.where(lane < state, even, odd)

    def twice(v):
        return jnp.concatenate([v, v], axis=1)

    for i in (4, 2, 5, 1):
        in_copies[i].wait()
    ld = ld_ref[...]

    def time_sums(cols):
        added = jnp.dot(jnp.concatenate(split3(ld), axis=0), sums[:, cols], preferred_element_type=F32)
        return added[:groups] + added[groups : 2 * groups] + added[2 * groups :]

    def per_channel(v):
        hi, mid, _ = split3(v.T)
        return jnp.dot(hi, to_chan[...], preferred_element_type=F32) + jnp.dot(
            mid, to_chan[...], preferred_element_type=F32
        )

    gain = jnp.sqrt(minus_expm1(2.0 * ld))
    chan_end[...] = per_channel(gain * jnp.exp(time_sums(slice(rows, 2 * rows))))
    tot = pair_up(
        3, jnp.broadcast_to(jnp.exp(jnp.sum(ld, axis=1, keepdims=True)), (groups, LANES))
    )
    theta = pair_up(0, twice(rot_ref[...]))
    turn = jnp.cos(theta), jnp.sin(theta)
    step = turn
    for k in range(8):
        for i in (0, 1):
            powers[i, pl.ds(k * prow, prow), :] = step[i]
        step = cmul(step, turn) if k < 7 else step
    far_step16 = cmul(step, step)
    for i in (0, 1):
        powers[i, pl.ds(8 * prow, prow), :] = far_step16[i]
    whole = cpow(step, rows // 8)
    for r in range(prow):
        even = [powers[i, pl.ds(r, 8, stride=prow), :] for i in (0, 1)]
        eight = [powers[i, pl.ds(7 * prow + r, 1), :] for i in (0, 1)]
        sixteen = [powers[i, pl.ds(8 * prow + r, 1), :] for i in (0, 1)]
        odd = cmul(even, eight)
        for t in range(0, rows, 16):
            for i in (0, 1):
                tbl[t : t + 16, (2 * r + i) * LANES : (2 * r + i + 1) * LANES] = jnp.concatenate(
                    [even[i], odd[i]], axis=0
                ).astype(BF16)
            even = cmul(even, sixteen)
            odd = cmul(odd, sixteen)

    def spread_map(src, dst):
        for b in range(blocks):
            for q in range(quads):
                g = b * per_block + 2 * q
                one = src[g].astype(F32)
                two = src[g + 1].astype(F32)
                one_r = jnp.concatenate([one[:, state:], one[:, :state]], axis=1)
                two_r = jnp.concatenate([two[:, state:], two[:, :state]], axis=1)
                low = lane < state
                re = jnp.concatenate([jnp.where(low, one, 0.0), jnp.where(low, 0.0, two_r)], axis=0)
                im = jnp.concatenate([jnp.where(low, one_r, 0.0), jnp.where(low, 0.0, two)], axis=0)
                at = pl.ds(b * LANES + q * 2 * gch, 2 * gch)
                dst[at, 2 * q * LANES : (2 * q + 1) * LANES] = re.astype(BF16)
                dst[at, (2 * q + 1) * LANES : (2 * q + 2) * LANES] = im.astype(BF16)

    spread_map(imap_ref, bd_in)
    own = x_ref[...].astype(F32)
    scaled = (own * gain_ref[:, pl.ds(pl.multiple_of(tp * half, LANES), half)]).astype(BF16)
    squares = jnp.sum(own * own, axis=1, keepdims=True)
    wait_weight(0)
    partial = jnp.dot(scaled, wv[0, :half], preferred_element_type=F32)
    acc[:, :half] = scaled

    x_copy.wait_recv()
    far_x = xr[...].astype(F32)
    scaled_far = (far_x * gain_ref[:, pl.ds(pl.multiple_of(other * half, LANES), half)]).astype(BF16)
    squares = squares + jnp.sum(far_x * far_x, axis=1, keepdims=True)
    scale = lax.rsqrt(squares / (2 * half) + EPS)

    acc[:, half:] = scaled_far
    total = partial + jnp.dot(scaled_far, wv[0, half:], preferred_element_type=F32)
    drive_in = (total * scale).astype(BF16)
    din[...] = drive_in
    ends_in = (drive_in.astype(F32) * chan_end[...]).astype(BF16).T
    for r in range(prow):
        q = r % quads
        at = slice(r * 2 * gch, (r + 1) * 2 * gch)
        seen = jnp.dot(
            ends_in[at], tbl[:, 2 * r * LANES : (2 * r + 2) * LANES], preferred_element_type=F32
        )
        m_re = bd_in[at, 2 * q * LANES : (2 * q + 1) * LANES].astype(F32)
        m_im = bd_in[at, (2 * q + 1) * LANES : (2 * q + 2) * LANES].astype(F32)
        c, d = seen[:, :LANES], seen[:, LANES:]
        rowed[0, r : r + 1, :] = jnp.sum(c * m_re + d * m_im, axis=0, keepdims=True)
        rowed[1, r : r + 1, :] = jnp.sum(c * m_im - d * m_re, axis=0, keepdims=True)
    e_re, e_im = cmul(whole, (rowed[0], rowed[1]))

    near_in[tp, b, pl.ds(0, prow), :] = e_re.astype(BF16)
    near_in[tp, b, pl.ds(prow, prow), :] = e_im.astype(BF16)
    fore = lax.rem(lax.broadcasted_iota(jnp.int32, (prow, LANES), 1), state) < state // 2

    def packed(v):
        hi, mid, _ = split3(v)
        return jnp.where(fore, hi.astype(F32), mid.astype(F32)).astype(BF16)

    near_in[tp, b, pl.ds(2 * prow, prow), :] = packed(tot)

    def wait_many(ref, sems, count, upto, sent):
        for j in range(1, upto + 1):
            @pl.when(count == j)
            def _():
                part = ref.at[pl.ds(0, j)]
                copy = remote(part, part, sems[0], sems[1], partner)
                copy.wait_send() if sent else copy.wait_recv()

    def near_copy(k):
        return remote(
            near_in.at[tp, b],
            near_in.at[tp, b],
            near_sem.at[2],
            near_sem.at[tp],
            {"sp": a * inner + k, "tp": 1},
        )

    def far_copy(k):
        return remote(
            far_out, far_in.at[a], far_sem.at[0], far_sem.at[1], {"sp": k * inner + b, "tp": 1}
        )

    near_from = jnp.where(a < last, 0, b + 1)
    near_upto = jnp.where(a < last, inner, b)
    @pl.when(b < inner - 1)
    def _():
        pl.semaphore_wait(near_ready, 1)

    def send_near(k, c):
        @pl.when((k != b) | ((tp == 0) & (a < last)))
        def _():
            near_copy(k).start()

        return c

    lax.fori_loop(near_from, inner, send_near, 0)

    in_copies[3].wait()
    aux[0], aux[1] = whole
    aux[2] = pair_up(1, twice(init_ref[0]))
    aux[3] = pair_up(2, twice(init_ref[1]))
    aux_copy = remote(aux, aux_far, aux_sem.at[0], aux_sem.at[1], partner)
    dup_copies = [
        remote(src, dst, dup_sem.at[0, (0, 1, 2, 2, 1)[i]], dup_sem.at[1, (0, 1, 2, 2, 1)[i]], partner)
        for i, (src, dst) in enumerate(
            (
                (tbl, table_far),
                (map_t.at[pl.ds(0, states), :], map_far.at[pl.ds(0, states), :]),
                (post.at[1], post_far.at[1]),
                (post.at[0], post_far.at[0]),
                (map_t.at[pl.ds(states, states), :], map_far.at[pl.ds(states, states), :]),
            )
        )
    ]

    def give(copy):
        @pl.when(tp == 0)
        def _():
            copy.start()

    waited = [
        remote(src, dst, dup_sem.at[0, i], dup_sem.at[1, i], partner)
        for i, (src, dst) in enumerate(((tbl, table_far), (map_t, map_far), (post, post_far)))
    ]

    give(aux_copy)

    def project(i):
        wait_weight(i)
        total = jnp.dot(acc[...], wv[i], preferred_element_type=F32)
        return (total * scale).astype(BF16)

    value = project(1)
    pre_gate = project(3)
    mixed = (pre_gate.astype(F32) * value.astype(F32)).astype(BF16).astype(F32)
    pad[pl.ds(8, rows), :] = mixed
    tail_copy = remote(
        pad.at[pl.ds(rows, 8), :],
        pad.at[pl.ds(0, 8), :],
        tail_sem.at[0],
        tail_sem.at[1],
        {"sp": lax.rem(sp + 1, n), "tp": tp},
    )

    @pl.when(hop_on)
    def _():
        pl.semaphore_wait(far_ready, 2 * (last - a))

    @pl.when(sp < n - 1)
    def _():
        tail_copy.start()

    give(dup_copies[0])

    for i in (6, 7):
        in_copies[i].wait()
    spread_map(omap_ref, bd_out)
    for k in range(blocks):
        map_t[2 * k * bstates : 2 * (k + 1) * bstates, :] = bd_out[k * LANES : (k + 1) * LANES, :].T
    give(dup_copies[1])

    ld = ld_ref[...]
    gain = jnp.sqrt(minus_expm1(2.0 * ld))
    late = per_channel(jnp.concatenate([jnp.exp(time_sums(slice(0, rows))), gain], axis=1))
    post[1] = late[:rows]
    give(dup_copies[2])
    chan_gain[...] = late[rows:]
    mags = split3(jnp.exp(ld).T)[:2]
    for k in range(blocks):
        col = lax.broadcasted_iota(jnp.int32, (groups, bstates), 1) + k * bstates
        row = lax.broadcasted_iota(jnp.int32, (groups, bstates), 0)
        spread = jnp.where(
            (col >= row * state) & (col < (row + 1) * state), 1.0, 0.0
        ).astype(BF16)
        m = jnp.dot(mags[0], spread, preferred_element_type=F32) + jnp.dot(
            mags[1], spread, preferred_element_type=F32
        )
        for q in range(quads):
            mag[pl.ds(k * quads + q, rows, stride=prow), :] = m[:, q * LANES : (q + 1) * LANES]

    zero = jnp.zeros((prow, LANES), F32)

    def unpacked(v):
        v = v.astype(F32)
        keep = lax.rem(lax.broadcasted_iota(jnp.int32, v.shape, 1), state) < state // 2
        return v + jnp.where(keep, pltpu.roll(v, LANES - state // 2, 1), pltpu.roll(v, state // 2, 1))

    def unpack_all(ref, count, index):
        packs = [
            ref[index(h, k) + (pl.ds(2 * prow, prow),)] for h in (0, 1) for k in range(count)
        ]
        v = unpacked(jnp.concatenate(packs, axis=0))
        for h in (0, 1):
            mags_in[h, : count * prow, :] = v[h * count * prow : (h + 1) * count * prow]

    def message(ref, h, k):
        return (
            ref[pl.ds(0, prow), :].astype(F32),
            ref[pl.ds(prow, prow), :].astype(F32),
            mags_in[h, pl.ds(pl.multiple_of(k * prow, prow), prow), :],
        )

    def send_far(k, c):
        far_copy(outer + a - k).start()
        return c

    def join_halves(turned, first):
        unpack_all(near_in, inner, lambda h, k: (h, k))

        def half_step(h, k, c):
            ends, mag_all, phase, mine = c[0:2], c[2], c[3:5], c[5:]
            k_re, k_im, k_mag = message(near_in.at[h, k], h, k)
            moved = cmul((turned[h][0] * k_mag, turned[h][1] * k_mag), ends)
            now = (moved[0] + k_re, moved[1] + k_im, mag_all * k_mag) + cmul(turned[h], phase)
            return now + tuple(jnp.where(k < b, v, w) for v, w in zip(now, mine))

        def near_step(k, c):
            return tuple(half_step(h, k, c[h]) for h in (0, 1))

        one = jnp.ones((prow, LANES), F32)
        begin = [tuple(jnp.where(a == 0, v, zero) for v in f) + (one, one, zero) for f in first]
        planes = lax.fori_loop(0, near_upto, near_step, tuple(v + v for v in begin))
        for h, plane in enumerate(planes):
            far_out[h, pl.ds(0, prow), :] = plane[0].astype(BF16)
            far_out[h, pl.ds(prow, prow), :] = plane[1].astype(BF16)
            far_out[h, pl.ds(2 * prow, prow), :] = packed(plane[2])
            for i in range(5):
                held[h, i] = plane[5 + i]

    def join_near():
        @pl.when(tp == 1)
        def _():
            for h in (1, 0):
                wait_many(
                    near_in.at[h],
                    (near_sem.at[2], near_sem.at[h]),
                    jnp.where(a < last, inner - h, b),
                    inner,
                    False,
                )
            join_halves(
                ((aux_far[0], aux_far[1]), whole), ((aux_far[2], aux_far[3]), (aux[2], aux[3]))
            )

        @pl.when((a < last) & (b < inner - 1))
        def _():
            pl.semaphore_wait(far_ready, 2 * (last - a))

        @pl.when((tp == 1) & (a < last))
        def _():
            lax.fori_loop(a + 1, outer, send_far, 0)

    @pl.when(tp == 1)
    def _():
        aux_copy.wait_recv()

    @pl.when(b > 1)
    def _():
        join_near()

    hc[0] = project(2)
    gained = (din[...].astype(F32) * chan_gain[...]).astype(BF16)
    for k in range(blocks):
        blk = jnp.dot(
            gained[:, k * LANES : (k + 1) * LANES],
            bd_in[k * LANES : (k + 1) * LANES, :],
            preferred_element_type=F32,
        )
        for q in range(quads):
            r = k * quads + q
            drv[pl.ds(r, rows, stride=pitch), :] = blk[:, 2 * q * LANES : (2 * q + 1) * LANES]
            drv[pl.ds(prow + r, rows, stride=pitch), :] = blk[
                :, (2 * q + 1) * LANES : (2 * q + 2) * LANES
            ]

    @pl.when(b == 1)
    def _():
        join_near()

    hc_copy = remote(hc.at[0], hc.at[1], hc_sem.at[0], hc_sem.at[1], partner)

    def convolve():
        @pl.when(sp == 0)
        def _():
            pad[pl.ds(0, 8), :] = jnp.zeros((8, cwide), F32)

        in_copies[8].wait()

        @pl.when(sp > 0)
        def _():
            tail_copy.wait_recv()

        conv = jnp.zeros((rows, cwide), F32)
        for k in range(width):
            conv = conv + pad[pl.ds(8 + k - (width - 1), rows), :] * taps_ref[k : k + 1, :].astype(F32)
        hc[0] = (hc[0].astype(F32) * conv).astype(BF16)
        hc_copy.start()

    even = (lax.rem(b, 2) == 0) & (sp > 0)

    @pl.when(jnp.logical_not(even))
    def _():
        convolve()

    give(dup_copies[4])

    def scan(t, h):
        m = mag[pl.ds(pl.multiple_of(t * prow, prow), prow), :]
        base = pl.multiple_of(t * pitch, 8)
        d_re = drv[pl.ds(base, prow), :]
        d_im = drv[pl.ds(base + prow, prow), :]
        f_re, f_im = m * turn[0], m * turn[1]
        new_re = (f_re * h[0] + d_re) - f_im * h[1]
        new_im = (f_re * h[1] + d_im) + f_im * h[0]
        drv[pl.ds(base, prow), :] = new_re
        drv[pl.ds(base + prow, prow), :] = new_im
        return new_re, new_im

    lax.fori_loop(0, rows, scan, (zero, zero), unroll=8)

    @pl.when(b == 0)
    def _():
        join_near()

    for k in range(blocks):
        cols = slice(k * LANES, (k + 1) * LANES)
        at = [half_row + k * quads + q for q in range(quads) for half_row in (0, prow)]
        st = jnp.concatenate(
            [drv[pl.ds(r, rows, stride=pitch), :].astype(BF16) for r in at], axis=1
        )
        read = jnp.dot(
            st, map_t[2 * k * bstates : 2 * (k + 1) * bstates, :], preferred_element_type=F32
        )
        post[0, :, cols] = read + skip_ref[:, cols] * din[:, cols].astype(F32)

    give(dup_copies[3])

    @pl.when(even)
    def _():
        convolve()

    pltpu.make_async_copy(ov, ov, osem.at[0]).wait()
    oacc[...] = jnp.dot(hc[0], ov[2 * chans : 2 * chans + cwide], preferred_element_type=F32)

    def add_far_conv():
        hc_copy.wait_recv()
        oacc[...] += jnp.dot(hc[1], ov[2 * chans + cwide :], preferred_element_type=F32)

    @pl.when(tp == 0)
    def _():
        add_far_conv()

    def entering(h, turned):
        plane_turn = cpow(turned, inner)

        def far_step(k, c):
            k_re, k_im, k_mag = message(far_in.at[k, h], h, k)
            moved = cmul((plane_turn[0] * k_mag, plane_turn[1] * k_mag), c)
            return moved[0] + k_re, moved[1] + k_im

        before = lax.fori_loop(0, a, far_step, (zero, zero))
        moved = cmul((held[h, 3] * held[h, 2], held[h, 4] * held[h, 2]), before)
        return held[h, 0] + moved[0], held[h, 1] + moved[1]

    def correct(h, table, mapped, local, slot):
        moved = []
        for k in range(blocks):
            turned = []
            for r in range(k * quads, (k + 1) * quads):
                c, d = (
                    table[:, (2 * r + i) * LANES : (2 * r + i + 1) * LANES].reshape(rows // 16, 16, LANES)
                    for i in (0, 1)
                )
                h_re, h_im = (
                    jnp.broadcast_to(enter[h, i, r : r + 1, :], (16, LANES)).astype(BF16)[None]
                    for i in (0, 1)
                )
                turned += cmul((c, d), (h_re, h_im))
            moved.append(
                jnp.dot(
                    jnp.concatenate([v.reshape(rows, LANES) for v in turned], axis=1),
                    mapped[2 * k * bstates : 2 * (k + 1) * bstates, :],
                    preferred_element_type=F32,
                )
            )
        made = []
        for k in range(blocks):
            cols = slice(k * LANES, (k + 1) * LANES)
            made.append(gelu(local[0, :, cols] + local[1, :, cols] * moved[k]).astype(BF16))
            hs[slot, :, cols] = made[k]
        return made

    enter_copy = remote(enter.at[0], enter.at[0], enter_sem.at[0], enter_sem.at[1], partner)

    @pl.when(tp == 1)
    def _():
        wait_many(far_in, (far_sem.at[0], far_sem.at[1]), a, last, False)
        unpack_all(far_in, last, lambda h, k: (k, h))
        enter[0, 0], enter[0, 1] = entering(0, (aux_far[0], aux_far[1]))

        @pl.when(sp > 0)
        def _():
            enter_copy.start()

        enter[1, 0], enter[1, 1] = entering(1, whole)

    @pl.when((tp == 0) & (sp > 0))
    def _():
        enter_copy.wait_recv()

    @pl.when((tp == 0) & (sp == 0))
    def _():
        enter[0, 0], enter[0, 1] = aux[2], aux[3]

    hs_copy = remote(hs.at[0], hs.at[1], hs_sem.at[0], hs_sem.at[1], partner)

    def add_own(blks):
        oacc[...] += jnp.dot(
            jnp.concatenate(blks, axis=1), ov[:chans], preferred_element_type=F32
        )

    @pl.when(tp == 1)
    def _():
        correct(1, tbl, map_t, post, 0)
        hs_copy.start()
        for copy in waited:
            copy.wait_recv()
        hc_copy.wait_recv()
        correct(0, table_far, map_far, post_far, 1)
        oacc[...] += jnp.dot(hs[0], ov[:chans], preferred_element_type=F32) + jnp.dot(
            hc[1], ov[2 * chans + cwide :], preferred_element_type=F32
        )

    @pl.when(tp == 0)
    def _():
        add_own(correct(0, tbl, map_t, post, 0))

    @pl.when(tp == 0)
    def _():
        hs_copy.wait_recv()

    out_ref[...] = (oacc[...] + jnp.dot(hs[1], ov[chans : 2 * chans], preferred_element_type=F32)).astype(BF16)

    x_copy.wait_send()
    hc_copy.wait_send()

    @pl.when(tp == 1)
    def _():
        hs_copy.wait_send()

    @pl.when((tp == 1) & (sp > 0))
    def _():
        enter_copy.wait_send()

    @pl.when(tp == 0)
    def _():
        aux_copy.wait_send()
        for copy in waited:
            copy.wait_send()

    @pl.when(sp < n - 1)
    def _():
        tail_copy.wait_send()

    wait_many(
        near_in.at[0],
        (near_sem.at[2], near_sem.at[0]),
        jnp.where(a < last, inner - tp, inner - 1 - b),
        inner,
        True,
    )

    @pl.when(tp == 1)
    def _():
        wait_many(far_in, (far_sem.at[0], far_sem.at[1]), last - a, last, True)


def on_device(
    activations,
    norm_gain,
    state_proj,
    value_proj,
    post_gate_proj,
    pre_gate_proj,
    input_map,
    output_map,
    skip_gain,
    rotation,
    log_decay,
    initial_state,
    conv_taps,
    state_out,
    conv_out,
):
    n = lax.axis_size("sp")
    rows, half = activations.shape
    groups, state = rotation.shape
    chans = state_proj.shape[1]
    cwide = value_proj.shape[1]
    outs = state_out.shape[1]
    states = groups * state
    prow = states // LANES
    inner = inner_of(n)
    bdw = 2 * states // (chans // LANES)
    vmem = pl.BlockSpec(memory_space=pltpu.VMEM)
    hbm = pl.BlockSpec(memory_space=pl.ANY)
    dma = pltpu.SemaphoreType.DMA
    return pl.pallas_call(
        functools.partial(kernel, n),
        out_shape=pltpu.VMEM((rows, outs), BF16),
        in_specs=[hbm] * 15,
        out_specs=vmem,
        scratch_shapes=[
            pltpu.VMEM((rows, half), BF16),
            pltpu.VMEM((1, 2 * half), F32),
            pltpu.VMEM(input_map.shape, BF16),
            pltpu.VMEM((groups, output_map.shape[2], output_map.shape[1]), F32),
            pltpu.VMEM((1, chans), F32),
            pltpu.VMEM((groups, state), F32),
            pltpu.VMEM((groups, rows), F32),
            pltpu.VMEM(initial_state.shape, F32),
            pltpu.VMEM(conv_taps.shape, BF16),
            pltpu.VMEM((4, 2 * half, chans), BF16),
            pltpu.VMEM((2 * chans + 2 * cwide, outs), BF16),
            pltpu.VMEM((rows, half), BF16),
            pltpu.VMEM((rows, 2 * half), BF16),
            pltpu.VMEM((rows, chans), BF16),
            pltpu.VMEM((chans, bdw), BF16),
            pltpu.VMEM((chans, bdw), BF16),
            pltpu.VMEM((2 * states, LANES), BF16),
            pltpu.VMEM((rows, 2 * states), BF16),
            pltpu.VMEM((2, 9 * prow, LANES), F32),
            pltpu.VMEM((rows, chans), F32),
            pltpu.VMEM((rows, chans), F32),
            pltpu.VMEM((2, prow, LANES), F32),
            pltpu.VMEM((2, rows, chans), F32),
            pltpu.VMEM((rows, 2 * states), BF16),
            pltpu.VMEM((2 * states, LANES), BF16),
            pltpu.VMEM((2, rows, chans), F32),
            pltpu.VMEM((4, prow, LANES), F32),
            pltpu.VMEM((4, prow, LANES), F32),
            pltpu.VMEM((2, max(inner, n // inner) * prow, LANES), F32),
            pltpu.VMEM((2, 5, prow, LANES), F32),
            pltpu.VMEM((2, 2, prow, LANES), F32),
            pltpu.VMEM((rows, 2 * rows), BF16),
            pltpu.VMEM((groups, chans), BF16),
            pltpu.VMEM((rows * prow, LANES), F32),
            pltpu.VMEM((rows * (2 * prow + 8), LANES), F32),
            pltpu.VMEM((4 * groups, LANES), F32),
            pltpu.VMEM((rows + 8, cwide), F32),
            pltpu.VMEM((2, inner, 3 * prow, LANES), BF16),
            pltpu.VMEM((n // inner, 2, 3 * prow, LANES), BF16),
            pltpu.VMEM((2, 3 * prow, LANES), BF16),
            pltpu.VMEM((2, rows, chans), BF16),
            pltpu.VMEM((2, rows, cwide), BF16),
            pltpu.VMEM((rows, outs), F32),
            dma((9,)),
            dma((4,)),
            dma((1,)),
            dma((2,)),
            dma((2,)),
            dma((2,)),
            dma((2,)),
            dma((3,)),
            dma((2,)),
            dma((2,)),
            dma((2,)),
            dma((2, 3)),
            pltpu.SemaphoreType.REGULAR,
            pltpu.SemaphoreType.REGULAR,
        ],
        compiler_params=pltpu.CompilerParams(collective_id=0, has_side_effects=True),
    )(
        activations,
        norm_gain.reshape(1, -1),
        state_proj,
        value_proj,
        post_gate_proj,
        pre_gate_proj,
        input_map,
        jnp.swapaxes(output_map, 1, 2),
        skip_gain.reshape(1, -1),
        rotation,
        jnp.swapaxes(log_decay, 0, 1),
        initial_state,
        conv_taps,
        state_out,
        conv_out,
    )


def solution(mesh):
    return jax.shard_map(
        on_device,
        mesh=mesh,
        in_specs=(
            P("sp", "tp"),
            P(),
            P(None, "tp"),
            P(None, "tp"),
            P(None, "tp"),
            P(None, "tp"),
            P("tp", None, None),
            P("tp", None, None),
            P("tp"),
            P("tp", None),
            P("sp", "tp"),
            P(None, "tp", None),
            P(None, "tp"),
            P(None, "tp"),
            P(None, "tp"),
        ),
        out_specs=P("sp", "tp"),
        check_vma=False,
    )
```

```python
import functools

import jax
import jax.numpy as jnp
from jax import lax
from jax.experimental import pallas as pl
from jax.experimental.pallas import tpu as pltpu
from jax.sharding import PartitionSpec as P

EPS = 1e-06
LANES = 128
MESH = pl.DeviceIdType.MESH
F32 = jnp.float32
BF16 = jnp.bfloat16


def minus_expm1(y):
    poly = jnp.ones_like(y)
    for k in range(11, 1, -1):
        poly = 1.0 + poly * y * (1.0 / k)
    return jnp.where(y > -0.5, -y * poly, 1.0 - jnp.exp(y))


def split3(v):
    hi = v.astype(BF16)
    rest = v - hi.astype(F32)
    mid = rest.astype(BF16)
    low = (rest - mid.astype(F32)).astype(BF16)
    return hi, mid, low


def cmul(a, b):
    return a[0] * b[0] - a[1] * b[1], a[0] * b[1] + a[1] * b[0]


def cpow(base, count):
    result = None
    while count:
        if count & 1:
            result = base if result is None else cmul(result, base)
        count >>= 1
        if count:
            base = cmul(base, base)
    return result


def inner_of(n):
    return max(d for d in range(1, n + 1) if n % d == 0 and d * d <= n)


def gelu(x):
    return 0.5 * x * (1.0 + jnp.tanh(0.7978845608028654 * (x + 0.044715 * x * x * x)))


def kernel(
    n,
    x_hbm,
    gain_hbm,
    w0_hbm,
    w1_hbm,
    w2_hbm,
    w3_hbm,
    imap_hbm,
    omap_hbm,
    skip_hbm,
    rot_hbm,
    ld_hbm,
    init_hbm,
    taps_hbm,
    so_hbm,
    co_hbm,
    out_ref,
    x_ref,
    gain_ref,
    imap_ref,
    omap_ref,
    skip_ref,
    rot_ref,
    ld_ref,
    init_ref,
    taps_ref,
    wv,
    ov,
    xr,
    acc,
    din,
    bd_in,
    bd_out,
    map_t,
    tbl,
    powers,
    chan_end,
    chan_gain,
    rowed,
    post,
    table_far,
    map_far,
    post_far,
    aux,
    aux_far,
    mags_in,
    held,
    enter,
    sums,
    to_chan,
    mag,
    drv,
    pairs,
    pad,
    near_in,
    far_in,
    far_out,
    hs,
    hc,
    oacc,
    in_sem,
    wsem,
    osem,
    x_sem,
    tail_sem,
    hc_sem,
    hs_sem,
    near_sem,
    far_sem,
    aux_sem,
    enter_sem,
    dup_sem,
    near_ready,
    far_ready,
):
    sp, tp = lax.axis_index("sp"), lax.axis_index("tp")
    other = 1 - tp
    rows, half = x_ref.shape
    groups, state = rot_ref.shape
    gch = imap_ref.shape[1]
    chans = groups * gch
    states = groups * state
    prow = states // LANES
    per_block = LANES // gch
    blocks = groups // per_block
    quads = prow // blocks
    pitch = drv.shape[0] // rows
    bstates = quads * LANES
    cwide = taps_ref.shape[1]
    width = taps_ref.shape[0]

    barrier = pltpu.get_barrier_semaphore()
    partner = {"sp": sp, "tp": other}

    inner = inner_of(n)
    outer = n // inner
    a, b = lax.div(sp, inner), lax.rem(sp, inner)
    last = outer - 1

    hop_on = (b == inner - 1) & (a < last)

    def tell(sem, j):
        for t in (0, 1):
            pl.semaphore_signal(sem, inc=1, device_id={"sp": j, "tp": t}, device_id_type=MESH)

    def greet_far(k, c):
        tell(barrier, k * inner + b)
        return c

    pl.semaphore_signal(barrier, inc=1, device_id=partner, device_id_type=MESH)

    @pl.when(b < inner - 1)
    def _():
        tell(barrier, sp + inner - 1 - b)

    lax.fori_loop(a + 1, outer, greet_far, 0)

    in_copies = {}
    def fetch(i, src, dst):
        in_copies[i] = pltpu.make_async_copy(src, dst, in_sem.at[i])
        in_copies[i].start()

    w_hbm = (w0_hbm, w1_hbm, w2_hbm, w3_hbm)

    def fetch_weight(i, h, sem):
        part = (tp, other)[h]
        pltpu.make_async_copy(
            w_hbm[i].at[pl.ds(part * half, half), :], wv.at[i, pl.ds(h * half, half), :], sem
        ).start()

    def wait_weight(i):
        pltpu.make_async_copy(w_hbm[i], wv.at[i], wsem.at[i]).wait()

    fetch(0, x_hbm, x_ref)
    fetch(4, ld_hbm, ld_ref)
    fetch(2, rot_hbm, rot_ref)
    fetch(5, imap_hbm, imap_ref)
    fetch(1, gain_hbm, gain_ref)
    fetch_weight(0, 0, wsem.at[0])
    fetch_weight(0, 1, wsem.at[0])

    pl.semaphore_wait(barrier, 1 + 2 * (a + jnp.where(b == inner - 1, b, 0)))

    def ready_near(k, c):
        tell(near_ready, a * inner + k)
        return c

    def ready_far(k, c):
        tell(far_ready, k * inner + b)
        return c

    @pl.when((tp == 1) & (b == inner - 1))
    def _():
        lax.fori_loop(0, b, ready_near, 0)


    lax.fori_loop(0, a, ready_far, 0)

    bd_in[...] = jnp.zeros_like(bd_in)
    bd_out[...] = jnp.zeros_like(bd_out)
    when = lax.broadcasted_iota(jnp.int32, (rows, 2 * rows), 0)
    upto = lax.broadcasted_iota(jnp.int32, (rows, 2 * rows), 1)
    sums[...] = jnp.where(
        ((upto < rows) & (when <= upto)) | ((upto >= rows) & (when > upto - rows)), 1.0, 0.0
    ).astype(BF16)
    col = lax.broadcasted_iota(jnp.int32, (groups, chans), 1)
    row = lax.broadcasted_iota(jnp.int32, (groups, chans), 0)
    to_chan[...] = jnp.where((col >= row * gch) & (col < (row + 1) * gch), 1.0, 0.0).astype(BF16)

    def remote(src, dst, s, r, dev):
        return pltpu.make_async_remote_copy(
            src_ref=src, dst_ref=dst, send_sem=s, recv_sem=r, device_id=dev, device_id_type=MESH
        )

    in_copies[0].wait()
    x_copy = remote(x_ref, xr, x_sem.at[0], x_sem.at[1], partner)
    x_copy.start()

    fetch(3, init_hbm, init_ref)
    fetch(6, omap_hbm, omap_ref)
    fetch(7, skip_hbm, skip_ref)
    fetch(8, taps_hbm, taps_ref)
    for i in (1, 3, 2):
        for h in (0, 1):
            fetch_weight(i, h, wsem.at[i])
    for i, w, deep in ((1, co_hbm, cwide), (0, so_hbm, chans)):
        for h, part in ((0, tp), (1, other)):
            pltpu.make_async_copy(
                w.at[pl.ds(part * deep, deep), :], ov.at[pl.ds(2 * i * chans + h * deep, deep), :], osem.at[0]
            ).start()

    lane = lax.broadcasted_iota(jnp.int32, (1, LANES), 1)

    def pair_up(i, v):
        pairs[pl.ds(i * groups, groups), :] = v
        even = pairs[pl.ds(i * groups, prow, stride=2), :]
        odd = pairs[pl.ds(i * groups + 1, prow, stride=2), :]
        return jnp.where(lane < state, even, odd)

    def twice(v):
        return jnp.concatenate([v, v], axis=1)

    for i in (4, 2, 5, 1):
        in_copies[i].wait()
    ld = ld_ref[...]

    def time_sums(cols):
        added = jnp.dot(jnp.concatenate(split3(ld), axis=0), sums[:, cols], preferred_element_type=F32)
        return added[:groups] + added[groups : 2 * groups] + added[2 * groups :]

    def per_channel(v):
        hi, mid, _ = split3(v.T)
        return jnp.dot(hi, to_chan[...], preferred_element_type=F32) + jnp.dot(
            mid, to_chan[...], preferred_element_type=F32
        )

    gain = jnp.sqrt(minus_expm1(2.0 * ld))
    chan_end[...] = per_channel(gain * jnp.exp(time_sums(slice(rows, 2 * rows))))
    tot = pair_up(
        3, jnp.broadcast_to(jnp.exp(jnp.sum(ld, axis=1, keepdims=True)), (groups, LANES))
    )
    theta = pair_up(0, twice(rot_ref[...]))
    turn = jnp.cos(theta), jnp.sin(theta)
    step = turn
    for k in range(8):
        for i in (0, 1):
            powers[i, pl.ds(k * prow, prow), :] = step[i]
        step = cmul(step, turn) if k < 7 else step
    sixteen = cmul(step, step)
    leap = sixteen
    for k in range(rows // 16 - 1):
        for i in (0, 1):
            powers[i, pl.ds((8 + k) * prow, prow), :] = leap[i]
        leap = cmul(leap, sixteen)
    whole = cpow(step, rows // 8)
    for r in range(prow):
        even = [powers[i, pl.ds(r, 8, stride=prow), :] for i in (0, 1)]
        eight = [powers[i, pl.ds(7 * prow + r, 1), :] for i in (0, 1)]
        odd = cmul(even, eight)
        base = [jnp.concatenate([even[i], odd[i]], axis=0).astype(BF16) for i in (0, 1)]
        for t in range(0, rows, 16):
            now = base
            if t > 0:
                at = pl.ds((8 + t // 16 - 1) * prow + r, 1)
                now = cmul(
                    base,
                    [jnp.broadcast_to(powers[i, at, :], (16, LANES)).astype(BF16) for i in (0, 1)],
                )
            for i in (0, 1):
                tbl[t : t + 16, (2 * r + i) * LANES : (2 * r + i + 1) * LANES] = now[i]

    def spread_map(src, dst):
        for b in range(blocks):
            for q in range(quads):
                g = b * per_block + 2 * q
                one = src[g].astype(F32)
                two = src[g + 1].astype(F32)
                one_r = jnp.concatenate([one[:, state:], one[:, :state]], axis=1)
                two_r = jnp.concatenate([two[:, state:], two[:, :state]], axis=1)
                low = lane < state
                re = jnp.concatenate([jnp.where(low, one, 0.0), jnp.where(low, 0.0, two_r)], axis=0)
                im = jnp.concatenate([jnp.where(low, one_r, 0.0), jnp.where(low, 0.0, two)], axis=0)
                at = pl.ds(b * LANES + q * 2 * gch, 2 * gch)
                dst[at, 2 * q * LANES : (2 * q + 1) * LANES] = re.astype(BF16)
                dst[at, (2 * q + 1) * LANES : (2 * q + 2) * LANES] = im.astype(BF16)

    spread_map(imap_ref, bd_in)
    own = x_ref[...].astype(F32)
    scaled = (own * gain_ref[:, pl.ds(pl.multiple_of(tp * half, LANES), half)]).astype(BF16)
    squares = jnp.sum(own * own, axis=1, keepdims=True)
    wait_weight(0)
    partial = jnp.dot(scaled, wv[0, :half], preferred_element_type=F32)
    acc[:, :half] = scaled

    x_copy.wait_recv()
    far_x = xr[...].astype(F32)
    scaled_far = (far_x * gain_ref[:, pl.ds(pl.multiple_of(other * half, LANES), half)]).astype(BF16)
    squares = squares + jnp.sum(far_x * far_x, axis=1, keepdims=True)
    scale = lax.rsqrt(squares / (2 * half) + EPS)

    acc[:, half:] = scaled_far
    total = partial + jnp.dot(scaled_far, wv[0, half:], preferred_element_type=F32)
    drive_in = (total * scale).astype(BF16)
    din[...] = drive_in
    ends_in = (drive_in.astype(F32) * chan_end[...]).astype(BF16).T
    for r in range(prow):
        q = r % quads
        at = slice(r * 2 * gch, (r + 1) * 2 * gch)
        seen = jnp.dot(
            ends_in[at], tbl[:, 2 * r * LANES : (2 * r + 2) * LANES], preferred_element_type=F32
        )
        m_re = bd_in[at, 2 * q * LANES : (2 * q + 1) * LANES].astype(F32)
        m_im = bd_in[at, (2 * q + 1) * LANES : (2 * q + 2) * LANES].astype(F32)
        c, d = seen[:, :LANES], seen[:, LANES:]
        rowed[0, r : r + 1, :] = jnp.sum(c * m_re + d * m_im, axis=0, keepdims=True)
        rowed[1, r : r + 1, :] = jnp.sum(c * m_im - d * m_re, axis=0, keepdims=True)
    e_re, e_im = cmul(whole, (rowed[0], rowed[1]))

    near_in[tp, b, pl.ds(0, prow), :] = e_re.astype(BF16)
    near_in[tp, b, pl.ds(prow, prow), :] = e_im.astype(BF16)
    fore = lax.rem(lax.broadcasted_iota(jnp.int32, (prow, LANES), 1), state) < state // 2

    def packed(v):
        hi, mid, _ = split3(v)
        return jnp.where(fore, hi.astype(F32), mid.astype(F32)).astype(BF16)

    near_in[tp, b, pl.ds(2 * prow, prow), :] = packed(tot)

    def wait_many(ref, sems, count, upto, sent):
        for j in range(1, upto + 1):
            @pl.when(count == j)
            def _():
                part = ref.at[pl.ds(0, j)]
                copy = remote(part, part, sems[0], sems[1], partner)
                copy.wait_send() if sent else copy.wait_recv()

    def near_copy(k):
        return remote(
            near_in.at[tp, b],
            near_in.at[tp, b],
            near_sem.at[2],
            near_sem.at[tp],
            {"sp": a * inner + k, "tp": 1},
        )

    def far_copy(k):
        return remote(
            far_out, far_in.at[a], far_sem.at[0], far_sem.at[1], {"sp": k * inner + b, "tp": 1}
        )

    near_from = jnp.where(a < last, 0, b + 1)
    near_upto = jnp.where(a < last, inner, b)
    @pl.when(b < inner - 1)
    def _():
        pl.semaphore_wait(near_ready, 1)

    def send_near(k, c):
        @pl.when((k != b) | ((tp == 0) & (a < last)))
        def _():
            near_copy(k).start()

        return c

    lax.fori_loop(near_from, inner, send_near, 0)

    in_copies[3].wait()
    aux[0], aux[1] = whole
    aux[2] = pair_up(1, twice(init_ref[0]))
    aux[3] = pair_up(2, twice(init_ref[1]))
    aux_copy = remote(aux, aux_far, aux_sem.at[0], aux_sem.at[1], partner)
    dup_copies = [
        remote(src, dst, dup_sem.at[0, (0, 1, 2, 2, 1)[i]], dup_sem.at[1, (0, 1, 2, 2, 1)[i]], partner)
        for i, (src, dst) in enumerate(
            (
                (tbl, table_far),
                (map_t.at[pl.ds(0, states), :], map_far.at[pl.ds(0, states), :]),
                (post.at[1], post_far.at[1]),
                (post.at[0], post_far.at[0]),
                (map_t.at[pl.ds(states, states), :], map_far.at[pl.ds(states, states), :]),
            )
        )
    ]

    def give(copy):
        @pl.when(tp == 0)
        def _():
            copy.start()

    waited = [
        remote(src, dst, dup_sem.at[0, i], dup_sem.at[1, i], partner)
        for i, (src, dst) in enumerate(((tbl, table_far), (map_t, map_far), (post, post_far)))
    ]

    give(aux_copy)

    def project(i):
        wait_weight(i)
        total = jnp.dot(acc[...], wv[i], preferred_element_type=F32)
        return (total * scale).astype(BF16)

    value = project(1)
    pre_gate = project(3)
    mixed = (pre_gate.astype(F32) * value.astype(F32)).astype(BF16).astype(F32)
    pad[pl.ds(8, rows), :] = mixed
    tail_copy = remote(
        pad.at[pl.ds(rows, 8), :],
        pad.at[pl.ds(0, 8), :],
        tail_sem.at[0],
        tail_sem.at[1],
        {"sp": lax.rem(sp + 1, n), "tp": tp},
    )

    @pl.when(hop_on)
    def _():
        pl.semaphore_wait(far_ready, 2 * (last - a))

    @pl.when(sp < n - 1)
    def _():
        tail_copy.start()

    give(dup_copies[0])

    for i in (6, 7):
        in_copies[i].wait()
    spread_map(omap_ref, bd_out)
    for k in range(blocks):
        map_t[2 * k * bstates : 2 * (k + 1) * bstates, :] = bd_out[k * LANES : (k + 1) * LANES, :].T
    give(dup_copies[1])

    ld = ld_ref[...]
    gain = jnp.sqrt(minus_expm1(2.0 * ld))
    late = per_channel(jnp.concatenate([jnp.exp(time_sums(slice(0, rows))), gain], axis=1))
    post[1] = late[:rows]
    give(dup_copies[2])
    chan_gain[...] = late[rows:]
    mags = split3(jnp.exp(ld).T)[:2]
    for k in range(blocks):
        col = lax.broadcasted_iota(jnp.int32, (groups, bstates), 1) + k * bstates
        row = lax.broadcasted_iota(jnp.int32, (groups, bstates), 0)
        spread = jnp.where(
            (col >= row * state) & (col < (row + 1) * state), 1.0, 0.0
        ).astype(BF16)
        m = jnp.dot(mags[0], spread, preferred_element_type=F32) + jnp.dot(
            mags[1], spread, preferred_element_type=F32
        )
        for q in range(quads):
            mag[pl.ds(k * quads + q, rows, stride=prow), :] = m[:, q * LANES : (q + 1) * LANES]

    zero = jnp.zeros((prow, LANES), F32)

    def unpacked(v):
        v = v.astype(F32)
        keep = lax.rem(lax.broadcasted_iota(jnp.int32, v.shape, 1), state) < state // 2
        return v + jnp.where(keep, pltpu.roll(v, LANES - state // 2, 1), pltpu.roll(v, state // 2, 1))

    def unpack_all(ref, count, index):
        packs = [
            ref[index(h, k) + (pl.ds(2 * prow, prow),)] for h in (0, 1) for k in range(count)
        ]
        v = unpacked(jnp.concatenate(packs, axis=0))
        for h in (0, 1):
            mags_in[h, : count * prow, :] = v[h * count * prow : (h + 1) * count * prow]

    def message(ref, h, k):
        return (
            ref[pl.ds(0, prow), :].astype(F32),
            ref[pl.ds(prow, prow), :].astype(F32),
            mags_in[h, pl.ds(pl.multiple_of(k * prow, prow), prow), :],
        )

    def send_far(k, c):
        far_copy(outer + a - k).start()
        return c

    def join_halves(turned, first):
        unpack_all(near_in, inner, lambda h, k: (h, k))

        def half_step(h, k, c):
            ends, mag_all, phase, mine = c[0:2], c[2], c[3:5], c[5:]
            k_re, k_im, k_mag = message(near_in.at[h, k], h, k)
            moved = cmul((turned[h][0] * k_mag, turned[h][1] * k_mag), ends)
            now = (moved[0] + k_re, moved[1] + k_im, mag_all * k_mag) + cmul(turned[h], phase)
            return now + tuple(jnp.where(k < b, v, w) for v, w in zip(now, mine))

        def near_step(k, c):
            return tuple(half_step(h, k, c[h]) for h in (0, 1))

        one = jnp.ones((prow, LANES), F32)
        begin = [tuple(jnp.where(a == 0, v, zero) for v in f) + (one, one, zero) for f in first]
        planes = lax.fori_loop(0, near_upto, near_step, tuple(v + v for v in begin))
        for h, plane in enumerate(planes):
            far_out[h, pl.ds(0, prow), :] = plane[0].astype(BF16)
            far_out[h, pl.ds(prow, prow), :] = plane[1].astype(BF16)
            far_out[h, pl.ds(2 * prow, prow), :] = packed(plane[2])
            for i in range(5):
                held[h, i] = plane[5 + i]

    def join_near():
        @pl.when(tp == 1)
        def _():
            for h in (1, 0):
                wait_many(
                    near_in.at[h],
                    (near_sem.at[2], near_sem.at[h]),
                    jnp.where(a < last, inner - h, b),
                    inner,
                    False,
                )
            join_halves(
                ((aux_far[0], aux_far[1]), whole), ((aux_far[2], aux_far[3]), (aux[2], aux[3]))
            )

        @pl.when((a < last) & (b < inner - 1))
        def _():
            pl.semaphore_wait(far_ready, 2 * (last - a))

        @pl.when((tp == 1) & (a < last))
        def _():
            lax.fori_loop(a + 1, outer, send_far, 0)

    @pl.when(tp == 1)
    def _():
        aux_copy.wait_recv()

    @pl.when(b > 1)
    def _():
        join_near()

    hc[0] = project(2)
    gained = (din[...].astype(F32) * chan_gain[...]).astype(BF16)
    for k in range(blocks):
        blk = jnp.dot(
            gained[:, k * LANES : (k + 1) * LANES],
            bd_in[k * LANES : (k + 1) * LANES, :],
            preferred_element_type=F32,
        )
        for q in range(quads):
            r = k * quads + q
            drv[pl.ds(r, rows, stride=pitch), :] = blk[:, 2 * q * LANES : (2 * q + 1) * LANES]
            drv[pl.ds(prow + r, rows, stride=pitch), :] = blk[
                :, (2 * q + 1) * LANES : (2 * q + 2) * LANES
            ]

    @pl.when(b == 1)
    def _():
        join_near()

    hc_copy = remote(hc.at[0], hc.at[1], hc_sem.at[0], hc_sem.at[1], partner)

    def convolve():
        @pl.when(sp == 0)
        def _():
            pad[pl.ds(0, 8), :] = jnp.zeros((8, cwide), F32)

        in_copies[8].wait()

        @pl.when(sp > 0)
        def _():
            tail_copy.wait_recv()

        conv = jnp.zeros((rows, cwide), F32)
        for k in range(width):
            conv = conv + pad[pl.ds(8 + k - (width - 1), rows), :] * taps_ref[k : k + 1, :].astype(F32)
        hc[0] = (hc[0].astype(F32) * conv).astype(BF16)
        hc_copy.start()

    even = (lax.rem(b, 2) == 0) & (sp > 0)

    @pl.when(jnp.logical_not(even))
    def _():
        convolve()

    give(dup_copies[4])

    def scan(t, h):
        m = mag[pl.ds(pl.multiple_of(t * prow, prow), prow), :]
        base = pl.multiple_of(t * pitch, 8)
        d_re = drv[pl.ds(base, prow), :]
        d_im = drv[pl.ds(base + prow, prow), :]
        f_re, f_im = m * turn[0], m * turn[1]
        new_re = (f_re * h[0] + d_re) - f_im * h[1]
        new_im = (f_re * h[1] + d_im) + f_im * h[0]
        drv[pl.ds(base, prow), :] = new_re
        drv[pl.ds(base + prow, prow), :] = new_im
        return new_re, new_im

    lax.fori_loop(0, rows, scan, (zero, zero), unroll=8)

    @pl.when(b == 0)
    def _():
        join_near()

    for k in range(blocks):
        cols = slice(k * LANES, (k + 1) * LANES)
        at = [half_row + k * quads + q for q in range(quads) for half_row in (0, prow)]
        st = jnp.concatenate(
            [drv[pl.ds(r, rows, stride=pitch), :].astype(BF16) for r in at], axis=1
        )
        read = jnp.dot(
            st, map_t[2 * k * bstates : 2 * (k + 1) * bstates, :], preferred_element_type=F32
        )
        post[0, :, cols] = read + skip_ref[:, cols] * din[:, cols].astype(F32)

    give(dup_copies[3])

    @pl.when(even)
    def _():
        convolve()

    pltpu.make_async_copy(ov, ov, osem.at[0]).wait()
    oacc[...] = jnp.dot(hc[0], ov[2 * chans : 2 * chans + cwide], preferred_element_type=F32)

    def add_far_conv():
        hc_copy.wait_recv()
        oacc[...] += jnp.dot(hc[1], ov[2 * chans + cwide :], preferred_element_type=F32)

    @pl.when(tp == 0)
    def _():
        add_far_conv()

    def entering(h, turned):
        plane_turn = cpow(turned, inner)

        def far_step(k, c):
            k_re, k_im, k_mag = message(far_in.at[k, h], h, k)
            moved = cmul((plane_turn[0] * k_mag, plane_turn[1] * k_mag), c)
            return moved[0] + k_re, moved[1] + k_im

        before = lax.fori_loop(0, a, far_step, (zero, zero))
        moved = cmul((held[h, 3] * held[h, 2], held[h, 4] * held[h, 2]), before)
        return held[h, 0] + moved[0], held[h, 1] + moved[1]

    def correct(h, table, mapped, local, slot):
        moved = []
        for k in range(blocks):
            turned = []
            for r in range(k * quads, (k + 1) * quads):
                c, d = (
                    table[:, (2 * r + i) * LANES : (2 * r + i + 1) * LANES].reshape(rows // 16, 16, LANES)
                    for i in (0, 1)
                )
                h_re, h_im = (
                    jnp.broadcast_to(enter[h, i, r : r + 1, :], (16, LANES)).astype(BF16)[None]
                    for i in (0, 1)
                )
                turned += cmul((c, d), (h_re, h_im))
            moved.append(
                jnp.dot(
                    jnp.concatenate([v.reshape(rows, LANES) for v in turned], axis=1),
                    mapped[2 * k * bstates : 2 * (k + 1) * bstates, :],
                    preferred_element_type=F32,
                )
            )
        made = []
        for k in range(blocks):
            cols = slice(k * LANES, (k + 1) * LANES)
            made.append(gelu(local[0, :, cols] + local[1, :, cols] * moved[k]).astype(BF16))
            hs[slot, :, cols] = made[k]
        return made

    enter_copy = remote(enter.at[0], enter.at[0], enter_sem.at[0], enter_sem.at[1], partner)

    @pl.when(tp == 1)
    def _():
        wait_many(far_in, (far_sem.at[0], far_sem.at[1]), a, last, False)
        unpack_all(far_in, last, lambda h, k: (k, h))
        enter[0, 0], enter[0, 1] = entering(0, (aux_far[0], aux_far[1]))

        @pl.when(sp > 0)
        def _():
            enter_copy.start()

        enter[1, 0], enter[1, 1] = entering(1, whole)

    @pl.when((tp == 0) & (sp > 0))
    def _():
        enter_copy.wait_recv()

    @pl.when((tp == 0) & (sp == 0))
    def _():
        enter[0, 0], enter[0, 1] = aux[2], aux[3]

    hs_copy = remote(hs.at[0], hs.at[1], hs_sem.at[0], hs_sem.at[1], partner)

    def add_own(blks):
        oacc[...] += jnp.dot(
            jnp.concatenate(blks, axis=1), ov[:chans], preferred_element_type=F32
        )

    @pl.when(tp == 1)
    def _():
        correct(1, tbl, map_t, post, 0)
        hs_copy.start()
        for copy in waited:
            copy.wait_recv()
        hc_copy.wait_recv()
        correct(0, table_far, map_far, post_far, 1)
        oacc[...] += jnp.dot(hs[0], ov[:chans], preferred_element_type=F32) + jnp.dot(
            hc[1], ov[2 * chans + cwide :], preferred_element_type=F32
        )

    @pl.when(tp == 0)
    def _():
        add_own(correct(0, tbl, map_t, post, 0))

    @pl.when(tp == 0)
    def _():
        hs_copy.wait_recv()

    out_ref[...] = (oacc[...] + jnp.dot(hs[1], ov[chans : 2 * chans], preferred_element_type=F32)).astype(BF16)

    x_copy.wait_send()
    hc_copy.wait_send()

    @pl.when(tp == 1)
    def _():
        hs_copy.wait_send()

    @pl.when((tp == 1) & (sp > 0))
    def _():
        enter_copy.wait_send()

    @pl.when(tp == 0)
    def _():
        aux_copy.wait_send()
        for copy in waited:
            copy.wait_send()

    @pl.when(sp < n - 1)
    def _():
        tail_copy.wait_send()

    wait_many(
        near_in.at[0],
        (near_sem.at[2], near_sem.at[0]),
        jnp.where(a < last, inner - tp, inner - 1 - b),
        inner,
        True,
    )

    @pl.when(tp == 1)
    def _():
        wait_many(far_in, (far_sem.at[0], far_sem.at[1]), last - a, last, True)


def on_device(
    activations,
    norm_gain,
    state_proj,
    value_proj,
    post_gate_proj,
    pre_gate_proj,
    input_map,
    output_map,
    skip_gain,
    rotation,
    log_decay,
    initial_state,
    conv_taps,
    state_out,
    conv_out,
):
    n = lax.axis_size("sp")
    rows, half = activations.shape
    groups, state = rotation.shape
    chans = state_proj.shape[1]
    cwide = value_proj.shape[1]
    outs = state_out.shape[1]
    states = groups * state
    prow = states // LANES
    inner = inner_of(n)
    bdw = 2 * states // (chans // LANES)
    vmem = pl.BlockSpec(memory_space=pltpu.VMEM)
    hbm = pl.BlockSpec(memory_space=pl.ANY)
    dma = pltpu.SemaphoreType.DMA
    return pl.pallas_call(
        functools.partial(kernel, n),
        out_shape=pltpu.VMEM((rows, outs), BF16),
        in_specs=[hbm] * 15,
        out_specs=vmem,
        scratch_shapes=[
            pltpu.VMEM((rows, half), BF16),
            pltpu.VMEM((1, 2 * half), F32),
            pltpu.VMEM(input_map.shape, BF16),
            pltpu.VMEM((groups, output_map.shape[2], output_map.shape[1]), F32),
            pltpu.VMEM((1, chans), F32),
            pltpu.VMEM((groups, state), F32),
            pltpu.VMEM((groups, rows), F32),
            pltpu.VMEM(initial_state.shape, F32),
            pltpu.VMEM(conv_taps.shape, BF16),
            pltpu.VMEM((4, 2 * half, chans), BF16),
            pltpu.VMEM((2 * chans + 2 * cwide, outs), BF16),
            pltpu.VMEM((rows, half), BF16),
            pltpu.VMEM((rows, 2 * half), BF16),
            pltpu.VMEM((rows, chans), BF16),
            pltpu.VMEM((chans, bdw), BF16),
            pltpu.VMEM((chans, bdw), BF16),
            pltpu.VMEM((2 * states, LANES), BF16),
            pltpu.VMEM((rows, 2 * states), BF16),
            pltpu.VMEM((2, (8 + rows // 16) * prow, LANES), F32),
            pltpu.VMEM((rows, chans), F32),
            pltpu.VMEM((rows, chans), F32),
            pltpu.VMEM((2, prow, LANES), F32),
            pltpu.VMEM((2, rows, chans), F32),
            pltpu.VMEM((rows, 2 * states), BF16),
            pltpu.VMEM((2 * states, LANES), BF16),
            pltpu.VMEM((2, rows, chans), F32),
            pltpu.VMEM((4, prow, LANES), F32),
            pltpu.VMEM((4, prow, LANES), F32),
            pltpu.VMEM((2, max(inner, n // inner) * prow, LANES), F32),
            pltpu.VMEM((2, 5, prow, LANES), F32),
            pltpu.VMEM((2, 2, prow, LANES), F32),
            pltpu.VMEM((rows, 2 * rows), BF16),
            pltpu.VMEM((groups, chans), BF16),
            pltpu.VMEM((rows * prow, LANES), F32),
            pltpu.VMEM((rows * (2 * prow + 8), LANES), F32),
            pltpu.VMEM((4 * groups, LANES), F32),
            pltpu.VMEM((rows + 8, cwide), F32),
            pltpu.VMEM((2, inner, 3 * prow, LANES), BF16),
            pltpu.VMEM((n // inner, 2, 3 * prow, LANES), BF16),
            pltpu.VMEM((2, 3 * prow, LANES), BF16),
            pltpu.VMEM((2, rows, chans), BF16),
            pltpu.VMEM((2, rows, cwide), BF16),
            pltpu.VMEM((rows, outs), F32),
            dma((9,)),
            dma((4,)),
            dma((1,)),
            dma((2,)),
            dma((2,)),
            dma((2,)),
            dma((2,)),
            dma((3,)),
            dma((2,)),
            dma((2,)),
            dma((2,)),
            dma((2, 3)),
            pltpu.SemaphoreType.REGULAR,
            pltpu.SemaphoreType.REGULAR,
        ],
        compiler_params=pltpu.CompilerParams(collective_id=0, has_side_effects=True),
    )(
        activations,
        norm_gain.reshape(1, -1),
        state_proj,
        value_proj,
        post_gate_proj,
        pre_gate_proj,
        input_map,
        jnp.swapaxes(output_map, 1, 2),
        skip_gain.reshape(1, -1),
        rotation,
        jnp.swapaxes(log_decay, 0, 1),
        initial_state,
        conv_taps,
        state_out,
        conv_out,
    )


def solution(mesh):
    return jax.shard_map(
        on_device,
        mesh=mesh,
        in_specs=(
            P("sp", "tp"),
            P(),
            P(None, "tp"),
            P(None, "tp"),
            P(None, "tp"),
            P(None, "tp"),
            P("tp", None, None),
            P("tp", None, None),
            P("tp"),
            P("tp", None),
            P("sp", "tp"),
            P(None, "tp", None),
            P(None, "tp"),
            P(None, "tp"),
            P(None, "tp"),
        ),
        out_specs=P("sp", "tp"),
        check_vma=False,
    )
```

```python
import functools

import jax
import jax.numpy as jnp
from jax import lax
from jax.experimental import pallas as pl
from jax.experimental.pallas import tpu as pltpu
from jax.sharding import PartitionSpec as P

EPS = 1e-06
LANES = 128
MESH = pl.DeviceIdType.MESH
F32 = jnp.float32
BF16 = jnp.bfloat16


def minus_expm1(y):
    poly = jnp.ones_like(y)
    for k in range(11, 1, -1):
        poly = 1.0 + poly * y * (1.0 / k)
    return jnp.where(y > -0.5, -y * poly, 1.0 - jnp.exp(y))


def split3(v):
    hi = v.astype(BF16)
    rest = v - hi.astype(F32)
    mid = rest.astype(BF16)
    low = (rest - mid.astype(F32)).astype(BF16)
    return hi, mid, low


def cmul(a, b):
    return a[0] * b[0] - a[1] * b[1], a[0] * b[1] + a[1] * b[0]


def cpow(base, count):
    result = None
    while count:
        if count & 1:
            result = base if result is None else cmul(result, base)
        count >>= 1
        if count:
            base = cmul(base, base)
    return result


def inner_of(n):
    return max(d for d in range(1, n + 1) if n % d == 0 and d * d <= n)


def gelu(x):
    return 0.5 * x * (1.0 + jnp.tanh(0.7978845608028654 * (x + 0.044715 * x * x * x)))


def kernel(
    n,
    x_hbm,
    gain_hbm,
    w0_hbm,
    w1_hbm,
    w2_hbm,
    w3_hbm,
    imap_hbm,
    omap_hbm,
    skip_hbm,
    rot_hbm,
    ld_hbm,
    init_hbm,
    taps_hbm,
    so_hbm,
    co_hbm,
    out_ref,
    x_ref,
    gain_ref,
    imap_ref,
    omap_ref,
    skip_ref,
    rot_ref,
    ld_ref,
    init_ref,
    taps_ref,
    wv,
    ov,
    xr,
    acc,
    din,
    bd_in,
    bd_out,
    map_t,
    tbl,
    powers,
    chan_end,
    chan_gain,
    rowed,
    post,
    table_far,
    map_far,
    post_far,
    aux,
    aux_far,
    mags_in,
    held,
    enter,
    sums,
    to_chan,
    mag,
    drv,
    pairs,
    pad,
    near_in,
    far_in,
    far_out,
    hs,
    hc,
    oacc,
    in_sem,
    wsem,
    osem,
    x_sem,
    tail_sem,
    hc_sem,
    hs_sem,
    near_sem,
    far_sem,
    aux_sem,
    enter_sem,
    dup_sem,
    near_ready,
    far_ready,
):
    sp, tp = lax.axis_index("sp"), lax.axis_index("tp")
    other = 1 - tp
    rows, half = x_ref.shape
    groups, state = rot_ref.shape
    gch = imap_ref.shape[1]
    chans = groups * gch
    states = groups * state
    prow = states // LANES
    per_block = LANES // gch
    blocks = groups // per_block
    quads = prow // blocks
    pitch = drv.shape[0] // rows
    bstates = quads * LANES
    cwide = taps_ref.shape[1]
    width = taps_ref.shape[0]

    barrier = pltpu.get_barrier_semaphore()
    partner = {"sp": sp, "tp": other}

    inner = inner_of(n)
    outer = n // inner
    a, b = lax.div(sp, inner), lax.rem(sp, inner)
    last = outer - 1

    hop_on = (b == inner - 1) & (a < last)

    def tell(sem, j):
        for t in (0, 1):
            pl.semaphore_signal(sem, inc=1, device_id={"sp": j, "tp": t}, device_id_type=MESH)

    def greet_far(k, c):
        tell(barrier, k * inner + b)
        return c

    pl.semaphore_signal(barrier, inc=1, device_id=partner, device_id_type=MESH)

    @pl.when(b < inner - 1)
    def _():
        tell(barrier, sp + inner - 1 - b)

    lax.fori_loop(a + 1, outer, greet_far, 0)

    in_copies = {}
    def fetch(i, src, dst):
        in_copies[i] = pltpu.make_async_copy(src, dst, in_sem.at[i])
        in_copies[i].start()

    w_hbm = (w0_hbm, w1_hbm, w2_hbm, w3_hbm)

    def fetch_weight(i, h, sem):
        part = (tp, other)[h]
        pltpu.make_async_copy(
            w_hbm[i].at[pl.ds(part * half, half), :], wv.at[i, pl.ds(h * half, half), :], sem
        ).start()

    def wait_weight(i):
        pltpu.make_async_copy(w_hbm[i], wv.at[i], wsem.at[i]).wait()

    fetch(0, x_hbm, x_ref)
    fetch(4, ld_hbm, ld_ref)
    fetch(2, rot_hbm, rot_ref)
    fetch(5, imap_hbm, imap_ref)
    fetch(1, gain_hbm, gain_ref)
    fetch_weight(0, 0, wsem.at[0])
    fetch_weight(0, 1, wsem.at[0])

    pl.semaphore_wait(barrier, 1 + 2 * (a + jnp.where(b == inner - 1, b, 0)))

    def ready_near(k, c):
        tell(near_ready, a * inner + k)
        return c

    def ready_far(k, c):
        tell(far_ready, k * inner + b)
        return c

    @pl.when((tp == 1) & (b == inner - 1))
    def _():
        lax.fori_loop(0, b, ready_near, 0)


    lax.fori_loop(0, a, ready_far, 0)

    bd_in[...] = jnp.zeros_like(bd_in)
    bd_out[...] = jnp.zeros_like(bd_out)
    when = lax.broadcasted_iota(jnp.int32, (rows, 2 * rows), 0)
    upto = lax.broadcasted_iota(jnp.int32, (rows, 2 * rows), 1)
    sums[...] = jnp.where(
        ((upto < rows) & (when <= upto)) | ((upto >= rows) & (when > upto - rows)), 1.0, 0.0
    ).astype(BF16)
    col = lax.broadcasted_iota(jnp.int32, (groups, chans), 1)
    row = lax.broadcasted_iota(jnp.int32, (groups, chans), 0)
    to_chan[...] = jnp.where((col >= row * gch) & (col < (row + 1) * gch), 1.0, 0.0).astype(BF16)

    def remote(src, dst, s, r, dev):
        return pltpu.make_async_remote_copy(
            src_ref=src, dst_ref=dst, send_sem=s, recv_sem=r, device_id=dev, device_id_type=MESH
        )

    in_copies[0].wait()
    x_copy = remote(x_ref, xr, x_sem.at[0], x_sem.at[1], partner)
    x_copy.start()

    fetch(3, init_hbm, init_ref)
    fetch(6, omap_hbm, omap_ref)
    fetch(7, skip_hbm, skip_ref)
    fetch(8, taps_hbm, taps_ref)
    for i in (1, 3, 2):
        for h in (0, 1):
            fetch_weight(i, h, wsem.at[i])
    for i, w, deep in ((1, co_hbm, cwide), (0, so_hbm, chans)):
        for h, part in ((0, tp), (1, other)):
            pltpu.make_async_copy(
                w.at[pl.ds(part * deep, deep), :], ov.at[pl.ds(2 * i * chans + h * deep, deep), :], osem.at[0]
            ).start()

    lane = lax.broadcasted_iota(jnp.int32, (1, LANES), 1)

    def pair_up(i, v):
        pairs[pl.ds(i * groups, groups), :] = v
        even = pairs[pl.ds(i * groups, prow, stride=2), :]
        odd = pairs[pl.ds(i * groups + 1, prow, stride=2), :]
        return jnp.where(lane < state, even, odd)

    def twice(v):
        return jnp.concatenate([v, v], axis=1)

    for i in (4, 2, 5, 1):
        in_copies[i].wait()
    ld = ld_ref[...]

    def time_sums(cols):
        added = jnp.dot(jnp.concatenate(split3(ld), axis=0), sums[:, cols], preferred_element_type=F32)
        return added[:groups] + added[groups : 2 * groups] + added[2 * groups :]

    def per_channel(v):
        hi, mid, _ = split3(v.T)
        return jnp.dot(hi, to_chan[...], preferred_element_type=F32) + jnp.dot(
            mid, to_chan[...], preferred_element_type=F32
        )

    gain = jnp.sqrt(minus_expm1(2.0 * ld))
    chan_end[...] = per_channel(gain * jnp.exp(time_sums(slice(rows, 2 * rows))))
    tot = pair_up(
        3, jnp.broadcast_to(jnp.exp(jnp.sum(ld, axis=1, keepdims=True)), (groups, LANES))
    )
    theta = pair_up(0, twice(rot_ref[...]))
    turn = jnp.cos(theta), jnp.sin(theta)
    step = turn
    for k in range(8):
        for i in (0, 1):
            powers[i, pl.ds(k * prow, prow), :] = step[i]
        step = cmul(step, turn) if k < 7 else step
    sixteen = cmul(step, step)
    leap = sixteen
    for k in range(rows // 16 - 1):
        for i in (0, 1):
            powers[i, pl.ds((8 + k) * prow, prow), :] = leap[i]
        leap = cmul(leap, sixteen)
    whole = cpow(step, rows // 8)
    for r in range(prow):
        even = [powers[i, pl.ds(r, 8, stride=prow), :] for i in (0, 1)]
        eight = [powers[i, pl.ds(7 * prow + r, 1), :] for i in (0, 1)]
        odd = cmul(even, eight)
        base = [jnp.concatenate([even[i], odd[i]], axis=0).astype(BF16) for i in (0, 1)]
        for t in range(0, rows, 16):
            now = base
            if t > 0:
                at = pl.ds((8 + t // 16 - 1) * prow + r, 1)
                now = cmul(
                    base,
                    [jnp.broadcast_to(powers[i, at, :], (16, LANES)).astype(BF16) for i in (0, 1)],
                )
            for i in (0, 1):
                tbl[t : t + 16, (2 * r + i) * LANES : (2 * r + i + 1) * LANES] = now[i]

    def spread_map(src, dst):
        for b in range(blocks):
            for q in range(quads):
                g = b * per_block + 2 * q
                one = src[g].astype(F32)
                two = src[g + 1].astype(F32)
                one_r = jnp.concatenate([one[:, state:], one[:, :state]], axis=1)
                two_r = jnp.concatenate([two[:, state:], two[:, :state]], axis=1)
                low = lane < state
                re = jnp.concatenate([jnp.where(low, one, 0.0), jnp.where(low, 0.0, two_r)], axis=0)
                im = jnp.concatenate([jnp.where(low, one_r, 0.0), jnp.where(low, 0.0, two)], axis=0)
                at = pl.ds(b * LANES + q * 2 * gch, 2 * gch)
                dst[at, 2 * q * LANES : (2 * q + 1) * LANES] = re.astype(BF16)
                dst[at, (2 * q + 1) * LANES : (2 * q + 2) * LANES] = im.astype(BF16)

    spread_map(imap_ref, bd_in)
    own = x_ref[...].astype(F32)
    scaled = (own * gain_ref[:, pl.ds(pl.multiple_of(tp * half, LANES), half)]).astype(BF16)
    squares = jnp.sum(own * own, axis=1, keepdims=True)
    wait_weight(0)
    partial = jnp.dot(scaled, wv[0, :half], preferred_element_type=F32)
    acc[:, :half] = scaled

    x_copy.wait_recv()
    far_x = xr[...].astype(F32)
    scaled_far = (far_x * gain_ref[:, pl.ds(pl.multiple_of(other * half, LANES), half)]).astype(BF16)
    squares = squares + jnp.sum(far_x * far_x, axis=1, keepdims=True)
    scale = lax.rsqrt(squares / (2 * half) + EPS)

    acc[:, half:] = scaled_far
    total = partial + jnp.dot(scaled_far, wv[0, half:], preferred_element_type=F32)
    drive_in = (total * scale).astype(BF16)
    din[...] = drive_in
    ends_in = (drive_in.astype(F32) * chan_end[...]).astype(BF16).T
    for r in range(prow):
        q = r % quads
        at = slice(r * 2 * gch, (r + 1) * 2 * gch)
        seen = jnp.dot(
            ends_in[at], tbl[:, 2 * r * LANES : (2 * r + 2) * LANES], preferred_element_type=F32
        )
        m_re = bd_in[at, 2 * q * LANES : (2 * q + 1) * LANES].astype(F32)
        m_im = bd_in[at, (2 * q + 1) * LANES : (2 * q + 2) * LANES].astype(F32)
        c, d = seen[:, :LANES], seen[:, LANES:]
        rowed[0, r : r + 1, :] = jnp.sum(c * m_re + d * m_im, axis=0, keepdims=True)
        rowed[1, r : r + 1, :] = jnp.sum(c * m_im - d * m_re, axis=0, keepdims=True)
    e_re, e_im = cmul(whole, (rowed[0], rowed[1]))

    near_in[tp, b, pl.ds(0, prow), :] = e_re.astype(BF16)
    near_in[tp, b, pl.ds(prow, prow), :] = e_im.astype(BF16)
    fore = lax.rem(lax.broadcasted_iota(jnp.int32, (prow, LANES), 1), state) < state // 2

    def packed(v):
        hi, mid, _ = split3(v)
        return jnp.where(fore, hi.astype(F32), mid.astype(F32)).astype(BF16)

    near_in[tp, b, pl.ds(2 * prow, prow), :] = packed(tot)

    def wait_many(ref, sems, count, upto, sent):
        for j in range(1, upto + 1):
            @pl.when(count == j)
            def _():
                part = ref.at[pl.ds(0, j)]
                copy = remote(part, part, sems[0], sems[1], partner)
                copy.wait_send() if sent else copy.wait_recv()

    def near_copy(k):
        return remote(
            near_in.at[tp, b],
            near_in.at[tp, b],
            near_sem.at[2],
            near_sem.at[tp],
            {"sp": a * inner + k, "tp": 1},
        )

    def far_copy(k):
        return remote(
            far_out, far_in.at[a], far_sem.at[0], far_sem.at[1], {"sp": k * inner + b, "tp": 1}
        )

    near_from = jnp.where(a < last, 0, b + 1)
    near_upto = jnp.where(a < last, inner, b)
    @pl.when(b < inner - 1)
    def _():
        pl.semaphore_wait(near_ready, 1)

    def send_near(k, c):
        @pl.when((k != b) | ((tp == 0) & (a < last)))
        def _():
            near_copy(k).start()

        return c

    lax.fori_loop(near_from, inner, send_near, 0)

    in_copies[3].wait()
    aux[0], aux[1] = whole
    aux[2] = pair_up(1, twice(init_ref[0]))
    aux[3] = pair_up(2, twice(init_ref[1]))
    aux_copy = remote(aux, aux_far, aux_sem.at[0], aux_sem.at[1], partner)
    dup_copies = [
        remote(src, dst, dup_sem.at[0, (0, 1, 2, 2, 1)[i]], dup_sem.at[1, (0, 1, 2, 2, 1)[i]], partner)
        for i, (src, dst) in enumerate(
            (
                (tbl, table_far),
                (map_t.at[pl.ds(0, states), :], map_far.at[pl.ds(0, states), :]),
                (post.at[1], post_far.at[1]),
                (post.at[0], post_far.at[0]),
                (map_t.at[pl.ds(states, states), :], map_far.at[pl.ds(states, states), :]),
            )
        )
    ]

    def give(copy):
        @pl.when(tp == 0)
        def _():
            copy.start()

    waited = [
        remote(src, dst, dup_sem.at[0, i], dup_sem.at[1, i], partner)
        for i, (src, dst) in enumerate(((tbl, table_far), (map_t, map_far), (post, post_far)))
    ]

    give(aux_copy)

    def project(i):
        wait_weight(i)
        total = jnp.dot(acc[...], wv[i], preferred_element_type=F32)
        return (total * scale).astype(BF16)

    value = project(1)
    pre_gate = project(3)
    mixed = (pre_gate.astype(F32) * value.astype(F32)).astype(BF16).astype(F32)
    pad[pl.ds(8, rows), :] = mixed
    tail_copy = remote(
        pad.at[pl.ds(rows, 8), :],
        pad.at[pl.ds(0, 8), :],
        tail_sem.at[0],
        tail_sem.at[1],
        {"sp": lax.rem(sp + 1, n), "tp": tp},
    )

    @pl.when(hop_on)
    def _():
        pl.semaphore_wait(far_ready, 2 * (last - a))

    @pl.when(sp < n - 1)
    def _():
        tail_copy.start()

    give(dup_copies[0])

    for i in (6, 7):
        in_copies[i].wait()
    spread_map(omap_ref, bd_out)
    for k in range(blocks):
        map_t[2 * k * bstates : 2 * (k + 1) * bstates, :] = bd_out[k * LANES : (k + 1) * LANES, :].T
    give(dup_copies[1])

    ld = ld_ref[...]
    gain = jnp.sqrt(minus_expm1(2.0 * ld))
    late = per_channel(jnp.concatenate([jnp.exp(time_sums(slice(0, rows))), gain], axis=1))
    post[1] = late[:rows]
    give(dup_copies[2])
    chan_gain[...] = late[rows:]
    mags = split3(jnp.exp(ld).T)[:2]
    for k in range(blocks):
        col = lax.broadcasted_iota(jnp.int32, (groups, bstates), 1) + k * bstates
        row = lax.broadcasted_iota(jnp.int32, (groups, bstates), 0)
        spread = jnp.where(
            (col >= row * state) & (col < (row + 1) * state), 1.0, 0.0
        ).astype(BF16)
        m = jnp.dot(mags[0], spread, preferred_element_type=F32) + jnp.dot(
            mags[1], spread, preferred_element_type=F32
        )
        for q in range(quads):
            mag[pl.ds(k * quads + q, rows, stride=prow), :] = m[:, q * LANES : (q + 1) * LANES]

    zero = jnp.zeros((prow, LANES), F32)

    def unpacked(v):
        v = v.astype(F32)
        keep = lax.rem(lax.broadcasted_iota(jnp.int32, v.shape, 1), state) < state // 2
        return v + jnp.where(keep, pltpu.roll(v, LANES - state // 2, 1), pltpu.roll(v, state // 2, 1))

    def unpack_all(ref, count, index):
        packs = [
            ref[index(h, k) + (pl.ds(2 * prow, prow),)] for h in (0, 1) for k in range(count)
        ]
        v = unpacked(jnp.concatenate(packs, axis=0))
        for h in (0, 1):
            mags_in[h, : count * prow, :] = v[h * count * prow : (h + 1) * count * prow]

    def message(ref, h, k):
        return (
            ref[pl.ds(0, prow), :].astype(F32),
            ref[pl.ds(prow, prow), :].astype(F32),
            mags_in[h, pl.ds(pl.multiple_of(k * prow, prow), prow), :],
        )

    def send_far(k, c):
        far_copy(outer + a - k).start()
        return c

    def join_halves(turned, first):
        unpack_all(near_in, inner, lambda h, k: (h, k))

        def half_step(h, k, c):
            ends, mag_all, phase, mine = c[0:2], c[2], c[3:5], c[5:]
            k_re, k_im, k_mag = message(near_in.at[h, k], h, k)
            moved = cmul((turned[h][0] * k_mag, turned[h][1] * k_mag), ends)
            now = (moved[0] + k_re, moved[1] + k_im, mag_all * k_mag) + cmul(turned[h], phase)
            return now + tuple(jnp.where(k < b, v, w) for v, w in zip(now, mine))

        def near_step(k, c):
            return tuple(half_step(h, k, c[h]) for h in (0, 1))

        one = jnp.ones((prow, LANES), F32)
        begin = [tuple(jnp.where(a == 0, v, zero) for v in f) + (one, one, zero) for f in first]
        planes = lax.fori_loop(0, near_upto, near_step, tuple(v + v for v in begin))
        for h, plane in enumerate(planes):
            far_out[h, pl.ds(0, prow), :] = plane[0].astype(BF16)
            far_out[h, pl.ds(prow, prow), :] = plane[1].astype(BF16)
            far_out[h, pl.ds(2 * prow, prow), :] = packed(plane[2])
            for i in range(5):
                held[h, i] = plane[5 + i]

    def join_near():
        @pl.when(tp == 1)
        def _():
            for h in (1, 0):
                wait_many(
                    near_in.at[h],
                    (near_sem.at[2], near_sem.at[h]),
                    jnp.where(a < last, inner - h, b),
                    inner,
                    False,
                )
            join_halves(
                ((aux_far[0], aux_far[1]), whole), ((aux_far[2], aux_far[3]), (aux[2], aux[3]))
            )

        @pl.when((a < last) & (b < inner - 1))
        def _():
            pl.semaphore_wait(far_ready, 2 * (last - a))

        @pl.when((tp == 1) & (a < last))
        def _():
            lax.fori_loop(a + 1, outer, send_far, 0)

    @pl.when(tp == 1)
    def _():
        aux_copy.wait_recv()

    @pl.when(b > 1)
    def _():
        join_near()

    hc[0] = project(2)
    gained = (din[...].astype(F32) * chan_gain[...]).astype(BF16)
    for k in range(blocks):
        blk = jnp.dot(
            gained[:, k * LANES : (k + 1) * LANES],
            bd_in[k * LANES : (k + 1) * LANES, :],
            preferred_element_type=F32,
        )
        for q in range(quads):
            r = k * quads + q
            drv[pl.ds(r, rows, stride=pitch), :] = blk[:, 2 * q * LANES : (2 * q + 1) * LANES]
            drv[pl.ds(prow + r, rows, stride=pitch), :] = blk[
                :, (2 * q + 1) * LANES : (2 * q + 2) * LANES
            ]

    @pl.when(b == 1)
    def _():
        join_near()

    hc_copy = remote(hc.at[0], hc.at[1], hc_sem.at[0], hc_sem.at[1], partner)

    def convolve():
        @pl.when(sp == 0)
        def _():
            pad[pl.ds(0, 8), :] = jnp.zeros((8, cwide), F32)

        in_copies[8].wait()

        @pl.when(sp > 0)
        def _():
            tail_copy.wait_recv()

        conv = jnp.zeros((rows, cwide), F32)
        for k in range(width):
            conv = conv + pad[pl.ds(8 + k - (width - 1), rows), :] * taps_ref[k : k + 1, :].astype(F32)
        hc[0] = (hc[0].astype(F32) * conv).astype(BF16)
        hc_copy.start()
        pltpu.make_async_copy(ov, ov, osem.at[0]).wait()
        oacc[...] = jnp.dot(hc[0], ov[2 * chans : 2 * chans + cwide], preferred_element_type=F32)

    even = (lax.rem(b, 2) == 0) & (sp > 0)

    @pl.when(jnp.logical_not(even))
    def _():
        convolve()

    give(dup_copies[4])

    def scan(t, h):
        m = mag[pl.ds(pl.multiple_of(t * prow, prow), prow), :]
        base = pl.multiple_of(t * pitch, 8)
        d_re = drv[pl.ds(base, prow), :]
        d_im = drv[pl.ds(base + prow, prow), :]
        f_re, f_im = m * turn[0], m * turn[1]
        new_re = (f_re * h[0] + d_re) - f_im * h[1]
        new_im = (f_re * h[1] + d_im) + f_im * h[0]
        drv[pl.ds(base, prow), :] = new_re
        drv[pl.ds(base + prow, prow), :] = new_im
        return new_re, new_im

    lax.fori_loop(0, rows, scan, (zero, zero), unroll=8)

    @pl.when(b == 0)
    def _():
        join_near()

    for k in range(blocks):
        cols = slice(k * LANES, (k + 1) * LANES)
        at = [half_row + k * quads + q for q in range(quads) for half_row in (0, prow)]
        st = jnp.concatenate(
            [drv[pl.ds(r, rows, stride=pitch), :].astype(BF16) for r in at], axis=1
        )
        read = jnp.dot(
            st, map_t[2 * k * bstates : 2 * (k + 1) * bstates, :], preferred_element_type=F32
        )
        post[0, :, cols] = read + skip_ref[:, cols] * din[:, cols].astype(F32)

    give(dup_copies[3])

    @pl.when(even)
    def _():
        convolve()


    def add_far_conv():
        hc_copy.wait_recv()
        oacc[...] += jnp.dot(hc[1], ov[2 * chans + cwide :], preferred_element_type=F32)

    @pl.when(tp == 0)
    def _():
        add_far_conv()

    def entering(h, turned):
        plane_turn = cpow(turned, inner)

        def far_step(k, c):
            k_re, k_im, k_mag = message(far_in.at[k, h], h, k)
            moved = cmul((plane_turn[0] * k_mag, plane_turn[1] * k_mag), c)
            return moved[0] + k_re, moved[1] + k_im

        before = lax.fori_loop(0, a, far_step, (zero, zero))
        moved = cmul((held[h, 3] * held[h, 2], held[h, 4] * held[h, 2]), before)
        return held[h, 0] + moved[0], held[h, 1] + moved[1]

    def correct(h, table, mapped, local, slot):
        moved = []
        for k in range(blocks):
            turned = []
            for r in range(k * quads, (k + 1) * quads):
                c, d = (
                    table[:, (2 * r + i) * LANES : (2 * r + i + 1) * LANES].reshape(rows // 16, 16, LANES)
                    for i in (0, 1)
                )
                h_re, h_im = (
                    jnp.broadcast_to(enter[h, i, r : r + 1, :], (16, LANES)).astype(BF16)[None]
                    for i in (0, 1)
                )
                turned += cmul((c, d), (h_re, h_im))
            moved.append(
                jnp.dot(
                    jnp.concatenate([v.reshape(rows, LANES) for v in turned], axis=1),
                    mapped[2 * k * bstates : 2 * (k + 1) * bstates, :],
                    preferred_element_type=F32,
                )
            )
        made = []
        for k in range(blocks):
            cols = slice(k * LANES, (k + 1) * LANES)
            made.append(gelu(local[0, :, cols] + local[1, :, cols] * moved[k]).astype(BF16))
            hs[slot, :, cols] = made[k]
        return made

    enter_copy = remote(enter.at[0], enter.at[0], enter_sem.at[0], enter_sem.at[1], partner)

    @pl.when(tp == 1)
    def _():
        wait_many(far_in, (far_sem.at[0], far_sem.at[1]), a, last, False)
        unpack_all(far_in, last, lambda h, k: (k, h))
        enter[0, 0], enter[0, 1] = entering(0, (aux_far[0], aux_far[1]))

        @pl.when(sp > 0)
        def _():
            enter_copy.start()

        enter[1, 0], enter[1, 1] = entering(1, whole)

    @pl.when((tp == 0) & (sp > 0))
    def _():
        enter_copy.wait_recv()

    @pl.when((tp == 0) & (sp == 0))
    def _():
        enter[0, 0], enter[0, 1] = aux[2], aux[3]

    hs_copy = remote(hs.at[0], hs.at[1], hs_sem.at[0], hs_sem.at[1], partner)

    def add_own(blks):
        oacc[...] += jnp.dot(
            jnp.concatenate(blks, axis=1), ov[:chans], preferred_element_type=F32
        )

    @pl.when(tp == 1)
    def _():
        correct(1, tbl, map_t, post, 0)
        hs_copy.start()
        for copy in waited:
            copy.wait_recv()
        hc_copy.wait_recv()
        correct(0, table_far, map_far, post_far, 1)
        oacc[...] += jnp.dot(hs[0], ov[:chans], preferred_element_type=F32) + jnp.dot(
            hc[1], ov[2 * chans + cwide :], preferred_element_type=F32
        )

    @pl.when(tp == 0)
    def _():
        add_own(correct(0, tbl, map_t, post, 0))

    @pl.when(tp == 0)
    def _():
        hs_copy.wait_recv()

    out_ref[...] = (oacc[...] + jnp.dot(hs[1], ov[chans : 2 * chans], preferred_element_type=F32)).astype(BF16)

    x_copy.wait_send()
    hc_copy.wait_send()

    @pl.when(tp == 1)
    def _():
        hs_copy.wait_send()

    @pl.when((tp == 1) & (sp > 0))
    def _():
        enter_copy.wait_send()

    @pl.when(tp == 0)
    def _():
        aux_copy.wait_send()
        for copy in waited:
            copy.wait_send()

    @pl.when(sp < n - 1)
    def _():
        tail_copy.wait_send()

    wait_many(
        near_in.at[0],
        (near_sem.at[2], near_sem.at[0]),
        jnp.where(a < last, inner - tp, inner - 1 - b),
        inner,
        True,
    )

    @pl.when(tp == 1)
    def _():
        wait_many(far_in, (far_sem.at[0], far_sem.at[1]), last - a, last, True)


def on_device(
    activations,
    norm_gain,
    state_proj,
    value_proj,
    post_gate_proj,
    pre_gate_proj,
    input_map,
    output_map,
    skip_gain,
    rotation,
    log_decay,
    initial_state,
    conv_taps,
    state_out,
    conv_out,
):
    n = lax.axis_size("sp")
    rows, half = activations.shape
    groups, state = rotation.shape
    chans = state_proj.shape[1]
    cwide = value_proj.shape[1]
    outs = state_out.shape[1]
    states = groups * state
    prow = states // LANES
    inner = inner_of(n)
    bdw = 2 * states // (chans // LANES)
    vmem = pl.BlockSpec(memory_space=pltpu.VMEM)
    hbm = pl.BlockSpec(memory_space=pl.ANY)
    dma = pltpu.SemaphoreType.DMA
    return pl.pallas_call(
        functools.partial(kernel, n),
        out_shape=pltpu.VMEM((rows, outs), BF16),
        in_specs=[hbm] * 15,
        out_specs=vmem,
        scratch_shapes=[
            pltpu.VMEM((rows, half), BF16),
            pltpu.VMEM((1, 2 * half), F32),
            pltpu.VMEM(input_map.shape, BF16),
            pltpu.VMEM((groups, output_map.shape[2], output_map.shape[1]), F32),
            pltpu.VMEM((1, chans), F32),
            pltpu.VMEM((groups, state), F32),
            pltpu.VMEM((groups, rows), F32),
            pltpu.VMEM(initial_state.shape, F32),
            pltpu.VMEM(conv_taps.shape, BF16),
            pltpu.VMEM((4, 2 * half, chans), BF16),
            pltpu.VMEM((2 * chans + 2 * cwide, outs), BF16),
            pltpu.VMEM((rows, half), BF16),
            pltpu.VMEM((rows, 2 * half), BF16),
            pltpu.VMEM((rows, chans), BF16),
            pltpu.VMEM((chans, bdw), BF16),
            pltpu.VMEM((chans, bdw), BF16),
            pltpu.VMEM((2 * states, LANES), BF16),
            pltpu.VMEM((rows, 2 * states), BF16),
            pltpu.VMEM((2, (8 + rows // 16) * prow, LANES), F32),
            pltpu.VMEM((rows, chans), F32),
            pltpu.VMEM((rows, chans), F32),
            pltpu.VMEM((2, prow, LANES), F32),
            pltpu.VMEM((2, rows, chans), F32),
            pltpu.VMEM((rows, 2 * states), BF16),
            pltpu.VMEM((2 * states, LANES), BF16),
            pltpu.VMEM((2, rows, chans), F32),
            pltpu.VMEM((4, prow, LANES), F32),
            pltpu.VMEM((4, prow, LANES), F32),
            pltpu.VMEM((2, max(inner, n // inner) * prow, LANES), F32),
            pltpu.VMEM((2, 5, prow, LANES), F32),
            pltpu.VMEM((2, 2, prow, LANES), F32),
            pltpu.VMEM((rows, 2 * rows), BF16),
            pltpu.VMEM((groups, chans), BF16),
            pltpu.VMEM((rows * prow, LANES), F32),
            pltpu.VMEM((rows * (2 * prow + 8), LANES), F32),
            pltpu.VMEM((4 * groups, LANES), F32),
            pltpu.VMEM((rows + 8, cwide), F32),
            pltpu.VMEM((2, inner, 3 * prow, LANES), BF16),
            pltpu.VMEM((n // inner, 2, 3 * prow, LANES), BF16),
            pltpu.VMEM((2, 3 * prow, LANES), BF16),
            pltpu.VMEM((2, rows, chans), BF16),
            pltpu.VMEM((2, rows, cwide), BF16),
            pltpu.VMEM((rows, outs), F32),
            dma((9,)),
            dma((4,)),
            dma((1,)),
            dma((2,)),
            dma((2,)),
            dma((2,)),
            dma((2,)),
            dma((3,)),
            dma((2,)),
            dma((2,)),
            dma((2,)),
            dma((2, 3)),
            pltpu.SemaphoreType.REGULAR,
            pltpu.SemaphoreType.REGULAR,
        ],
        compiler_params=pltpu.CompilerParams(collective_id=0, has_side_effects=True),
    )(
        activations,
        norm_gain.reshape(1, -1),
        state_proj,
        value_proj,
        post_gate_proj,
        pre_gate_proj,
        input_map,
        jnp.swapaxes(output_map, 1, 2),
        skip_gain.reshape(1, -1),
        rotation,
        jnp.swapaxes(log_decay, 0, 1),
        initial_state,
        conv_taps,
        state_out,
        conv_out,
    )


def solution(mesh):
    return jax.shard_map(
        on_device,
        mesh=mesh,
        in_specs=(
            P("sp", "tp"),
            P(),
            P(None, "tp"),
            P(None, "tp"),
            P(None, "tp"),
            P(None, "tp"),
            P("tp", None, None),
            P("tp", None, None),
            P("tp"),
            P("tp", None),
            P("sp", "tp"),
            P(None, "tp", None),
            P(None, "tp"),
            P(None, "tp"),
            P(None, "tp"),
        ),
        out_specs=P("sp", "tp"),
        check_vma=False,
    )
```
